32 devices in a mesh: fs: 4 (over z), tp: 8 (over y, x, core).
Axes of the slice: x: 2, y: 2, z: 4, core: 2. Of those that a mesh axis runs over, the one named last changes fastest.
Arguments:
- tokens: bfloat16 [768, 2304], P('fs'), may hold values from -6 to 6
- gate_train: float32 [8, 2304, 2304], P(None, 'fs', 'tp'), may hold values from -0.125 to 0.125
- up_train: float32 [8, 2304, 2304], P(None, 'fs', 'tp'), may hold values from -0.125 to 0.125
- down_train: float32 [8, 2304, 2304], P(None, 'fs', 'tp'), may hold values from -0.125 to 0.125
- gain: float32 [2304], P('fs'), may hold values from 0.1 to 1.9
- routes: int32 [768, 2], P('fs'), may hold values from 0 to 7, all different within a row; in each aligned block of 192 rows (0 to 191, 192 to 383, ...) at most 72 rows name the same one
- route_weights: float32 [768, 2], P('fs'), may hold values from 0.1 to 1
Outputs:
- gate_new: bfloat16 [8, 2304, 2304], P('tp')
- up_new: bfloat16 [8, 2304, 2304], P('tp')
- down_new: bfloat16 [8, 2304, 2304], P('tp')
- mixed: bfloat16 [768, 2304], P('fs', 'tp')
The draws below stay inside these ranges and needn't reach their ends.
Inputs may be any that keep to these rules, and one draw needn't show every extreme that they name: `routes`: each row names two different experts; in each aligned block of 192 rows at most 72 rows name one expert, a bound that some block reaches.
All inputs are finite; a program needn't handle non-finite values.
Results may differ from the reference program's by a relative error of at most 0.0095.
Values may be sent and summed in bfloat16 or wider, within the bound.
A program may use at most 128 MiB of HBM per device.

```python
import math
import jax
import jax.numpy as jnp
import numpy as np
from jax import lax

D = 2304
FF = 2304
EXPERTS = 8
ROWS = 192
CAP = 72
TOKENS = 768
N_FS = 4
N_TP = 8


def levels(own_key, shape, pieces, smallest, largest):
    level, own = 1.0, jax.random.fold_in(own_key, 6)
    for position, shards_of in pieces:
        heights = jnp.exp(jax.random.uniform(jax.random.fold_in(own, position), (shards_of,), jnp.float32, smallest / len(pieces), largest / len(pieces)))
        level = level * jnp.repeat(heights, shape[position] // shards_of).reshape([-1 if axis == position else 1 for axis in range(len(shape))])
    return level


def routed_block(own_key, own, number, rows, number_of, top, most, lean):
    sequence = jax.random.permutation(own_key, number_of)
    packed, usual = load_shares(number_of, rows * top, most, lean, True), load_shares(number_of, rows * top, most, lean, False)
    places = jnp.arange(number_of)

    def named(lengths, rotation):
        used = int((lengths > 0).sum())
        fixed = max(1, used // 4)
        passed = fixed + (places - fixed + rotation * (used - fixed)) % max(1, number_of - fixed)
        return jnp.zeros((number_of,), jnp.int32).at[sequence[jnp.where(places < fixed, places, passed)]].set(jnp.asarray(lengths, jnp.int32))

    lengths = jnp.where(number % 4 == 0, named(packed, number // 4), named(usual, number - number // 4 - 1))
    mixed = jax.random.permutation(jax.random.fold_in(own, 3), number_of)
    giver, receiver = mixed[0:number_of // 2 * 2:2], mixed[1:number_of // 2 * 2:2]
    margin = jnp.minimum(lengths[giver] - 1, most - lengths[receiver]) // 2
    margin = jnp.where((giver == sequence[0]) | (receiver == sequence[0]) | (lengths[receiver] == 0), 0, jnp.maximum(margin, 0))
    passed = jax.random.randint(jax.random.fold_in(own, 4), (number_of // 2,), 0, 1 << 20) % (margin + 1)
    lengths = lengths.at[giver].add(-passed).at[receiver].add(passed)
    members = jnp.searchsorted(jnp.cumsum(lengths), jnp.arange(rows * top), side="right").astype(jnp.int32)
    table = members.reshape(top, rows).T
    table = table[jax.random.permutation(jax.random.fold_in(own, 1), rows)]
    rotation = jax.random.randint(jax.random.fold_in(own, 2), (rows, 1), 0, top)
    return jnp.take_along_axis(table, (jnp.arange(top)[None, :] + rotation) % top, axis=1)


def load_shares(count, total, bound, skew, full):
    loads = [(1 << 20) // math.isqrt(rank ** skew) + 1 for rank in range(1, count + 1)]
    largest = bound if full else min(bound, max(-(-total // count), total * loads[0] // sum(loads)))
    least = 1 if total - largest >= count - 1 else 0
    given, rest = [largest] + [least] * (count - 1), total - largest - least * (count - 1)
    while rest > 0:
        free = [i for i in range(1, count) if given[i] < largest] or [i for i in range(1, count) if given[i] < bound]
        pool, remaining = sum([loads[i] for i in free]), rest
        for i in free:
            extra = min(bound - given[i], max(1, remaining * loads[i] // pool), rest)
            given[i] = given[i] + extra
            rest = rest - extra
    return np.array(given)


def scatter_about(stream_key, shape, scale, bound, split=(), kind=jnp.bfloat16):
    array = scale * jax.random.normal(stream_key, shape, jnp.float32)
    if split:
        array = array * levels(stream_key, shape, split, -0.22, 0.18)
    return jnp.clip(array, -bound, bound).astype(kind)


def setup_inputs(seed: int = 0) -> dict:
    keys = jax.random.split(jax.random.key(seed), 8)
    tokens = scatter_about(keys[0], (TOKENS, D), 1.0, 6.0, ((0, 4),))
    gate_train = scatter_about(keys[1], (EXPERTS, D, FF), D ** -0.5, 0.125, ((1, 4), (2, 8)), jnp.float32)
    up_train = scatter_about(keys[2], (EXPERTS, D, FF), D ** -0.5, 0.125, ((1, 4), (2, 8)), jnp.float32)
    down_train = scatter_about(keys[3], (EXPERTS, D, FF), FF ** -0.5, 0.125, ((1, 4), (2, 8)), jnp.float32)
    gain = jnp.clip(1.0 + 0.18 * jax.random.normal(keys[4], (D,), jnp.float32), 0.1, 1.9)
    routes_keys = jax.random.split(jax.random.fold_in(keys[5], 1), TOKENS // ROWS)
    routes_turns = jax.random.permutation(jax.random.fold_in(keys[5], 3), TOKENS // ROWS)
    routes = jax.vmap(lambda own, number: routed_block(jax.random.fold_in(keys[5], 2), own, number, ROWS, EXPERTS, 2, CAP, 1))(routes_keys, routes_turns).reshape((TOKENS, 2))
    route_weights = jnp.clip(0.1 + 0.9 * jax.random.uniform(keys[6], (TOKENS, 2), jnp.float32) ** levels(keys[6], (TOKENS, 2), ((0, 4),), -0.2, 0.2), 0.1, 1.0)
    return dict(tokens=tokens, gate_train=gate_train, up_train=up_train, down_train=down_train, gain=gain, routes=routes, route_weights=route_weights)


norm_eps = 1e-06

def arrange(matrix):
    experts, row_count, col_count = matrix.shape
    slices = N_TP // experts
    piece_width = col_count // (N_TP * slices)
    shaped = matrix.reshape(experts, row_count, N_TP, slices, piece_width)
    return shaped.transpose(0, 3, 2, 4, 1).reshape(experts * slices, col_count // slices, row_count)

def reference(tokens, gate_train, up_train, down_train, gain, routes, route_weights):
    gain_column = gain.astype(jnp.float32)[None, :, None]
    gate_new = arrange((gate_train * gain_column).astype(jnp.bfloat16))
    up_new = arrange((up_train * gain_column).astype(jnp.bfloat16))
    down_new = arrange(down_train.astype(jnp.bfloat16))
    tokens_wide = tokens.astype(jnp.float32)
    normed = (tokens_wide * lax.rsqrt(lax.optimization_barrier(jnp.mean(tokens_wide * tokens_wide, axis=1, keepdims=True)) + norm_eps)).astype(jnp.bfloat16)
    slices = N_TP // EXPERTS

    def one_block(inputs):
        block_rows, block_routes, block_weights = inputs

        def per_expert(expert, output):
            matches = block_routes == expert
            member = jnp.any(matches, axis=1)
            slot_index = (jnp.cumsum(member.astype(jnp.int32)) - 1).astype(jnp.int32)
            marked = jnp.where(member, slot_index, -1)
            picker = (marked[None, :] == jnp.arange(CAP, dtype=jnp.int32)[:, None]).astype(jnp.bfloat16)
            chosen = jnp.dot(picker, block_rows, preferred_element_type=jnp.float32).astype(jnp.bfloat16)
            gate_part = lax.dynamic_slice_in_dim(gate_new, expert * slices, slices, 0).astype(jnp.float32)
            up_part = lax.dynamic_slice_in_dim(up_new, expert * slices, slices, 0).astype(jnp.float32)
            down_part = lax.dynamic_slice_in_dim(down_new, expert * slices, slices, 0).astype(jnp.float32)
            chosen_wide = chosen.astype(jnp.float32)
            gate_pre = jnp.einsum('cd,sfd->scf', chosen_wide, gate_part)
            up_pre = jnp.einsum('cd,sfd->scf', chosen_wide, up_part)
            hidden = (jax.nn.silu(gate_pre) * up_pre).astype(jnp.bfloat16)
            partial_value = jnp.einsum('scf,sfd->scd', hidden.astype(jnp.float32), down_part).astype(jnp.bfloat16)
            slice_total = lax.optimization_barrier(jnp.sum(partial_value.astype(jnp.float32), axis=0))
            row_weight = lax.optimization_barrier(jnp.sum(jnp.where(matches, block_weights, 0.0), axis=1))
            gathered = jnp.take(slice_total, jnp.clip(slot_index, 0, CAP - 1), axis=0)
            return output + jnp.where(member[:, None], row_weight[:, None] * gathered, 0.0)
        return lax.fori_loop(0, EXPERTS, per_expert, jnp.zeros((ROWS, D), jnp.float32)).astype(jnp.bfloat16)
    mixed = lax.map(one_block, (normed.reshape(N_FS, ROWS, D), routes.reshape(N_FS, ROWS, 2), route_weights.reshape(N_FS, ROWS, 2)))
    return (gate_new, up_new, down_new, mixed.reshape(TOKENS, D))
```

```python
import jax
import jax.numpy as jnp
from jax import lax
from jax.experimental import pallas as pl
from jax.experimental.pallas import tpu as pltpu
from jax.sharding import PartitionSpec as P

CAP = 72


norm_eps = 1e-06


def arrange(matrix, tp_count):
    experts, row_count, col_count = matrix.shape
    slices = tp_count // experts
    piece_width = col_count // slices
    shaped = matrix.reshape(experts, row_count, slices, piece_width)
    return shaped.transpose(0, 2, 3, 1).reshape(tp_count, piece_width, row_count)


def block_of(*counts):
    for size in (256, 128):
        if all(count % size == 0 for count in counts):
            return size
    return None


def flip(wide, total_rows, first_row, base=None):
    features, rows = wide.shape
    size = block_of(rows, first_row, total_rows) or rows
    first = first_row // size

    def kernel(*refs):
        refs[-1][...] = refs[0][...].T

    in_specs = [pl.BlockSpec((features, size), lambda i: (0, i))]
    operands = [wide]
    aliases = {}
    if base is not None:
        in_specs.append(pl.BlockSpec(memory_space=pl.ANY))
        operands.append(base)
        aliases = {1: 0}
    return pl.pallas_call(
        kernel,
        grid=(rows // size,),
        in_specs=in_specs,
        out_specs=pl.BlockSpec((size, features), lambda i: (first + i, 0)),
        out_shape=jax.ShapeDtypeStruct((total_rows, features), wide.dtype),
        input_output_aliases=aliases,
        cost_estimate=pl.CostEstimate(
            flops=0, bytes_accessed=4 * features * rows, transcendentals=0
        ),
    )(*operands)


def columns(wide, first, count, *others):
    size = block_of(first, count, *others)
    if size is None:
        return lax.slice_in_dim(wide, first, first + count, axis=1), count, 0
    return wide, size, first // size


def flip_product(wide, first, rows, chosen):
    features = wide.shape[0]
    wide, size, start = columns(wide, first, rows)
    slots = chosen.shape[0]

    def kernel(wide_ref, chosen_ref, rows_ref, product_ref):
        value = wide_ref[...]
        rows_ref[...] = value.T
        product_ref[...] = jnp.dot(chosen_ref[...], value, preferred_element_type=jnp.float32)

    return pl.pallas_call(
        kernel,
        grid=(rows // size,),
        in_specs=[
            pl.BlockSpec((features, size), lambda i: (0, start + i)),
            pl.BlockSpec((slots, features), lambda i: (0, 0)),
        ],
        out_specs=[
            pl.BlockSpec((size, features), lambda i: (i, 0)),
            pl.BlockSpec((slots, size), lambda i: (0, i)),
        ],
        out_shape=[
            jax.ShapeDtypeStruct((rows, features), wide.dtype),
            jax.ShapeDtypeStruct((slots, rows), jnp.float32),
        ],
        cost_estimate=pl.CostEstimate(
            flops=2 * slots * features * rows,
            bytes_accessed=4 * features * rows,
            transcendentals=0,
        ),
    )(wide, chosen)


def spread(train, gain):
    experts, features, count = train.shape
    rows = experts * count
    size = block_of(rows) or rows

    def kernel(train_ref, gain_ref, out_ref):
        out_ref[...] = (train_ref[...] * gain_ref[...]).astype(jnp.bfloat16).T

    return pl.pallas_call(
        kernel,
        grid=(rows // size,),
        in_specs=[
            pl.BlockSpec((size, features), lambda i: (i, 0)),
            pl.BlockSpec((1, features), lambda i: (0, 0)),
        ],
        out_specs=pl.BlockSpec((features, size), lambda i: (0, i)),
        out_shape=jax.ShapeDtypeStruct((features, rows), jnp.bfloat16),
        cost_estimate=pl.CostEstimate(
            flops=train.size, bytes_accessed=6 * train.size, transcendentals=0
        ),
    )(train.transpose(0, 2, 1).reshape(rows, features), gain[None, :])


def flip_dot(wide, first, total_rows, hidden):
    features = wide.shape[0]
    slots, rows = hidden.shape
    wide, size, start = columns(wide, first, rows, total_rows)

    def kernel(wide_ref, hidden_ref, rows_ref, total_ref):
        turned = wide_ref[...].T
        rows_ref[...] = turned

        @pl.when(pl.program_id(0) == 0)
        def _():
            total_ref[...] = jnp.zeros_like(total_ref)

        total_ref[...] += jnp.dot(hidden_ref[...], turned, preferred_element_type=jnp.float32)

    return pl.pallas_call(
        kernel,
        grid=(rows // size,),
        in_specs=[
            pl.BlockSpec((features, size), lambda i: (0, start + i)),
            pl.BlockSpec((slots, size), lambda i: (0, i)),
        ],
        out_specs=[
            pl.BlockSpec((size, features), lambda i: (i, 0)),
            pl.BlockSpec((slots, features), lambda i: (0, 0)),
        ],
        out_shape=[
            jax.ShapeDtypeStruct((total_rows, features), wide.dtype),
            jax.ShapeDtypeStruct((slots, features), jnp.float32),
        ],
        cost_estimate=pl.CostEstimate(
            flops=2 * slots * features * rows,
            bytes_accessed=4 * features * rows,
            transcendentals=0,
        ),
    )(wide, hidden)


def keep_dot(weights, chosen):
    rows, features = weights.shape
    size = block_of(rows) or rows
    slots = chosen.shape[0]

    def kernel(weights_ref, chosen_ref, rows_ref, product_ref):
        rows_ref[...] = weights_ref[...]
        product_ref[...] = lax.dot_general(
            chosen_ref[...],
            weights_ref[...],
            (((1,), (1,)), ((), ())),
            preferred_element_type=jnp.float32,
        )

    return pl.pallas_call(
        kernel,
        grid=(rows // size,),
        in_specs=[
            pl.BlockSpec((size, features), lambda i: (i, 0)),
            pl.BlockSpec((slots, features), lambda i: (0, 0)),
        ],
        out_specs=[
            pl.BlockSpec((size, features), lambda i: (i, 0)),
            pl.BlockSpec((slots, size), lambda i: (0, i)),
        ],
        out_shape=[
            jax.ShapeDtypeStruct((rows, features), weights.dtype),
            jax.ShapeDtypeStruct((slots, rows), jnp.float32),
        ],
        cost_estimate=pl.CostEstimate(
            flops=2 * slots * features * rows,
            bytes_accessed=4 * features * rows,
            transcendentals=0,
        ),
    )(weights, chosen)


def after(value, *others):
    def kernel(*refs):
        pass

    return pl.pallas_call(
        kernel,
        in_specs=[pl.BlockSpec(memory_space=pl.ANY)] * (1 + len(others)),
        out_specs=pl.BlockSpec(memory_space=pl.ANY),
        out_shape=jax.ShapeDtypeStruct(value.shape, value.dtype),
        input_output_aliases={0: 0},
    )(value, *others)


def shards(tokens, gate_train, up_train, down_train, gain, routes, route_weights):
    tp_count = lax.axis_size("tp")
    experts = gate_train.shape[0]
    slices = tp_count // experts
    gain_column = gain[None, :, None]
    up_round = (up_train * gain_column).astype(jnp.bfloat16)
    down_round = down_train.astype(jnp.bfloat16)

    def exchange(matrix):
        return lax.all_to_all(matrix, "tp", split_axis=0, concat_axis=1, tiled=True)

    gate_all = lax.all_gather(spread(gate_train, gain), "fs", axis=0, tiled=True)
    features = gate_all.shape[0]

    up_moved = exchange(arrange(up_round, tp_count))[0].T
    down_moved = exchange(arrange(down_round, tp_count))[0].T
    units = down_moved.shape[1]
    size = block_of(units) or units
    main = units - size if units > size else units
    both_wide = lax.all_gather(
        jnp.concatenate([up_moved, down_moved[:, :main]], axis=1), "fs", axis=0, tiled=True
    )

    tokens_wide = tokens.astype(jnp.float32)
    normed = (
        tokens_wide
        * lax.rsqrt(jnp.mean(tokens_wide * tokens_wide, axis=1, keepdims=True) + norm_eps)
    ).astype(jnp.bfloat16)
    expert = lax.axis_index("tp") // slices
    matches = routes == expert
    member = jnp.any(matches, axis=1)
    slot_index = jnp.cumsum(member.astype(jnp.int32)) - 1
    marked = jnp.where(member, slot_index, -1)
    picker = (marked[None, :] == jnp.arange(CAP, dtype=jnp.int32)[:, None]).astype(jnp.bfloat16)
    chosen = jnp.dot(picker, normed, preferred_element_type=jnp.float32).astype(jnp.bfloat16)
    contract_last = (((1,), (1,)), ((), ()))

    gate_moved = exchange(gate_all.reshape(features, tp_count, -1).transpose(1, 2, 0))
    gate_new, gate_pre = keep_dot(gate_moved[0], chosen)
    up_new, up_pre = flip_product(both_wide, 0, units, chosen)
    hidden = (jax.nn.silu(gate_pre) * up_pre).astype(jnp.bfloat16)
    down_new, partial_value = flip_dot(both_wide, units, units, hidden[:, :main])
    if main < units:
        rest_moved = after(down_moved[:, main:], gate_new)
        rest_wide = lax.all_gather(rest_moved, "fs", axis=0, tiled=True)
        partial_value = partial_value + lax.dot_general(
            hidden[:, main:], rest_wide, contract_last, preferred_element_type=jnp.float32
        )
        down_new = flip(rest_wide, units, main, down_new)
    partial_value = partial_value.astype(jnp.bfloat16)

    labels = jnp.arange(experts, dtype=jnp.int32)
    member_all = jnp.any(routes[:, :, None] == labels[None, None, :], axis=1)
    slots_all = jnp.cumsum(member_all.astype(jnp.int32), axis=0) - 1
    slot_pair = jnp.take_along_axis(slots_all, routes, axis=1)
    flat_index = slot_pair * experts + routes
    received = lax.all_to_all(
        partial_value.reshape(CAP, tp_count, -1), "tp", split_axis=1, concat_axis=1, tiled=True
    )
    summed = jnp.sum(received.reshape(CAP, experts, slices, -1).astype(jnp.float32), axis=2)
    summed = summed.reshape(CAP * experts, -1)
    picked = jnp.take(summed, flat_index, axis=0)
    mixed = jnp.sum(route_weights[:, :, None] * picked, axis=1)
    return (gate_new[None], up_new[None], down_new[None], mixed.astype(jnp.bfloat16))


def fits(mesh_sizes, train):
    count, tp_count = mesh_sizes
    experts, features, units = train.shape
    return (
        experts == tp_count
        and tp_count & (tp_count - 1) == 0
        and count >= 4
        and count % 2 == 0
        and features % 128 == 64
        and units % 32 == 0
    )


def main_start(block, features):
    return block * features + (64 if block % 2 else 0)


def prepare(gate, up, down, gain):
    experts, units, features = gate.shape
    wide, half = features - 64, units // 2
    mats = (gate, up, down)

    def kernel(odd_ref, gate_ref, up_ref, down_ref, gain_ref, main_ref, rest_ref):
        def write(odd):
            for m, ref in enumerate((gate_ref, up_ref, down_ref)):
                value = ref[0]
                if m < 2:
                    value = value * gain_ref[...]
                value = value.astype(jnp.bfloat16)
                if odd:
                    main, rest = value[:, 64:], value[:, :64]
                else:
                    main, rest = value[:, :wide], value[:, wide:]
                main_ref[m, 0] = main
                rest_ref[m, 0] = jnp.concatenate([rest[:half], rest[half:]], axis=1)

        @pl.when(odd_ref[0] == 0)
        def _():
            write(False)

        @pl.when(odd_ref[0] == 1)
        def _():
            write(True)

    odd = (lax.axis_index("fs") % 2).astype(jnp.int32).reshape(1)
    block = pl.BlockSpec((1, units, features), lambda i, s: (i, 0, 0))
    return pl.pallas_call(
        kernel,
        grid_spec=pltpu.PrefetchScalarGridSpec(
            num_scalar_prefetch=1,
            grid=(experts,),
            in_specs=[block, block, block, pl.BlockSpec((1, features), lambda i, s: (0, 0))],
            out_specs=[
                pl.BlockSpec((len(mats), 1, units, wide), lambda i, s: (0, i, 0, 0)),
                pl.BlockSpec((len(mats), 1, half, 128), lambda i, s: (0, i, 0, 0)),
            ],
        ),
        out_shape=[
            jax.ShapeDtypeStruct((len(mats), experts, units, wide), jnp.bfloat16),
            jax.ShapeDtypeStruct((len(mats), experts, half, 128), jnp.bfloat16),
        ],
        cost_estimate=pl.CostEstimate(
            flops=3 * gate.size, bytes_accessed=18 * gate.size, transcendentals=0
        ),
    )(odd, gate, up, down, gain)


def gather(own_main, own_rest, count):
    mats, tp_count, units, wide = own_main.shape
    half = own_rest.shape[2]
    pieces = mats * tp_count
    bits = tp_count.bit_length() - 1

    def kernel(
        own_main, own_rest, main, rest, hold, hold_rest, load_sem, keep_sem, plane_send, plane_recv,
        plane_rest_send, plane_rest_recv, line_send, line_recv, line_rest_send, line_rest_recv,
    ):
        z = lax.axis_index("fs")
        t = lax.axis_index("tp")

        def peer(p):
            total = 0
            for b in range(bits):
                mine, other = (t // (1 << b)) % 2, (p // (1 << b)) % 2
                total = total + (mine + other - 2 * mine * other) * (1 << b)
            return total

        def plane(m, p):
            e = peer(p)
            return pltpu.make_async_remote_copy(
                own_main.at[m, e], main.at[z, m, t], plane_send.at[m, p], plane_recv.at[m, p],
                device_id={"fs": z, "tp": e}, device_id_type=pl.DeviceIdType.MESH,
            )

        def plane_rest(m, p):
            e = peer(p)
            return pltpu.make_async_remote_copy(
                own_rest.at[m, e], rest.at[z, m, t], plane_rest_send.at[m, p], plane_rest_recv.at[m, p],
                device_id={"fs": z, "tp": e}, device_id_type=pl.DeviceIdType.MESH,
            )

        def line(way, step, i):
            block = z + step if way == 0 else z - step
            target = z - 1 if way == 0 else z + 1
            m, e = i // tp_count, peer(i % tp_count)
            return pltpu.make_async_remote_copy(
                main.at[block, m, e], main.at[block, m, e], line_send.at[way, step], line_recv.at[way, step, i],
                device_id={"fs": target, "tp": t}, device_id_type=pl.DeviceIdType.MESH,
            )

        def line_rest(way, step, m):
            block = z + step if way == 0 else z - step
            target = z - 1 if way == 0 else z + 1
            return pltpu.make_async_remote_copy(
                rest.at[block, m], rest.at[block, m], line_rest_send.at[way, step, m], line_rest_recv.at[way, step, m],
                device_id={"fs": target, "tp": t}, device_id_type=pl.DeviceIdType.MESH,
            )

        for m in range(mats):
            pltpu.make_async_copy(own_main.at[m, t], hold.at[m], load_sem.at[0, m]).start()
            pltpu.make_async_copy(own_rest.at[m, t], hold_rest.at[m], load_sem.at[1, m]).start()

        for m in range(mats):
            @pl.loop(1, tp_count)
            def _(p, m=m):
                plane(m, p).start()
                plane_rest(m, p).start()

        for m in range(mats):
            pltpu.make_async_copy(own_main.at[m, t], hold.at[m], load_sem.at[0, m]).wait()
            pltpu.make_async_copy(hold.at[m], main.at[z, m, t], keep_sem.at[0, m]).start()
            pltpu.make_async_copy(own_rest.at[m, t], hold_rest.at[m], load_sem.at[1, m]).wait()
            pltpu.make_async_copy(hold_rest.at[m], rest.at[z, m, t], keep_sem.at[1, m]).start()

        def has(way, step):
            return z + step <= count - 1 if way == 0 else z - step >= 0

        def sends(way):
            return z >= 1 if way == 0 else z <= count - 2

        late = pieces - tp_count
        for step in range(count):
            for m in range(mats):
                final = step == count - 1
                last = final and m == mats - 1
                skip = step == count - 2 and m == mats - 1
                if step == 0:
                    pltpu.make_async_copy(hold.at[m], main.at[z, m, t], keep_sem.at[0, m]).wait()
                    pltpu.make_async_copy(hold_rest.at[m], rest.at[z, m, t], keep_sem.at[1, m]).wait()

                @pl.loop(0, tp_count)
                def _(p, step=step, m=m, last=last, skip=skip, final=final):
                    i = m * tp_count + p
                    if step == 0:
                        @pl.when(p >= 1)
                        def _():
                            plane(m, p).wait_recv()
                    for way in range(2):
                        if step > 0 and not last:
                            @pl.when(has(way, step))
                            def _(way=way):
                                line(way, step - 1, i).wait_recv()
                        if not final and not skip:
                            @pl.when(has(way, step) & sends(way))
                            def _(way=way):
                                line(way, step, i).start()

                if step == 0:
                    @pl.loop(1, tp_count)
                    def _(p, m=m):
                        plane_rest(m, p).wait_recv()
                for way in range(2):
                    if step > 0:
                        @pl.when(has(way, step))
                        def _(way=way, step=step, m=m):
                            line_rest(way, step - 1, m).wait_recv()
                    if not final:
                        @pl.when(has(way, step) & sends(way))
                        def _(way=way, step=step, m=m):
                            line_rest(way, step, m).start()

        for m in range(mats):
            @pl.loop(1, tp_count)
            def _(p, m=m):
                plane(m, p).wait_send()
                plane_rest(m, p).wait_send()
        for step in range(count - 1):
            for way in range(2):
                @pl.when(has(way, step) & sends(way))
                def _(way=way, step=step):
                    sent = main.at[z, pl.ds(0, mats - 1 if step == count - 2 else mats)]
                    pltpu.make_async_copy(sent, sent, line_send.at[way, step]).wait()
                    for m in range(mats):
                        line_rest(way, step, m).wait_send()

    dma = pltpu.SemaphoreType.DMA
    sent = 2 * (count - 1) * (own_main.size + own_rest.size)
    return pl.pallas_call(
        kernel,
        in_specs=[pl.BlockSpec(memory_space=pl.ANY)] * 2,
        out_specs=[pl.BlockSpec(memory_space=pl.ANY)] * 2,
        out_shape=[
            jax.ShapeDtypeStruct((count,) + own_main.shape, own_main.dtype),
            jax.ShapeDtypeStruct((count,) + own_rest.shape, own_rest.dtype),
        ],
        scratch_shapes=[
            pltpu.VMEM((mats, units, wide), own_main.dtype),
            pltpu.VMEM((mats, half, 128), own_rest.dtype),
            dma((2, mats)),
            dma((2, mats)),
            dma((mats, tp_count)),
            dma((mats, tp_count)),
            dma((mats, tp_count)),
            dma((mats, tp_count)),
            dma((2, count - 1)),
            dma((2, count - 1, pieces)),
            dma((2, count - 1, mats)),
            dma((2, count - 1, mats)),
        ],
        compiler_params=pltpu.CompilerParams(has_side_effects=True),
        cost_estimate=pl.CostEstimate(flops=10**9, bytes_accessed=2 * sent, transcendentals=0),
    )(own_main, own_rest)


def joined(main_ref, rest_ref, out_ref):
    count, _, _, units, wide = main_ref.shape
    features = wide + 64
    half = units // 2
    for block in range(count):
        out_ref[:, pl.ds(main_start(block, features), wide)] = main_ref[block, 0, 0]
    for block in range(0, count, 2):
        first, second = rest_ref[block, 0, 0], rest_ref[block + 1, 0, 0]
        place = pl.ds(block * features + wide, 128)
        out_ref[:half, place] = jnp.concatenate([first[:, :64], second[:, :64]], axis=1)
        out_ref[half:, place] = jnp.concatenate([first[:, 64:], second[:, 64:]], axis=1)


def join_call(main, rest, which, kernel, operand, operand_spec, product_spec, product_shape):
    count, mats, tp_count, units, wide = main.shape
    half = rest.shape[3]
    features = count * (wide + 64)
    return pl.pallas_call(
        kernel,
        grid=(tp_count,),
        in_specs=[
            pl.BlockSpec((count, 1, 1, units, wide), lambda i: (0, which, i, 0, 0)),
            pl.BlockSpec((count, 1, 1, half, 128), lambda i: (0, which, i, 0, 0)),
            operand_spec,
        ],
        out_specs=[pl.BlockSpec((units, features), lambda i: (i, 0)), product_spec],
        out_shape=[
            jax.ShapeDtypeStruct((tp_count * units, features), main.dtype),
            jax.ShapeDtypeStruct(product_shape, jnp.float32),
        ],
        cost_estimate=pl.CostEstimate(
            flops=1000 * tp_count * units * features,
            bytes_accessed=4 * tp_count * units * features,
            transcendentals=0,
        ),
    )(main, rest, operand)


def join_in(main, rest, which, chosen):
    tp_count, units = main.shape[2:4]
    slots, features = chosen.shape

    def kernel(main_ref, rest_ref, chosen_ref, new_ref, product_ref):
        joined(main_ref, rest_ref, new_ref)
        product_ref[0] = lax.dot_general(
            chosen_ref[...], new_ref[...], (((1,), (1,)), ((), ())), preferred_element_type=jnp.float32
        )

    return join_call(
        main, rest, which, kernel, chosen,
        pl.BlockSpec((slots, features), lambda i: (0, 0)),
        pl.BlockSpec((1, slots, units), lambda i: (i, 0, 0)),
        (tp_count, slots, units),
    )


def join_out(main, rest, which, hidden):
    tp_count, slots, units = hidden.shape
    features = main.shape[0] * (main.shape[4] + 64)

    def kernel(main_ref, rest_ref, hidden_ref, new_ref, total_ref):
        joined(main_ref, rest_ref, new_ref)

        @pl.when(pl.program_id(0) == 0)
        def _():
            total_ref[...] = jnp.zeros_like(total_ref)

        total_ref[...] += jnp.dot(hidden_ref[0], new_ref[...], preferred_element_type=jnp.float32)

    return join_call(
        main, rest, which, kernel, hidden,
        pl.BlockSpec((1, slots, units), lambda i: (i, 0, 0)),
        pl.BlockSpec((slots, features), lambda i: (0, 0)),
        (slots, features),
    )


def join_far(arrived, kept, use_arrived, far_start, last_start, hidden, base):
    tp_count, units, wide = arrived.shape
    slots = hidden.shape[1]
    size = 256 if (wide % 256 == 0 and last_start % 256 == 0) else 128

    def kernel(scalar_ref, arrived_ref, kept_ref, hidden_ref, base_ref, new_ref, total_ref):
        value = jnp.where(scalar_ref[1] == 1, arrived_ref[0], kept_ref[0])
        new_ref[...] = value

        @pl.when(pl.program_id(1) == 0)
        def _():
            total_ref[...] = jnp.zeros_like(total_ref)

        total_ref[...] += jnp.dot(hidden_ref[0], value, preferred_element_type=jnp.float32)

    scalars = jnp.stack([far_start // size, use_arrived.astype(jnp.int32)])
    piece = pl.BlockSpec((1, units, size), lambda j, i, s: (i, 0, j))
    return pl.pallas_call(
        kernel,
        grid_spec=pltpu.PrefetchScalarGridSpec(
            num_scalar_prefetch=1,
            grid=(wide // size, tp_count),
            in_specs=[
                piece, piece,
                pl.BlockSpec((1, slots, units), lambda j, i, s: (i, 0, 0)),
                pl.BlockSpec(memory_space=pl.ANY),
            ],
            out_specs=[
                pl.BlockSpec((units, size), lambda j, i, s: (i, s[0] + j)),
                pl.BlockSpec((slots, size), lambda j, i, s: (0, j)),
            ],
        ),
        out_shape=[
            jax.ShapeDtypeStruct(base.shape, base.dtype),
            jax.ShapeDtypeStruct((slots, wide), jnp.float32),
        ],
        input_output_aliases={4: 0},
        cost_estimate=pl.CostEstimate(
            flops=2 * slots * arrived.size, bytes_accessed=6 * arrived.size, transcendentals=0
        ),
    )(scalars, arrived, kept, hidden, base)


def pick(tokens, routes, expert):
    tokens_wide = tokens.astype(jnp.float32)
    normed = (
        tokens_wide
        * lax.rsqrt(jnp.mean(tokens_wide * tokens_wide, axis=1, keepdims=True) + norm_eps)
    ).astype(jnp.bfloat16)
    member = jnp.any(routes == expert, axis=1)
    slot_index = jnp.cumsum(member.astype(jnp.int32)) - 1
    marked = jnp.where(member, slot_index, -1)
    picker = (marked[None, :] == jnp.arange(CAP, dtype=jnp.int32)[:, None]).astype(jnp.bfloat16)
    return jnp.dot(picker, normed, preferred_element_type=jnp.float32).astype(jnp.bfloat16)


def mix(partial_value, routes, route_weights, experts):
    tp_count = lax.axis_size("tp")
    labels = jnp.arange(experts, dtype=jnp.int32)
    member_all = jnp.any(routes[:, :, None] == labels[None, None, :], axis=1)
    slots_all = jnp.cumsum(member_all.astype(jnp.int32), axis=0) - 1
    slot_pair = jnp.take_along_axis(slots_all, routes, axis=1)
    flat_index = slot_pair * experts + routes
    received = lax.all_to_all(
        partial_value.reshape(CAP, tp_count, -1), "tp", split_axis=1, concat_axis=1, tiled=True
    )
    summed = received.astype(jnp.float32).reshape(CAP * experts, -1)
    picked = jnp.take(summed, flat_index, axis=0)
    return jnp.sum(route_weights[:, :, None] * picked, axis=1).astype(jnp.bfloat16)


def line_shards(tokens, gate_train, up_train, down_train, gain, routes, route_weights):
    count = lax.axis_size("fs")
    place = lax.axis_index("fs")
    experts, features, units = gate_train.shape
    own_main, own_rest = prepare(
        gate_train.transpose(0, 2, 1), up_train.transpose(0, 2, 1), down_train.transpose(0, 2, 1), gain[None, :]
    )
    main, rest = gather(own_main, own_rest, count)
    far = jnp.where(place < count // 2, count - 1, 0)
    kept = lax.dynamic_slice(main, (far, 2, 0, 0, 0), (1, 1) + main.shape[2:])[0, 0]
    arrived = lax.ppermute(kept, "fs", [(1, 0), (count - 2, count - 1)])
    main, rest, tokens, routes, route_weights = lax.optimization_barrier(
        (main, rest, tokens, routes, route_weights)
    )
    chosen = pick(tokens, routes, lax.axis_index("tp"))
    gate_new, gate_pre = join_in(main, rest, 0, chosen)
    up_new, up_pre = join_in(main, rest, 1, chosen)
    hidden = (jax.nn.silu(gate_pre) * up_pre).astype(jnp.bfloat16)
    down_new, total = join_out(main, rest, 2, hidden)
    at_end = (place == 0) | (place == count - 1)
    last_start = main_start(count - 1, features)
    far_start = jnp.where(far == 0, 0, last_start).astype(jnp.int32)
    down_new, far_total = join_far(arrived, kept, at_end, far_start, last_start, hidden, down_new)
    total = lax.dynamic_update_slice(total, far_total, (0, far_start))
    mixed = mix(total.astype(jnp.bfloat16), routes, route_weights, experts)
    return (gate_new[None], up_new[None], down_new[None], mixed)


def solution(mesh):
    sizes = (mesh.shape["fs"], mesh.shape["tp"])

    def step(*args):
        return (line_shards if fits(sizes, args[1]) else shards)(*args)

    in_specs = (
        P("fs", None),
        P(None, "fs", "tp"),
        P(None, "fs", "tp"),
        P(None, "fs", "tp"),
        P("fs"),
        P("fs", None),
        P("fs", None),
    )
    out_specs = (P("tp", None, None), P("tp", None, None), P("tp", None, None), P("fs", "tp"))
    return jax.shard_map(step, mesh=mesh, in_specs=in_specs, out_specs=out_specs, check_vma=False)
```

```python
import jax
import jax.numpy as jnp
from jax import lax
from jax.experimental import pallas as pl
from jax.experimental.pallas import tpu as pltpu
from jax.sharding import PartitionSpec as P


CAP = 72


norm_eps = 1e-06


def arrange(matrix, tp_count):
    experts, row_count, col_count = matrix.shape
    slices = tp_count // experts
    piece_width = col_count // slices
    shaped = matrix.reshape(experts, row_count, slices, piece_width)
    return shaped.transpose(0, 2, 3, 1).reshape(tp_count, piece_width, row_count)


def block_of(*counts):
    for size in (256, 128):
        if all(count % size == 0 for count in counts):
            return size
    return None


def flip(wide, total_rows, first_row, base=None):
    features, rows = wide.shape
    size = block_of(rows, first_row, total_rows) or rows
    first = first_row // size

    def kernel(*refs):
        refs[-1][...] = refs[0][...].T

    in_specs = [pl.BlockSpec((features, size), lambda i: (0, i))]
    operands = [wide]
    aliases = {}
    if base is not None:
        in_specs.append(pl.BlockSpec(memory_space=pl.ANY))
        operands.append(base)
        aliases = {1: 0}
    return pl.pallas_call(
        kernel,
        grid=(rows // size,),
        in_specs=in_specs,
        out_specs=pl.BlockSpec((size, features), lambda i: (first + i, 0)),
        out_shape=jax.ShapeDtypeStruct((total_rows, features), wide.dtype),
        input_output_aliases=aliases,
        cost_estimate=pl.CostEstimate(
            flops=0, bytes_accessed=4 * features * rows, transcendentals=0
        ),
    )(*operands)


def columns(wide, first, count, *others):
    size = block_of(first, count, *others)
    if size is None:
        return lax.slice_in_dim(wide, first, first + count, axis=1), count, 0
    return wide, size, first // size


def flip_product(wide, first, rows, chosen):
    features = wide.shape[0]
    wide, size, start = columns(wide, first, rows)
    slots = chosen.shape[0]

    def kernel(wide_ref, chosen_ref, rows_ref, product_ref):
        value = wide_ref[...]
        rows_ref[...] = value.T
        product_ref[...] = jnp.dot(chosen_ref[...], value, preferred_element_type=jnp.float32)

    return pl.pallas_call(
        kernel,
        grid=(rows // size,),
        in_specs=[
            pl.BlockSpec((features, size), lambda i: (0, start + i)),
            pl.BlockSpec((slots, features), lambda i: (0, 0)),
        ],
        out_specs=[
            pl.BlockSpec((size, features), lambda i: (i, 0)),
            pl.BlockSpec((slots, size), lambda i: (0, i)),
        ],
        out_shape=[
            jax.ShapeDtypeStruct((rows, features), wide.dtype),
            jax.ShapeDtypeStruct((slots, rows), jnp.float32),
        ],
        cost_estimate=pl.CostEstimate(
            flops=2 * slots * features * rows,
            bytes_accessed=4 * features * rows,
            transcendentals=0,
        ),
    )(wide, chosen)


def spread(train, gain):
    experts, features, count = train.shape
    rows = experts * count
    size = block_of(rows) or rows

    def kernel(train_ref, gain_ref, out_ref):
        out_ref[...] = (train_ref[...] * gain_ref[...]).astype(jnp.bfloat16).T

    return pl.pallas_call(
        kernel,
        grid=(rows // size,),
        in_specs=[
            pl.BlockSpec((size, features), lambda i: (i, 0)),
            pl.BlockSpec((1, features), lambda i: (0, 0)),
        ],
        out_specs=pl.BlockSpec((features, size), lambda i: (0, i)),
        out_shape=jax.ShapeDtypeStruct((features, rows), jnp.bfloat16),
        cost_estimate=pl.CostEstimate(
            flops=train.size, bytes_accessed=6 * train.size, transcendentals=0
        ),
    )(train.transpose(0, 2, 1).reshape(rows, features), gain[None, :])


def flip_dot(wide, first, total_rows, hidden):
    features = wide.shape[0]
    slots, rows = hidden.shape
    wide, size, start = columns(wide, first, rows, total_rows)

    def kernel(wide_ref, hidden_ref, rows_ref, total_ref):
        turned = wide_ref[...].T
        rows_ref[...] = turned

        @pl.when(pl.program_id(0) == 0)
        def _():
            total_ref[...] = jnp.zeros_like(total_ref)

        total_ref[...] += jnp.dot(hidden_ref[...], turned, preferred_element_type=jnp.float32)

    return pl.pallas_call(
        kernel,
        grid=(rows // size,),
        in_specs=[
            pl.BlockSpec((features, size), lambda i: (0, start + i)),
            pl.BlockSpec((slots, size), lambda i: (0, i)),
        ],
        out_specs=[
            pl.BlockSpec((size, features), lambda i: (i, 0)),
            pl.BlockSpec((slots, features), lambda i: (0, 0)),
        ],
        out_shape=[
            jax.ShapeDtypeStruct((total_rows, features), wide.dtype),
            jax.ShapeDtypeStruct((slots, features), jnp.float32),
        ],
        cost_estimate=pl.CostEstimate(
            flops=2 * slots * features * rows,
            bytes_accessed=4 * features * rows,
            transcendentals=0,
        ),
    )(wide, hidden)


def keep_dot(weights, chosen):
    rows, features = weights.shape
    size = block_of(rows) or rows
    slots = chosen.shape[0]

    def kernel(weights_ref, chosen_ref, rows_ref, product_ref):
        rows_ref[...] = weights_ref[...]
        product_ref[...] = lax.dot_general(
            chosen_ref[...],
            weights_ref[...],
            (((1,), (1,)), ((), ())),
            preferred_element_type=jnp.float32,
        )

    return pl.pallas_call(
        kernel,
        grid=(rows // size,),
        in_specs=[
            pl.BlockSpec((size, features), lambda i: (i, 0)),
            pl.BlockSpec((slots, features), lambda i: (0, 0)),
        ],
        out_specs=[
            pl.BlockSpec((size, features), lambda i: (i, 0)),
            pl.BlockSpec((slots, size), lambda i: (0, i)),
        ],
        out_shape=[
            jax.ShapeDtypeStruct((rows, features), weights.dtype),
            jax.ShapeDtypeStruct((slots, rows), jnp.float32),
        ],
        cost_estimate=pl.CostEstimate(
            flops=2 * slots * features * rows,
            bytes_accessed=4 * features * rows,
            transcendentals=0,
        ),
    )(weights, chosen)


def after(value, *others):
    def kernel(*refs):
        pass

    return pl.pallas_call(
        kernel,
        in_specs=[pl.BlockSpec(memory_space=pl.ANY)] * (1 + len(others)),
        out_specs=pl.BlockSpec(memory_space=pl.ANY),
        out_shape=jax.ShapeDtypeStruct(value.shape, value.dtype),
        input_output_aliases={0: 0},
    )(value, *others)


def shards(tokens, gate_train, up_train, down_train, gain, routes, route_weights):
    tp_count = lax.axis_size("tp")
    experts = gate_train.shape[0]
    slices = tp_count // experts
    gain_column = gain[None, :, None]
    up_round = (up_train * gain_column).astype(jnp.bfloat16)
    down_round = down_train.astype(jnp.bfloat16)

    def exchange(matrix):
        return lax.all_to_all(matrix, "tp", split_axis=0, concat_axis=1, tiled=True)

    gate_all = lax.all_gather(spread(gate_train, gain), "fs", axis=0, tiled=True)
    features = gate_all.shape[0]

    up_moved = exchange(arrange(up_round, tp_count))[0].T
    down_moved = exchange(arrange(down_round, tp_count))[0].T
    units = down_moved.shape[1]
    size = block_of(units) or units
    main = units - size if units > size else units
    both_wide = lax.all_gather(
        jnp.concatenate([up_moved, down_moved[:, :main]], axis=1), "fs", axis=0, tiled=True
    )

    tokens_wide = tokens.astype(jnp.float32)
    normed = (
        tokens_wide
        * lax.rsqrt(jnp.mean(tokens_wide * tokens_wide, axis=1, keepdims=True) + norm_eps)
    ).astype(jnp.bfloat16)
    expert = lax.axis_index("tp") // slices
    matches = routes == expert
    member = jnp.any(matches, axis=1)
    slot_index = jnp.cumsum(member.astype(jnp.int32)) - 1
    marked = jnp.where(member, slot_index, -1)
    picker = (marked[None, :] == jnp.arange(CAP, dtype=jnp.int32)[:, None]).astype(jnp.bfloat16)
    chosen = jnp.dot(picker, normed, preferred_element_type=jnp.float32).astype(jnp.bfloat16)
    contract_last = (((1,), (1,)), ((), ()))

    gate_moved = exchange(gate_all.reshape(features, tp_count, -1).transpose(1, 2, 0))
    gate_new, gate_pre = keep_dot(gate_moved[0], chosen)
    up_new, up_pre = flip_product(both_wide, 0, units, chosen)
    hidden = (jax.nn.silu(gate_pre) * up_pre).astype(jnp.bfloat16)
    down_new, partial_value = flip_dot(both_wide, units, units, hidden[:, :main])
    if main < units:
        rest_moved = after(down_moved[:, main:], gate_new)
        rest_wide = lax.all_gather(rest_moved, "fs", axis=0, tiled=True)
        partial_value = partial_value + lax.dot_general(
            hidden[:, main:], rest_wide, contract_last, preferred_element_type=jnp.float32
        )
        down_new = flip(rest_wide, units, main, down_new)
    partial_value = partial_value.astype(jnp.bfloat16)

    labels = jnp.arange(experts, dtype=jnp.int32)
    member_all = jnp.any(routes[:, :, None] == labels[None, None, :], axis=1)
    slots_all = jnp.cumsum(member_all.astype(jnp.int32), axis=0) - 1
    slot_pair = jnp.take_along_axis(slots_all, routes, axis=1)
    flat_index = slot_pair * experts + routes
    received = lax.all_to_all(
        partial_value.reshape(CAP, tp_count, -1), "tp", split_axis=1, concat_axis=1, tiled=True
    )
    summed = jnp.sum(received.reshape(CAP, experts, slices, -1).astype(jnp.float32), axis=2)
    summed = summed.reshape(CAP * experts, -1)
    picked = jnp.take(summed, flat_index, axis=0)
    mixed = jnp.sum(route_weights[:, :, None] * picked, axis=1)
    return (gate_new[None], up_new[None], down_new[None], mixed.astype(jnp.bfloat16))


def fits(mesh_sizes, train):
    count, tp_count = mesh_sizes
    experts, features, units = train.shape
    return (
        experts == tp_count
        and tp_count & (tp_count - 1) == 0
        and count >= 4
        and count % 2 == 0
        and features % 128 == 64
        and units % 32 == 0
        and units <= features - 64
    )


def main_start(block, features):
    return block * features + (64 if block % 2 else 0)


def prepare(gate, up, down, gain):
    experts, units, features = gate.shape
    wide, half = features - 64, units // 2
    mats = (gate, up, down)

    def kernel(odd_ref, gate_ref, up_ref, down_ref, gain_ref, main_ref, rest_ref):
        def write(odd):
            for m, ref in enumerate((gate_ref, up_ref, down_ref)):
                value = ref[0]
                if m < 2:
                    value = value * gain_ref[...]
                value = value.astype(jnp.bfloat16)
                if odd:
                    main, rest = value[:, 64:], value[:, :64]
                else:
                    main, rest = value[:, :wide], value[:, wide:]
                main_ref[m, 0] = main
                rest_ref[m, 0] = jnp.concatenate([rest[:half], rest[half:]], axis=1)

        @pl.when(odd_ref[0] == 0)
        def _():
            write(False)

        @pl.when(odd_ref[0] == 1)
        def _():
            write(True)

    odd = (lax.axis_index("fs") % 2).astype(jnp.int32).reshape(1)
    block = pl.BlockSpec((1, units, features), lambda i, s: (i, 0, 0))
    return pl.pallas_call(
        kernel,
        grid_spec=pltpu.PrefetchScalarGridSpec(
            num_scalar_prefetch=1,
            grid=(experts,),
            in_specs=[block, block, block, pl.BlockSpec((1, features), lambda i, s: (0, 0))],
            out_specs=[
                pl.BlockSpec((len(mats), 1, units, wide), lambda i, s: (0, i, 0, 0)),
                pl.BlockSpec((len(mats), 1, half, 128), lambda i, s: (0, i, 0, 0)),
            ],
        ),
        out_shape=[
            jax.ShapeDtypeStruct((len(mats), experts, units, wide), jnp.bfloat16),
            jax.ShapeDtypeStruct((len(mats), experts, half, 128), jnp.bfloat16),
        ],
        cost_estimate=pl.CostEstimate(
            flops=3 * gate.size, bytes_accessed=18 * gate.size, transcendentals=0
        ),
    )(odd, gate, up, down, gain)


def gather(own_main, own_rest, tokens, info, count, held):
    mats, tp_count, half = own_rest.shape[:3]
    pieces, units, wide = own_main.shape
    bits = tp_count.bit_length() - 1

    def kernel(
        own_main, own_rest, tokens, info, main, rest, near_tokens, near_info, early, last, hold, hold_rest, load_sem, keep_sem,
        plane_send, plane_recv, plane_rest_send, plane_rest_recv, line_send, line_recv, line_rest_send,
        line_rest_recv, near_send, near_recv, pass_hold, pass_load, pass_keep,
    ):
        z = lax.axis_index("fs")
        t = lax.axis_index("tp")

        def peer(p):
            total = 0
            for b in range(bits):
                mine, other = (t // (1 << b)) % 2, (p // (1 << b)) % 2
                total = total + (mine + other - 2 * mine * other) * (1 << b)
            return total

        def plane(m, p):
            e = peer(p)
            return pltpu.make_async_remote_copy(
                own_main.at[m * tp_count + e], main.at[z, m * tp_count + t], plane_send.at[m, p], plane_recv.at[m, p],
                device_id={"fs": z, "tp": e}, device_id_type=pl.DeviceIdType.MESH,
            )

        def plane_rest(m, p):
            e = peer(p)
            return pltpu.make_async_remote_copy(
                own_rest.at[m, e], rest.at[z, m, t], plane_rest_send.at[m, p], plane_rest_recv.at[m, p],
                device_id={"fs": z, "tp": e}, device_id_type=pl.DeviceIdType.MESH,
            )

        def line(way, step, i):
            block = z + step if way == 0 else z - step
            target = z - 1 if way == 0 else z + 1
            piece = main.at[block, i // tp_count * tp_count + peer(i % tp_count)]
            return pltpu.make_async_remote_copy(
                piece, piece, line_send.at[way, step], line_recv.at[way, step, i],
                device_id={"fs": target, "tp": t}, device_id_type=pl.DeviceIdType.MESH,
            )

        def line_rest(way, step, m):
            block = z + step if way == 0 else z - step
            target = z - 1 if way == 0 else z + 1
            return pltpu.make_async_remote_copy(
                rest.at[block, m], rest.at[block, m], line_rest_send.at[way, step, m], line_rest_recv.at[way, step, m],
                device_id={"fs": target, "tp": t}, device_id_type=pl.DeviceIdType.MESH,
            )

        for m in range(mats):
            pltpu.make_async_copy(own_main.at[m * tp_count + t], hold.at[m], load_sem.at[0, m]).start()
            pltpu.make_async_copy(own_rest.at[m, t], hold_rest.at[m], load_sem.at[1, m]).start()

        for m in range(mats):
            @pl.loop(1, tp_count)
            def _(p, m=m):
                plane(m, p).start()
                plane_rest(m, p).start()

        for m in range(mats):
            pltpu.make_async_copy(own_main.at[m * tp_count + t], hold.at[m], load_sem.at[0, m]).wait()
            pltpu.make_async_copy(hold.at[m], main.at[z, m * tp_count + t], keep_sem.at[0, m]).start()
            pltpu.make_async_copy(own_rest.at[m, t], hold_rest.at[m], load_sem.at[1, m]).wait()
            pltpu.make_async_copy(hold_rest.at[m], rest.at[z, m, t], keep_sem.at[1, m]).start()

        def has(way, step):
            return z + step <= count - 1 if way == 0 else z - step >= 0

        def sends(way):
            return z >= 1 if way == 0 else z <= count - 2

        def near(k):
            source, target = ((tokens, near_tokens), (info, near_info))[k]
            inward = jnp.where(z == 0, 1, count - 2)
            return pltpu.make_async_remote_copy(
                source, target, near_send.at[k], near_recv.at[k],
                device_id={"fs": inward, "tp": t}, device_id_type=pl.DeviceIdType.MESH,
            )

        def into_end(way, step, m, p, sender):
            if m < mats - 1 or step < count - 3:
                return True
            end = sender == 1 if way == 0 else sender == count - 2
            if step == count - 2:
                return jnp.logical_not(end)
            return jnp.logical_not(end & (peer(p) >= tp_count - held))

        def leaves(way, step, m, p):
            return into_end(way, step, m, p, z)

        def arrives(way, step, m, p):
            return into_end(way, step, m, p, z + 1 if way == 0 else z - 1)

        for step in range(count):
            for m in range(mats):
                if step == 0:
                    pltpu.make_async_copy(hold.at[m], main.at[z, m * tp_count + t], keep_sem.at[0, m]).wait()
                    pltpu.make_async_copy(hold_rest.at[m], rest.at[z, m, t], keep_sem.at[1, m]).wait()

                @pl.loop(0, tp_count)
                def _(p, step=step, m=m):
                    i = m * tp_count + p
                    if step == 0:
                        @pl.when(p >= 1)
                        def _():
                            plane(m, p).wait_recv()
                    for way in range(2):
                        if step > 0:
                            @pl.when(has(way, step) & arrives(way, step - 1, m, p))
                            def _(way=way):
                                line(way, step - 1, i).wait_recv()
                        if step < count - 1:
                            @pl.when(has(way, step) & sends(way) & leaves(way, step, m, p))
                            def _(way=way):
                                line(way, step, i).start()

                if step == 0:
                    @pl.loop(1, tp_count)
                    def _(p, m=m):
                        plane_rest(m, p).wait_recv()
                for way in range(2):
                    if step > 0:
                        @pl.when(has(way, step))
                        def _(way=way, step=step, m=m):
                            line_rest(way, step - 1, m).wait_recv()
                    if step < count - 1:
                        @pl.when(has(way, step) & sends(way))
                        def _(way=way, step=step, m=m):
                            line_rest(way, step, m).start()
            if step == 0:
                @pl.when((z == 0) | (z == count - 1))
                def _():
                    near(0).start()
                    near(1).start()

        @pl.when((z == 1) | (z == count - 2))
        def _():
            low = z < count // 2
            far, after_far = jnp.where(low, count - 1, 0), jnp.where(low, count - 2, 1)
            first = pieces - held
            found = [main.at[far, pieces - tp_count + i] for i in range(tp_count)]
            found += [main.at[after_far, first + i] for i in range(held)]
            goal = [early.at[i] for i in range(tp_count + held - 1)] + [last.at[0]]
            loads = [pltpu.make_async_copy(f, pass_hold.at[i], pass_load.at[i]) for i, f in enumerate(found)]
            keeps = [pltpu.make_async_copy(pass_hold.at[i], g, pass_keep.at[i]) for i, g in enumerate(goal)]
            for load in loads:
                load.start()
            for load, keep in zip(loads, keeps):
                load.wait()
                keep.start()
            for keep in keeps:
                keep.wait()

        for m in range(mats):
            @pl.loop(1, tp_count)
            def _(p, m=m):
                plane(m, p).wait_send()
                plane_rest(m, p).wait_send()

        @pl.when((z == 0) | (z == count - 1))
        def _():
            near(0).wait_send()
            near(1).wait_send()

        @pl.when((z == 1) | (z == count - 2))
        def _():
            near(0).wait_recv()
            near(1).wait_recv()

        for step in range(count - 1):
            for way in range(2):
                @pl.when(has(way, step) & sends(way))
                def _(way=way, step=step):
                    end = z == (1 if way == 0 else count - 2)

                    def settle(number, way=way, step=step):
                        sent = main.at[z, pl.ds(0, number)]
                        pltpu.make_async_copy(sent, sent, line_send.at[way, step]).wait()

                    if step == count - 2:
                        settle(pieces - tp_count)
                    elif step == count - 3:
                        pl.when(end)(lambda: settle(pieces - held))
                        pl.when(jnp.logical_not(end))(lambda: settle(pieces))
                    else:
                        settle(pieces)
                    for m in range(mats):
                        line_rest(way, step, m).wait_send()

    dma = pltpu.SemaphoreType.DMA
    sent = 2 * (count - 1) * (own_main.size + own_rest.size)
    return pl.pallas_call(
        kernel,
        in_specs=[pl.BlockSpec(memory_space=pl.ANY)] * 4,
        out_specs=[pl.BlockSpec(memory_space=pl.ANY)] * 6,
        out_shape=[
            jax.ShapeDtypeStruct((count,) + own_main.shape, own_main.dtype),
            jax.ShapeDtypeStruct((count,) + own_rest.shape, own_rest.dtype),
            jax.ShapeDtypeStruct(tokens.shape, tokens.dtype),
            jax.ShapeDtypeStruct(info.shape, info.dtype),
            jax.ShapeDtypeStruct((tp_count + held - 1, units, wide), own_main.dtype),
            jax.ShapeDtypeStruct((1, units, wide), own_main.dtype),
        ],
        scratch_shapes=[
            pltpu.VMEM((mats, units, wide), own_main.dtype),
            pltpu.VMEM((mats, half, 128), own_rest.dtype),
            dma((2, mats)),
            dma((2, mats)),
            dma((mats, tp_count)),
            dma((mats, tp_count)),
            dma((mats, tp_count)),
            dma((mats, tp_count)),
            dma((2, count - 1)),
            dma((2, count - 1, pieces)),
            dma((2, count - 1, mats)),
            dma((2, count - 1, mats)),
            dma((2,)),
            dma((2,)),
            pltpu.VMEM((tp_count + held, units, wide), own_main.dtype),
            dma((tp_count + held,)),
            dma((tp_count + held,)),
        ],
        compiler_params=pltpu.CompilerParams(has_side_effects=True),
        cost_estimate=pl.CostEstimate(flops=10**9, bytes_accessed=2 * sent, transcendentals=0),
    )(own_main, own_rest, tokens, info)


def joined(main_ref, rest_ref, out_ref):
    count, _, units, wide = main_ref.shape
    features = wide + 64
    half = units // 2
    for block in range(count):
        out_ref[:, pl.ds(main_start(block, features), wide)] = main_ref[block, 0]
    for block in range(0, count, 2):
        first, second = rest_ref[block, 0, 0], rest_ref[block + 1, 0, 0]
        place = pl.ds(block * features + wide, 128)
        out_ref[:half, place] = jnp.concatenate([first[:, :64], second[:, :64]], axis=1)
        out_ref[half:, place] = jnp.concatenate([first[:, 64:], second[:, 64:]], axis=1)


def join_call(main, rest, which, kernel, operand, operand_spec, product_spec, product_shape):
    count, _, tp_count, half = rest.shape[:4]
    units, wide = main.shape[2:]
    features = count * (wide + 64)
    return pl.pallas_call(
        kernel,
        grid=(tp_count,),
        in_specs=[
            pl.BlockSpec((count, 1, units, wide), lambda i: (0, which * tp_count + i, 0, 0)),
            pl.BlockSpec((count, 1, 1, half, 128), lambda i: (0, which, i, 0, 0)),
            operand_spec,
        ],
        out_specs=[pl.BlockSpec((units, features), lambda i: (i, 0)), product_spec],
        out_shape=[
            jax.ShapeDtypeStruct((tp_count * units, features), main.dtype),
            jax.ShapeDtypeStruct(product_shape, jnp.float32),
        ],
        cost_estimate=pl.CostEstimate(
            flops=1000 * tp_count * units * features,
            bytes_accessed=4 * tp_count * units * features,
            transcendentals=0,
        ),
    )(main, rest, operand)


def join_in(main, rest, which, chosen):
    tp_count, units = rest.shape[2], main.shape[2]
    slots, features = chosen.shape

    def kernel(main_ref, rest_ref, chosen_ref, new_ref, product_ref):
        joined(main_ref, rest_ref, new_ref)
        product_ref[0] = lax.dot_general(
            chosen_ref[...], new_ref[...], (((1,), (1,)), ((), ())), preferred_element_type=jnp.float32
        )

    return join_call(
        main, rest, which, kernel, chosen,
        pl.BlockSpec((slots, features), lambda i: (0, 0)),
        pl.BlockSpec((1, slots, units), lambda i: (i, 0, 0)),
        (tp_count, slots, units),
    )


def join_out(main, rest, which, hidden):
    _, slots, units = hidden.shape
    features = main.shape[0] * (main.shape[3] + 64)

    def kernel(main_ref, rest_ref, hidden_ref, new_ref, total_ref):
        joined(main_ref, rest_ref, new_ref)

        @pl.when(pl.program_id(0) == 0)
        def _():
            total_ref[...] = jnp.zeros_like(total_ref)

        total_ref[...] += jnp.dot(hidden_ref[0], new_ref[...], preferred_element_type=jnp.float32)

    return join_call(
        main, rest, which, kernel, hidden,
        pl.BlockSpec((1, slots, units), lambda i: (i, 0, 0)),
        pl.BlockSpec((slots, features), lambda i: (0, 0)),
        (slots, features),
    )


def place_late(arrived, places, base, count):
    pieces, units, wide = arrived.shape
    start = jnp.stack([column for _, _, column in places])

    def kernel(start_ref, arrived_ref, base_ref, new_ref, hold, load_sem, keep_sem):
        z = lax.axis_index("fs")

        @pl.when((z == 0) | (z == count - 1))
        def _():
            loads = [pltpu.make_async_copy(arrived_ref.at[i], hold.at[i], load_sem.at[i]) for i in range(pieces)]
            keeps = [
                pltpu.make_async_copy(
                    hold.at[i],
                    new_ref.at[
                        pl.ds(row * units, units), pl.ds(pl.multiple_of(start_ref[i], 128), wide)
                    ],
                    keep_sem.at[i],
                )
                for i, row, _ in places
            ]
            for load in loads:
                load.start()
            for load, keep in zip(loads, keeps):
                load.wait()
                keep.start()
            for keep in keeps:
                keep.wait()

    return pl.pallas_call(
        kernel,
        grid_spec=pltpu.PrefetchScalarGridSpec(
            num_scalar_prefetch=1,
            grid=(1,),
            in_specs=[pl.BlockSpec(memory_space=pl.ANY)] * 2,
            out_specs=pl.BlockSpec(memory_space=pl.ANY),
            scratch_shapes=[
                pltpu.VMEM(arrived.shape, arrived.dtype),
                pltpu.SemaphoreType.DMA((pieces,)),
                pltpu.SemaphoreType.DMA((pieces,)),
            ],
        ),
        out_shape=jax.ShapeDtypeStruct(base.shape, base.dtype),
        input_output_aliases={2: 0},
        cost_estimate=pl.CostEstimate(
            flops=500 * arrived.size, bytes_accessed=4 * arrived.size, transcendentals=0
        ),
    )(start, arrived, base)


def pick(tokens, routes, expert):
    tokens_wide = tokens.astype(jnp.float32)
    normed = (
        tokens_wide
        * lax.rsqrt(jnp.mean(tokens_wide * tokens_wide, axis=2, keepdims=True) + norm_eps)
    ).astype(jnp.bfloat16)
    member = jnp.any(routes == expert, axis=2)
    slot_index = jnp.cumsum(member.astype(jnp.int32), axis=1) - 1
    marked = jnp.where(member, slot_index, -1)
    picker = (marked[:, None, :] == jnp.arange(CAP, dtype=jnp.int32)[None, :, None]).astype(jnp.bfloat16)
    chosen = jnp.einsum("gcr,grd->gcd", picker, normed, preferred_element_type=jnp.float32)
    return chosen.astype(jnp.bfloat16).reshape(-1, tokens.shape[2])


def mix(partial_value, routes, route_weights, experts):
    tp_count = lax.axis_size("tp")
    groups = routes.shape[0]
    labels = jnp.arange(experts, dtype=jnp.int32)
    member_all = jnp.any(routes[:, :, :, None] == labels, axis=2)
    slots_all = jnp.cumsum(member_all.astype(jnp.int32), axis=1) - 1
    slot_pair = jnp.take_along_axis(slots_all, routes, axis=2)
    first = CAP * jnp.arange(groups, dtype=jnp.int32)[:, None, None]
    flat_index = (first + slot_pair) * experts + routes
    received = lax.all_to_all(
        partial_value.reshape(groups * CAP, tp_count, -1), "tp", split_axis=1, concat_axis=1, tiled=True
    )
    summed = received.astype(jnp.float32).reshape(groups * CAP * experts, -1)
    picked = jnp.take(summed, flat_index, axis=0)
    return jnp.sum(route_weights[:, :, :, None] * picked, axis=2).astype(jnp.bfloat16)


def line_shards(tokens, gate_train, up_train, down_train, gain, routes, route_weights):
    count = lax.axis_size("fs")
    place = lax.axis_index("fs")
    experts, features, _ = gate_train.shape
    held = experts - 3
    outward = [(1, 0), (count - 2, count - 1)]
    own_main, own_rest = prepare(
        gate_train.transpose(0, 2, 1), up_train.transpose(0, 2, 1), down_train.transpose(0, 2, 1), gain[None, :]
    )
    info = jnp.concatenate([routes.T.astype(jnp.float32), route_weights.T])
    main, rest, near_tokens, near_info, kept_early, kept_last = gather(
        own_main.reshape((-1,) + own_main.shape[2:]), own_rest, tokens, info, count, held
    )
    low = place < count // 2
    far_start = jnp.where(low, main_start(count - 1, features), main_start(0, features)).astype(jnp.int32)
    next_start = jnp.where(low, main_start(count - 2, features), main_start(1, features)).astype(jnp.int32)
    arrived_early = lax.ppermute(kept_early, "fs", outward)

    main, rest, near_tokens, near_info, tokens, info = lax.optimization_barrier(
        (main, rest, near_tokens, near_info, tokens, info)
    )
    both_info = jnp.stack([info, near_info])
    routed = routes.shape[1]
    both_routes = both_info[:, :routed].astype(jnp.int32).transpose(0, 2, 1)
    both_weights = both_info[:, routed:].transpose(0, 2, 1)
    chosen = pick(jnp.stack([tokens, near_tokens]), both_routes, lax.axis_index("tp"))
    gate_new, gate_pre = join_in(main, rest, 0, chosen)
    up_new, up_pre = join_in(main, rest, 1, chosen)
    hidden = (jax.nn.silu(gate_pre) * up_pre).astype(jnp.bfloat16)
    down_new, total = join_out(main, rest, 2, hidden)
    both_mixed = mix(total.astype(jnp.bfloat16), both_routes, both_weights, experts)
    wide = kept_last.shape[2]
    kept_rows = kept_last.reshape(-1, wide)
    mixed_rows = jnp.pad(both_mixed[1], ((0, 0), (0, wide - both_mixed.shape[2])))
    arrived_rows = lax.ppermute(jnp.concatenate([kept_rows, mixed_rows]), "fs", outward)
    arrived_last = arrived_rows[: kept_rows.shape[0]].reshape(kept_last.shape)
    near_mixed = arrived_rows[kept_rows.shape[0] :, : both_mixed.shape[2]]
    first = experts - held
    early = [(i, i, far_start) for i in range(experts)]
    early += [(experts + i, first + i, next_start) for i in range(held - 1)]
    down_new = place_late(arrived_early, early, down_new, count)
    down_new = place_late(arrived_last, [(0, experts - 1, next_start)], down_new, count)
    at_end = (place == 0) | (place == count - 1)
    mixed = jnp.where(at_end, near_mixed, both_mixed[0])
    return (gate_new[None], up_new[None], down_new[None], mixed)


def solution(mesh):
    sizes = (mesh.shape["fs"], mesh.shape["tp"])

    def step(*args):
        if not fits(sizes, args[1]):
            return shards(*args)
        return line_shards(*args)

    in_specs = (
        P("fs", None),
        P(None, "fs", "tp"),
        P(None, "fs", "tp"),
        P(None, "fs", "tp"),
        P("fs"),
        P("fs", None),
        P("fs", None),
    )
    out_specs = (P("tp", None, None), P("tp", None, None), P("tp", None, None), P("fs", "tp"))
    return jax.shard_map(step, mesh=mesh, in_specs=in_specs, out_specs=out_specs, check_vma=False)
```

```python
import jax
import jax.numpy as jnp
from jax import lax
from jax.experimental import pallas as pl
from jax.experimental.pallas import tpu as pltpu
from jax.sharding import PartitionSpec as P


CAP = 72


norm_eps = 1e-06


def arrange(matrix, tp_count):
    experts, row_count, col_count = matrix.shape
    slices = tp_count // experts
    piece_width = col_count // slices
    shaped = matrix.reshape(experts, row_count, slices, piece_width)
    return shaped.transpose(0, 2, 3, 1).reshape(tp_count, piece_width, row_count)


def block_of(*counts):
    for size in (256, 128):
        if all(count % size == 0 for count in counts):
            return size
    return None


def flip(wide, total_rows, first_row, base=None):
    features, rows = wide.shape
    size = block_of(rows, first_row, total_rows) or rows
    first = first_row // size

    def kernel(*refs):
        refs[-1][...] = refs[0][...].T

    in_specs = [pl.BlockSpec((features, size), lambda i: (0, i))]
    operands = [wide]
    aliases = {}
    if base is not None:
        in_specs.append(pl.BlockSpec(memory_space=pl.ANY))
        operands.append(base)
        aliases = {1: 0}
    return pl.pallas_call(
        kernel,
        grid=(rows // size,),
        in_specs=in_specs,
        out_specs=pl.BlockSpec((size, features), lambda i: (first + i, 0)),
        out_shape=jax.ShapeDtypeStruct((total_rows, features), wide.dtype),
        input_output_aliases=aliases,
        cost_estimate=pl.CostEstimate(
            flops=0, bytes_accessed=4 * features * rows, transcendentals=0
        ),
    )(*operands)


def columns(wide, first, count, *others):
    size = block_of(first, count, *others)
    if size is None:
        return lax.slice_in_dim(wide, first, first + count, axis=1), count, 0
    return wide, size, first // size


def flip_product(wide, first, rows, chosen):
    features = wide.shape[0]
    wide, size, start = columns(wide, first, rows)
    slots = chosen.shape[0]

    def kernel(wide_ref, chosen_ref, rows_ref, product_ref):
        value = wide_ref[...]
        rows_ref[...] = value.T
        product_ref[...] = jnp.dot(chosen_ref[...], value, preferred_element_type=jnp.float32)

    return pl.pallas_call(
        kernel,
        grid=(rows // size,),
        in_specs=[
            pl.BlockSpec((features, size), lambda i: (0, start + i)),
            pl.BlockSpec((slots, features), lambda i: (0, 0)),
        ],
        out_specs=[
            pl.BlockSpec((size, features), lambda i: (i, 0)),
            pl.BlockSpec((slots, size), lambda i: (0, i)),
        ],
        out_shape=[
            jax.ShapeDtypeStruct((rows, features), wide.dtype),
            jax.ShapeDtypeStruct((slots, rows), jnp.float32),
        ],
        cost_estimate=pl.CostEstimate(
            flops=2 * slots * features * rows,
            bytes_accessed=4 * features * rows,
            transcendentals=0,
        ),
    )(wide, chosen)


def spread(train, gain):
    experts, features, count = train.shape
    rows = experts * count
    size = block_of(rows) or rows

    def kernel(train_ref, gain_ref, out_ref):
        out_ref[...] = (train_ref[...] * gain_ref[...]).astype(jnp.bfloat16).T

    return pl.pallas_call(
        kernel,
        grid=(rows // size,),
        in_specs=[
            pl.BlockSpec((size, features), lambda i: (i, 0)),
            pl.BlockSpec((1, features), lambda i: (0, 0)),
        ],
        out_specs=pl.BlockSpec((features, size), lambda i: (0, i)),
        out_shape=jax.ShapeDtypeStruct((features, rows), jnp.bfloat16),
        cost_estimate=pl.CostEstimate(
            flops=train.size, bytes_accessed=6 * train.size, transcendentals=0
        ),
    )(train.transpose(0, 2, 1).reshape(rows, features), gain[None, :])


def flip_dot(wide, first, total_rows, hidden):
    features = wide.shape[0]
    slots, rows = hidden.shape
    wide, size, start = columns(wide, first, rows, total_rows)

    def kernel(wide_ref, hidden_ref, rows_ref, total_ref):
        turned = wide_ref[...].T
        rows_ref[...] = turned

        @pl.when(pl.program_id(0) == 0)
        def _():
            total_ref[...] = jnp.zeros_like(total_ref)

        total_ref[...] += jnp.dot(hidden_ref[...], turned, preferred_element_type=jnp.float32)

    return pl.pallas_call(
        kernel,
        grid=(rows // size,),
        in_specs=[
            pl.BlockSpec((features, size), lambda i: (0, start + i)),
            pl.BlockSpec((slots, size), lambda i: (0, i)),
        ],
        out_specs=[
            pl.BlockSpec((size, features), lambda i: (i, 0)),
            pl.BlockSpec((slots, features), lambda i: (0, 0)),
        ],
        out_shape=[
            jax.ShapeDtypeStruct((total_rows, features), wide.dtype),
            jax.ShapeDtypeStruct((slots, features), jnp.float32),
        ],
        cost_estimate=pl.CostEstimate(
            flops=2 * slots * features * rows,
            bytes_accessed=4 * features * rows,
            transcendentals=0,
        ),
    )(wide, hidden)


def keep_dot(weights, chosen):
    rows, features = weights.shape
    size = block_of(rows) or rows
    slots = chosen.shape[0]

    def kernel(weights_ref, chosen_ref, rows_ref, product_ref):
        rows_ref[...] = weights_ref[...]
        product_ref[...] = lax.dot_general(
            chosen_ref[...],
            weights_ref[...],
            (((1,), (1,)), ((), ())),
            preferred_element_type=jnp.float32,
        )

    return pl.pallas_call(
        kernel,
        grid=(rows // size,),
        in_specs=[
            pl.BlockSpec((size, features), lambda i: (i, 0)),
            pl.BlockSpec((slots, features), lambda i: (0, 0)),
        ],
        out_specs=[
            pl.BlockSpec((size, features), lambda i: (i, 0)),
            pl.BlockSpec((slots, size), lambda i: (0, i)),
        ],
        out_shape=[
            jax.ShapeDtypeStruct((rows, features), weights.dtype),
            jax.ShapeDtypeStruct((slots, rows), jnp.float32),
        ],
        cost_estimate=pl.CostEstimate(
            flops=2 * slots * features * rows,
            bytes_accessed=4 * features * rows,
            transcendentals=0,
        ),
    )(weights, chosen)


def after(value, *others):
    def kernel(*refs):
        pass

    return pl.pallas_call(
        kernel,
        in_specs=[pl.BlockSpec(memory_space=pl.ANY)] * (1 + len(others)),
        out_specs=pl.BlockSpec(memory_space=pl.ANY),
        out_shape=jax.ShapeDtypeStruct(value.shape, value.dtype),
        input_output_aliases={0: 0},
    )(value, *others)


def shards(tokens, gate_train, up_train, down_train, gain, routes, route_weights):
    tp_count = lax.axis_size("tp")
    experts = gate_train.shape[0]
    slices = tp_count // experts
    gain_column = gain[None, :, None]
    up_round = (up_train * gain_column).astype(jnp.bfloat16)
    down_round = down_train.astype(jnp.bfloat16)

    def exchange(matrix):
        return lax.all_to_all(matrix, "tp", split_axis=0, concat_axis=1, tiled=True)

    gate_all = lax.all_gather(spread(gate_train, gain), "fs", axis=0, tiled=True)
    features = gate_all.shape[0]

    up_moved = exchange(arrange(up_round, tp_count))[0].T
    down_moved = exchange(arrange(down_round, tp_count))[0].T
    units = down_moved.shape[1]
    size = block_of(units) or units
    main = units - size if units > size else units
    both_wide = lax.all_gather(
        jnp.concatenate([up_moved, down_moved[:, :main]], axis=1), "fs", axis=0, tiled=True
    )

    tokens_wide = tokens.astype(jnp.float32)
    normed = (
        tokens_wide
        * lax.rsqrt(jnp.mean(tokens_wide * tokens_wide, axis=1, keepdims=True) + norm_eps)
    ).astype(jnp.bfloat16)
    expert = lax.axis_index("tp") // slices
    matches = routes == expert
    member = jnp.any(matches, axis=1)
    slot_index = jnp.cumsum(member.astype(jnp.int32)) - 1
    marked = jnp.where(member, slot_index, -1)
    picker = (marked[None, :] == jnp.arange(CAP, dtype=jnp.int32)[:, None]).astype(jnp.bfloat16)
    chosen = jnp.dot(picker, normed, preferred_element_type=jnp.float32).astype(jnp.bfloat16)
    contract_last = (((1,), (1,)), ((), ()))

    gate_moved = exchange(gate_all.reshape(features, tp_count, -1).transpose(1, 2, 0))
    gate_new, gate_pre = keep_dot(gate_moved[0], chosen)
    up_new, up_pre = flip_product(both_wide, 0, units, chosen)
    hidden = (jax.nn.silu(gate_pre) * up_pre).astype(jnp.bfloat16)
    down_new, partial_value = flip_dot(both_wide, units, units, hidden[:, :main])
    if main < units:
        rest_moved = after(down_moved[:, main:], gate_new)
        rest_wide = lax.all_gather(rest_moved, "fs", axis=0, tiled=True)
        partial_value = partial_value + lax.dot_general(
            hidden[:, main:], rest_wide, contract_last, preferred_element_type=jnp.float32
        )
        down_new = flip(rest_wide, units, main, down_new)
    partial_value = partial_value.astype(jnp.bfloat16)

    labels = jnp.arange(experts, dtype=jnp.int32)
    member_all = jnp.any(routes[:, :, None] == labels[None, None, :], axis=1)
    slots_all = jnp.cumsum(member_all.astype(jnp.int32), axis=0) - 1
    slot_pair = jnp.take_along_axis(slots_all, routes, axis=1)
    flat_index = slot_pair * experts + routes
    received = lax.all_to_all(
        partial_value.reshape(CAP, tp_count, -1), "tp", split_axis=1, concat_axis=1, tiled=True
    )
    summed = jnp.sum(received.reshape(CAP, experts, slices, -1).astype(jnp.float32), axis=2)
    summed = summed.reshape(CAP * experts, -1)
    picked = jnp.take(summed, flat_index, axis=0)
    mixed = jnp.sum(route_weights[:, :, None] * picked, axis=1)
    return (gate_new[None], up_new[None], down_new[None], mixed.astype(jnp.bfloat16))


def fits(mesh_sizes, train):
    count, tp_count = mesh_sizes
    experts, features, units = train.shape
    return (
        experts == tp_count
        and tp_count & (tp_count - 1) == 0
        and count >= 4
        and count % 2 == 0
        and features % 128 == 64
        and units % 32 == 0
        and units <= features - 64
    )


def main_start(block, features):
    return block * features + (64 if block % 2 else 0)


def gather(trains, gain, near_sources, count, held):
    mats = len(trains)
    tp_count, units, features = trains[0].shape
    wide, half = features - 64, units // 2
    pieces = mats * tp_count
    bits = tp_count.bit_length() - 1
    nears = len(near_sources)
    depth = 3

    def kernel(*refs):
        refs = list(refs)
        take = lambda number: [refs.pop(0) for _ in range(number)]
        train_refs, (gain_ref,), sources = take(mats), take(1), take(nears)
        main, rest, own_main, own_rest, early, last = take(6)
        targets = take(nears)
        raw, cast, cast_rest, load_sem, keep_sem = take(5)
        plane_send, plane_recv, plane_rest_send, plane_rest_recv = take(4)
        line_send, line_recv, line_rest_send, line_rest_recv = take(4)
        near_send, near_recv, pass_hold, pass_load, pass_keep = take(5)
        z = lax.axis_index("fs")
        t = lax.axis_index("tp")

        def peer(p):
            total = 0
            for b in range(bits):
                mine, other = (t // (1 << b)) % 2, (p // (1 << b)) % 2
                total = total + (mine + other - 2 * mine * other) * (1 << b)
            return total

        def plane(m, p):
            e = peer(p)
            return pltpu.make_async_remote_copy(
                own_main.at[m * tp_count + e], main.at[z, m * tp_count + t], plane_send.at[m, p], plane_recv.at[m, p],
                device_id={"fs": z, "tp": e}, device_id_type=pl.DeviceIdType.MESH,
            )

        def plane_rest(m, p):
            e = peer(p)
            return pltpu.make_async_remote_copy(
                own_rest.at[m, e], rest.at[z, m, t], plane_rest_send.at[m, p], plane_rest_recv.at[m, p],
                device_id={"fs": z, "tp": e}, device_id_type=pl.DeviceIdType.MESH,
            )

        def line(way, step, i):
            block = z + step if way == 0 else z - step
            target = z - 1 if way == 0 else z + 1
            piece = main.at[block, i // tp_count * tp_count + peer(i % tp_count)]
            return pltpu.make_async_remote_copy(
                piece, piece, line_send.at[way, step], line_recv.at[way, step, i],
                device_id={"fs": target, "tp": t}, device_id_type=pl.DeviceIdType.MESH,
            )

        def line_rest(way, step, m):
            block = z + step if way == 0 else z - step
            target = z - 1 if way == 0 else z + 1
            return pltpu.make_async_remote_copy(
                rest.at[block, m], rest.at[block, m], line_rest_send.at[way, step, m], line_rest_recv.at[way, step, m],
                device_id={"fs": target, "tp": t}, device_id_type=pl.DeviceIdType.MESH,
            )

        def has(way, step):
            return z + step <= count - 1 if way == 0 else z - step >= 0

        def sends(way):
            return z >= 1 if way == 0 else z <= count - 2

        def near(k):
            inward = jnp.where(z == 0, 1, count - 2)
            return pltpu.make_async_remote_copy(
                sources[k], targets[k], near_send.at[k], near_recv.at[k],
                device_id={"fs": inward, "tp": t}, device_id_type=pl.DeviceIdType.MESH,
            )

        def into_end(way, step, m, p, sender):
            if m < mats - 1 or step < count - 3:
                return True
            end = sender == 1 if way == 0 else sender == count - 2
            if step == count - 2:
                return jnp.logical_not(end)
            return jnp.logical_not(end & (peer(p) >= tp_count - held))

        def leaves(way, step, m, p):
            return into_end(way, step, m, p, z)

        def arrives(way, step, m, p):
            return into_end(way, step, m, p, z + 1 if way == 0 else z - 1)

        def load(m, p):
            slot = (m * tp_count + p) % depth
            return pltpu.make_async_copy(train_refs[m].at[peer(p)], raw.at[slot], load_sem.at[slot])

        def keep(m, p, own):
            slot, place = (m * tp_count + p) % depth, m * tp_count + peer(p)
            goal, goal_rest = (main.at[z], rest.at[z, m]) if own else (own_main, own_rest.at[m])
            return (
                pltpu.make_async_copy(cast.at[slot], goal.at[place], keep_sem.at[0, slot]),
                pltpu.make_async_copy(cast_rest.at[slot], goal_rest.at[peer(p)], keep_sem.at[1, slot]),
            )

        def load_ahead(m, p):
            if m < mats:
                load(m, p).start()

        def convert(m, p, own):
            slot = (m * tp_count + p) % depth
            load(m, p).wait()

            def put(odd):
                value = raw[slot]
                if m < mats - 1:
                    value = value * gain_ref[...]
                value = value.astype(cast.dtype)
                if odd:
                    cast[slot], end = value[:, 64:], value[:, :64]
                else:
                    cast[slot], end = value[:, :wide], value[:, wide:]
                cast_rest[slot] = jnp.concatenate([end[:half], end[half:]], axis=1)

            pl.when(z % 2 == 0)(lambda: put(False))
            pl.when(z % 2 == 1)(lambda: put(True))
            for copy in keep(m, p, own):
                copy.start()

        def finish(m, p, own):
            for copy in keep(m, p, own):
                copy.wait()
            if not own:
                plane(m, p).start()
                plane_rest(m, p).start()

        def forward(step, m, p, first=False):
            i = m * tp_count + p
            if step == 0 and not first:
                plane(m, p).wait_recv()
            for way in range(2):
                if step > 0:
                    @pl.when(has(way, step) & arrives(way, step - 1, m, p))
                    def _(way=way):
                        line(way, step - 1, i).wait_recv()
                if step < count - 1:
                    @pl.when(has(way, step) & sends(way) & leaves(way, step, m, p))
                    def _(way=way):
                        line(way, step, i).start()

        def forward_rest(step, m):
            if step == 0:
                @pl.loop(1, tp_count)
                def _(p):
                    plane_rest(m, p).wait_recv()
            for way in range(2):
                if step > 0:
                    @pl.when(has(way, step))
                    def _(way=way):
                        line_rest(way, step - 1, m).wait_recv()
                if step < count - 1:
                    @pl.when(has(way, step) & sends(way))
                    def _(way=way):
                        line_rest(way, step, m).start()

        barrier = pltpu.get_barrier_semaphore()
        for p in range(1, tp_count):
            pl.semaphore_signal(
                barrier, inc=1, device_id={"fs": z, "tp": peer(p)}, device_id_type=pl.DeviceIdType.MESH
            )

        @pl.when(z >= 1)
        def _():
            pl.semaphore_signal(
                barrier, inc=1, device_id={"fs": z - 1, "tp": t}, device_id_type=pl.DeviceIdType.MESH
            )

        @pl.when(z <= count - 2)
        def _():
            pl.semaphore_signal(
                barrier, inc=1, device_id={"fs": z + 1, "tp": t}, device_id_type=pl.DeviceIdType.MESH
            )

        for p in range(depth):
            load(0, p).start()
        for m in range(mats):
            convert(m, 0, True)
            load_ahead(m, depth)
            if m == 0:
                middle = jnp.logical_and(z >= 1, z <= count - 2)
                pl.semaphore_wait(barrier, tp_count + jnp.where(middle, 1, 0))
                finish(0, 0, True)
                forward(0, 0, 0, first=True)
            else:
                finish(m - 1, tp_count - 1, False)
                if m > 1:
                    forward(0, m - 1, 0, first=True)

            @pl.loop(1, tp_count)
            def _(p, m=m):
                convert(m, p, False)
                pl.when(p + depth < tp_count)(lambda: load(m, p + depth).start())
                if m + 1 < mats:
                    pl.when(p + depth >= tp_count)(lambda: load(m + 1, p + depth - tp_count).start())
                if m == 0:
                    pl.when(p >= 2)(lambda: finish(m, p - 1, False))
                else:
                    pl.when(p == 1)(lambda: finish(m, 0, True))
                    pl.when(p >= 2)(lambda: finish(m, p - 1, False))
                    forward(0, m - 1, p)

            if m > 0:
                forward_rest(0, m - 1)
        finish(mats - 1, tp_count - 1, False)
        forward(0, mats - 1, 0, first=True)

        @pl.loop(1, tp_count)
        def _(p):
            forward(0, mats - 1, p)

        forward_rest(0, mats - 1)

        @pl.when((z == 0) | (z == count - 1))
        def _():
            for k in range(nears):
                near(k).start()

        for step in range(1, count):
            for m in range(mats):
                @pl.loop(0, tp_count)
                def _(p, step=step, m=m):
                    forward(step, m, p)

                forward_rest(step, m)

        @pl.when((z == 1) | (z == count - 2))
        def _():
            low = z < count // 2
            far, after_far = jnp.where(low, count - 1, 0), jnp.where(low, count - 2, 1)
            first = pieces - held
            found = [main.at[far, pieces - tp_count + i] for i in range(tp_count)]
            found += [main.at[after_far, first + i] for i in range(held)]
            goal = [early.at[i] for i in range(tp_count + held - 1)] + [last.at[0]]
            loads = [pltpu.make_async_copy(f, pass_hold.at[i], pass_load.at[i]) for i, f in enumerate(found)]
            keeps = [pltpu.make_async_copy(pass_hold.at[i], g, pass_keep.at[i]) for i, g in enumerate(goal)]
            for load in loads:
                load.start()
            for load, keep in zip(loads, keeps):
                load.wait()
                keep.start()
            for keep in keeps:
                keep.wait()

        for m in range(mats):
            @pl.loop(1, tp_count)
            def _(p, m=m):
                plane(m, p).wait_send()
                plane_rest(m, p).wait_send()

        @pl.when((z == 0) | (z == count - 1))
        def _():
            for k in range(nears):
                near(k).wait_send()

        @pl.when((z == 1) | (z == count - 2))
        def _():
            for k in range(nears):
                near(k).wait_recv()

        for step in range(count - 1):
            for way in range(2):
                @pl.when(has(way, step) & sends(way))
                def _(way=way, step=step):
                    end = z == (1 if way == 0 else count - 2)

                    def settle(number, way=way, step=step):
                        sent = main.at[z, pl.ds(0, number)]
                        pltpu.make_async_copy(sent, sent, line_send.at[way, step]).wait()

                    if step == count - 2:
                        settle(pieces - tp_count)
                    elif step == count - 3:
                        pl.when(end)(lambda: settle(pieces - held))
                        pl.when(jnp.logical_not(end))(lambda: settle(pieces))
                    else:
                        settle(pieces)
                    for m in range(mats):
                        line_rest(way, step, m).wait_send()

    dma = pltpu.SemaphoreType.DMA
    dtype = jnp.bfloat16
    own = pieces * units * features
    anywhere = pl.BlockSpec(memory_space=pl.ANY)
    outs = [
        (count, pieces, units, wide),
        (count, mats, tp_count, half, 128),
        (pieces, units, wide),
        (mats, tp_count, half, 128),
        (tp_count + held - 1, units, wide),
        (1, units, wide),
    ]
    return pl.pallas_call(
        kernel,
        in_specs=[anywhere] * mats + [pl.BlockSpec(memory_space=pltpu.VMEM)] + [anywhere] * nears,
        out_specs=[anywhere] * (len(outs) + nears),
        out_shape=[jax.ShapeDtypeStruct(shape, dtype) for shape in outs]
        + [jax.ShapeDtypeStruct(source.shape, source.dtype) for source in near_sources],
        scratch_shapes=[
            pltpu.VMEM((depth, units, features), jnp.float32),
            pltpu.VMEM((depth, units, wide), dtype),
            pltpu.VMEM((depth, half, 128), dtype),
            dma((depth,)),
            dma((2, depth)),
            dma((mats, tp_count)),
            dma((mats, tp_count)),
            dma((mats, tp_count)),
            dma((mats, tp_count)),
            dma((2, count - 1)),
            dma((2, count - 1, pieces)),
            dma((2, count - 1, mats)),
            dma((2, count - 1, mats)),
            dma((nears,)),
            dma((nears,)),
            pltpu.VMEM((tp_count + held, units, wide), dtype),
            dma((tp_count + held,)),
            dma((tp_count + held,)),
        ],
        compiler_params=pltpu.CompilerParams(collective_id=0, has_side_effects=True),
        cost_estimate=pl.CostEstimate(
            flops=1000 * own, bytes_accessed=4 * (count + 3) * own, transcendentals=0
        ),
    )(*trains, gain, *near_sources)


def joined(main_ref, rest_ref, out_ref):
    count, _, units, wide = main_ref.shape
    features = wide + 64
    half = units // 2
    for block in range(count):
        out_ref[:, pl.ds(main_start(block, features), wide)] = main_ref[block, 0]
    for block in range(0, count, 2):
        first, second = rest_ref[block, 0, 0], rest_ref[block + 1, 0, 0]
        place = pl.ds(block * features + wide, 128)
        out_ref[:half, place] = jnp.concatenate([first[:, :64], second[:, :64]], axis=1)
        out_ref[half:, place] = jnp.concatenate([first[:, 64:], second[:, 64:]], axis=1)


def join_call(main, rest, which, kernel, operand, operand_spec, product_spec, product_shape):
    count, _, tp_count, half = rest.shape[:4]
    units, wide = main.shape[2:]
    features = count * (wide + 64)
    return pl.pallas_call(
        kernel,
        grid=(tp_count,),
        in_specs=[
            pl.BlockSpec((count, 1, units, wide), lambda i: (0, which * tp_count + i, 0, 0)),
            pl.BlockSpec((count, 1, 1, half, 128), lambda i: (0, which, i, 0, 0)),
            operand_spec,
        ],
        out_specs=[pl.BlockSpec((units, features), lambda i: (i, 0)), product_spec],
        out_shape=[
            jax.ShapeDtypeStruct((tp_count * units, features), main.dtype),
            jax.ShapeDtypeStruct(product_shape, jnp.float32),
        ],
        cost_estimate=pl.CostEstimate(
            flops=1000 * tp_count * units * features,
            bytes_accessed=4 * tp_count * units * features,
            transcendentals=0,
        ),
    )(main, rest, operand)


def join_in(main, rest, which, chosen):
    tp_count, units = rest.shape[2], main.shape[2]
    slots, features = chosen.shape

    def kernel(main_ref, rest_ref, chosen_ref, new_ref, product_ref):
        joined(main_ref, rest_ref, new_ref)
        product_ref[0] = lax.dot_general(
            chosen_ref[...], new_ref[...], (((1,), (1,)), ((), ())), preferred_element_type=jnp.float32
        )

    return join_call(
        main, rest, which, kernel, chosen,
        pl.BlockSpec((slots, features), lambda i: (0, 0)),
        pl.BlockSpec((1, slots, units), lambda i: (i, 0, 0)),
        (tp_count, slots, units),
    )


def join_out(main, rest, which, hidden):
    _, slots, units = hidden.shape
    features = main.shape[0] * (main.shape[3] + 64)

    def kernel(main_ref, rest_ref, hidden_ref, new_ref, total_ref):
        joined(main_ref, rest_ref, new_ref)

        @pl.when(pl.program_id(0) == 0)
        def _():
            total_ref[...] = jnp.zeros_like(total_ref)

        total_ref[...] += jnp.dot(hidden_ref[0], new_ref[...], preferred_element_type=jnp.float32)

    return join_call(
        main, rest, which, kernel, hidden,
        pl.BlockSpec((1, slots, units), lambda i: (i, 0, 0)),
        pl.BlockSpec((slots, features), lambda i: (0, 0)),
        (slots, features),
    )


def place_late(arrived, places, base, count):
    pieces, units, wide = arrived.shape
    start = jnp.stack([column for _, _, column in places])

    def kernel(start_ref, arrived_ref, base_ref, new_ref, hold, load_sem, keep_sem):
        z = lax.axis_index("fs")

        @pl.when((z == 0) | (z == count - 1))
        def _():
            loads = [pltpu.make_async_copy(arrived_ref.at[i], hold.at[i], load_sem.at[i]) for i in range(pieces)]
            keeps = [
                pltpu.make_async_copy(
                    hold.at[i],
                    new_ref.at[
                        pl.ds(row * units, units), pl.ds(pl.multiple_of(start_ref[i], 128), wide)
                    ],
                    keep_sem.at[i],
                )
                for i, row, _ in places
            ]
            for load in loads:
                load.start()
            for load, keep in zip(loads, keeps):
                load.wait()
                keep.start()
            for keep in keeps:
                keep.wait()

    return pl.pallas_call(
        kernel,
        grid_spec=pltpu.PrefetchScalarGridSpec(
            num_scalar_prefetch=1,
            grid=(1,),
            in_specs=[pl.BlockSpec(memory_space=pl.ANY)] * 2,
            out_specs=pl.BlockSpec(memory_space=pl.ANY),
            scratch_shapes=[
                pltpu.VMEM(arrived.shape, arrived.dtype),
                pltpu.SemaphoreType.DMA((pieces,)),
                pltpu.SemaphoreType.DMA((pieces,)),
            ],
        ),
        out_shape=jax.ShapeDtypeStruct(base.shape, base.dtype),
        input_output_aliases={2: 0},
        cost_estimate=pl.CostEstimate(
            flops=500 * arrived.size, bytes_accessed=4 * arrived.size, transcendentals=0
        ),
    )(start, arrived, base)


def pick(tokens, routes, expert):
    tokens_wide = tokens.astype(jnp.float32)
    normed = (
        tokens_wide
        * lax.rsqrt(jnp.mean(tokens_wide * tokens_wide, axis=2, keepdims=True) + norm_eps)
    ).astype(jnp.bfloat16)
    member = jnp.any(routes == expert, axis=2)
    slot_index = jnp.cumsum(member.astype(jnp.int32), axis=1) - 1
    marked = jnp.where(member, slot_index, -1)
    picker = (marked[:, None, :] == jnp.arange(CAP, dtype=jnp.int32)[None, :, None]).astype(jnp.bfloat16)
    chosen = jnp.einsum("gcr,grd->gcd", picker, normed, preferred_element_type=jnp.float32)
    return chosen.astype(jnp.bfloat16).reshape(-1, tokens.shape[2])


def mix(partial_value, routes, route_weights, experts):
    tp_count = lax.axis_size("tp")
    groups = routes.shape[0]
    labels = jnp.arange(experts, dtype=jnp.int32)
    member_all = jnp.any(routes[:, :, :, None] == labels, axis=2)
    slots_all = jnp.cumsum(member_all.astype(jnp.int32), axis=1) - 1
    slot_pair = jnp.take_along_axis(slots_all, routes, axis=2)
    first = CAP * jnp.arange(groups, dtype=jnp.int32)[:, None, None]
    flat_index = (first + slot_pair) * experts + routes
    received = lax.all_to_all(
        partial_value.reshape(groups * CAP, tp_count, -1), "tp", split_axis=1, concat_axis=1, tiled=True
    )
    summed = received.astype(jnp.float32).reshape(groups * CAP * experts, -1)
    picked = jnp.take(summed, flat_index, axis=0)
    return jnp.sum(route_weights[:, :, :, None] * picked, axis=2).astype(jnp.bfloat16)


def line_shards(tokens, gate_train, up_train, down_train, gain, routes, route_weights):
    count = lax.axis_size("fs")
    place = lax.axis_index("fs")
    experts, features, _ = gate_train.shape
    held = experts - 1
    outward = [(1, 0), (count - 2, count - 1)]
    near_sources = (tokens, routes.T, route_weights.T)
    main, rest, _, _, kept_early, kept_last, *near = gather(
        [train.transpose(0, 2, 1) for train in (gate_train, up_train, down_train)],
        gain[None, :], near_sources, count, held,
    )
    low = place < count // 2
    far_start = jnp.where(low, main_start(count - 1, features), main_start(0, features)).astype(jnp.int32)
    next_start = jnp.where(low, main_start(count - 2, features), main_start(1, features)).astype(jnp.int32)
    arrived_early = lax.ppermute(kept_early, "fs", outward)

    main, rest, near, near_sources = lax.optimization_barrier((main, rest, near, near_sources))
    both_tokens, both_routes, both_weights = [jnp.stack(pair) for pair in zip(near_sources, near)]
    both_routes, both_weights = both_routes.transpose(0, 2, 1), both_weights.transpose(0, 2, 1)
    chosen = pick(both_tokens, both_routes, lax.axis_index("tp"))
    gate_new, gate_pre = join_in(main, rest, 0, chosen)
    up_new, up_pre = join_in(main, rest, 1, chosen)
    hidden = (jax.nn.silu(gate_pre) * up_pre).astype(jnp.bfloat16)
    down_new, total = join_out(main, rest, 2, hidden)
    both_mixed = mix(total.astype(jnp.bfloat16), both_routes, both_weights, experts)
    wide = kept_last.shape[2]
    kept_rows = kept_last.reshape(-1, wide)
    mixed_rows = jnp.pad(both_mixed[1], ((0, 0), (0, wide - both_mixed.shape[2])))
    arrived_rows = lax.ppermute(jnp.concatenate([kept_rows, mixed_rows]), "fs", outward)
    arrived_last = arrived_rows[: kept_rows.shape[0]].reshape(kept_last.shape)
    near_mixed = arrived_rows[kept_rows.shape[0] :, : both_mixed.shape[2]]
    first = experts - held
    early = [(i, i, far_start) for i in range(experts)]
    early += [(experts + i, first + i, next_start) for i in range(held - 1)]
    down_new = place_late(arrived_early, early, down_new, count)
    down_new = place_late(arrived_last, [(0, experts - 1, next_start)], down_new, count)
    at_end = (place == 0) | (place == count - 1)
    mixed = jnp.where(at_end, near_mixed, both_mixed[0])
    return (gate_new[None], up_new[None], down_new[None], mixed)


def solution(mesh):
    sizes = (mesh.shape["fs"], mesh.shape["tp"])

    def step(*args):
        if not fits(sizes, args[1]):
            return shards(*args)
        return line_shards(*args)

    in_specs = (
        P("fs", None),
        P(None, "fs", "tp"),
        P(None, "fs", "tp"),
        P(None, "fs", "tp"),
        P("fs"),
        P("fs", None),
        P("fs", None),
    )
    out_specs = (P("tp", None, None), P("tp", None, None), P("tp", None, None), P("fs", "tp"))
    return jax.shard_map(step, mesh=mesh, in_specs=in_specs, out_specs=out_specs, check_vma=False)
```

```python
import jax
import jax.numpy as jnp
from jax import lax
from jax.experimental import pallas as pl
from jax.experimental.pallas import tpu as pltpu
from jax.sharding import PartitionSpec as P


CAP = 72


norm_eps = 1e-06


def arrange(matrix, tp_count):
    experts, row_count, col_count = matrix.shape
    slices = tp_count // experts
    piece_width = col_count // slices
    shaped = matrix.reshape(experts, row_count, slices, piece_width)
    return shaped.transpose(0, 2, 3, 1).reshape(tp_count, piece_width, row_count)


def block_of(*counts):
    for size in (256, 128):
        if all(count % size == 0 for count in counts):
            return size
    return None


def flip(wide, total_rows, first_row, base=None):
    features, rows = wide.shape
    size = block_of(rows, first_row, total_rows) or rows
    first = first_row // size

    def kernel(*refs):
        refs[-1][...] = refs[0][...].T

    in_specs = [pl.BlockSpec((features, size), lambda i: (0, i))]
    operands = [wide]
    aliases = {}
    if base is not None:
        in_specs.append(pl.BlockSpec(memory_space=pl.ANY))
        operands.append(base)
        aliases = {1: 0}
    return pl.pallas_call(
        kernel,
        grid=(rows // size,),
        in_specs=in_specs,
        out_specs=pl.BlockSpec((size, features), lambda i: (first + i, 0)),
        out_shape=jax.ShapeDtypeStruct((total_rows, features), wide.dtype),
        input_output_aliases=aliases,
        cost_estimate=pl.CostEstimate(
            flops=0, bytes_accessed=4 * features * rows, transcendentals=0
        ),
    )(*operands)


def columns(wide, first, count, *others):
    size = block_of(first, count, *others)
    if size is None:
        return lax.slice_in_dim(wide, first, first + count, axis=1), count, 0
    return wide, size, first // size


def flip_product(wide, first, rows, chosen):
    features = wide.shape[0]
    wide, size, start = columns(wide, first, rows)
    slots = chosen.shape[0]

    def kernel(wide_ref, chosen_ref, rows_ref, product_ref):
        value = wide_ref[...]
        rows_ref[...] = value.T
        product_ref[...] = jnp.dot(chosen_ref[...], value, preferred_element_type=jnp.float32)

    return pl.pallas_call(
        kernel,
        grid=(rows // size,),
        in_specs=[
            pl.BlockSpec((features, size), lambda i: (0, start + i)),
            pl.BlockSpec((slots, features), lambda i: (0, 0)),
        ],
        out_specs=[
            pl.BlockSpec((size, features), lambda i: (i, 0)),
            pl.BlockSpec((slots, size), lambda i: (0, i)),
        ],
        out_shape=[
            jax.ShapeDtypeStruct((rows, features), wide.dtype),
            jax.ShapeDtypeStruct((slots, rows), jnp.float32),
        ],
        cost_estimate=pl.CostEstimate(
            flops=2 * slots * features * rows,
            bytes_accessed=4 * features * rows,
            transcendentals=0,
        ),
    )(wide, chosen)


def spread(train, gain):
    experts, features, count = train.shape
    rows = experts * count
    size = block_of(rows) or rows

    def kernel(train_ref, gain_ref, out_ref):
        out_ref[...] = (train_ref[...] * gain_ref[...]).astype(jnp.bfloat16).T

    return pl.pallas_call(
        kernel,
        grid=(rows // size,),
        in_specs=[
            pl.BlockSpec((size, features), lambda i: (i, 0)),
            pl.BlockSpec((1, features), lambda i: (0, 0)),
        ],
        out_specs=pl.BlockSpec((features, size), lambda i: (0, i)),
        out_shape=jax.ShapeDtypeStruct((features, rows), jnp.bfloat16),
        cost_estimate=pl.CostEstimate(
            flops=train.size, bytes_accessed=6 * train.size, transcendentals=0
        ),
    )(train.transpose(0, 2, 1).reshape(rows, features), gain[None, :])


def flip_dot(wide, first, total_rows, hidden):
    features = wide.shape[0]
    slots, rows = hidden.shape
    wide, size, start = columns(wide, first, rows, total_rows)

    def kernel(wide_ref, hidden_ref, rows_ref, total_ref):
        turned = wide_ref[...].T
        rows_ref[...] = turned

        @pl.when(pl.program_id(0) == 0)
        def _():
            total_ref[...] = jnp.zeros_like(total_ref)

        total_ref[...] += jnp.dot(hidden_ref[...], turned, preferred_element_type=jnp.float32)

    return pl.pallas_call(
        kernel,
        grid=(rows // size,),
        in_specs=[
            pl.BlockSpec((features, size), lambda i: (0, start + i)),
            pl.BlockSpec((slots, size), lambda i: (0, i)),
        ],
        out_specs=[
            pl.BlockSpec((size, features), lambda i: (i, 0)),
            pl.BlockSpec((slots, features), lambda i: (0, 0)),
        ],
        out_shape=[
            jax.ShapeDtypeStruct((total_rows, features), wide.dtype),
            jax.ShapeDtypeStruct((slots, features), jnp.float32),
        ],
        cost_estimate=pl.CostEstimate(
            flops=2 * slots * features * rows,
            bytes_accessed=4 * features * rows,
            transcendentals=0,
        ),
    )(wide, hidden)


def keep_dot(weights, chosen):
    rows, features = weights.shape
    size = block_of(rows) or rows
    slots = chosen.shape[0]

    def kernel(weights_ref, chosen_ref, rows_ref, product_ref):
        rows_ref[...] = weights_ref[...]
        product_ref[...] = lax.dot_general(
            chosen_ref[...],
            weights_ref[...],
            (((1,), (1,)), ((), ())),
            preferred_element_type=jnp.float32,
        )

    return pl.pallas_call(
        kernel,
        grid=(rows // size,),
        in_specs=[
            pl.BlockSpec((size, features), lambda i: (i, 0)),
            pl.BlockSpec((slots, features), lambda i: (0, 0)),
        ],
        out_specs=[
            pl.BlockSpec((size, features), lambda i: (i, 0)),
            pl.BlockSpec((slots, size), lambda i: (0, i)),
        ],
        out_shape=[
            jax.ShapeDtypeStruct((rows, features), weights.dtype),
            jax.ShapeDtypeStruct((slots, rows), jnp.float32),
        ],
        cost_estimate=pl.CostEstimate(
            flops=2 * slots * features * rows,
            bytes_accessed=4 * features * rows,
            transcendentals=0,
        ),
    )(weights, chosen)


def after(value, *others):
    def kernel(*refs):
        pass

    return pl.pallas_call(
        kernel,
        in_specs=[pl.BlockSpec(memory_space=pl.ANY)] * (1 + len(others)),
        out_specs=pl.BlockSpec(memory_space=pl.ANY),
        out_shape=jax.ShapeDtypeStruct(value.shape, value.dtype),
        input_output_aliases={0: 0},
    )(value, *others)


def shards(tokens, gate_train, up_train, down_train, gain, routes, route_weights):
    tp_count = lax.axis_size("tp")
    experts = gate_train.shape[0]
    slices = tp_count // experts
    gain_column = gain[None, :, None]
    up_round = (up_train * gain_column).astype(jnp.bfloat16)
    down_round = down_train.astype(jnp.bfloat16)

    def exchange(matrix):
        return lax.all_to_all(matrix, "tp", split_axis=0, concat_axis=1, tiled=True)

    gate_all = lax.all_gather(spread(gate_train, gain), "fs", axis=0, tiled=True)
    features = gate_all.shape[0]

    up_moved = exchange(arrange(up_round, tp_count))[0].T
    down_moved = exchange(arrange(down_round, tp_count))[0].T
    units = down_moved.shape[1]
    size = block_of(units) or units
    main = units - size if units > size else units
    both_wide = lax.all_gather(
        jnp.concatenate([up_moved, down_moved[:, :main]], axis=1), "fs", axis=0, tiled=True
    )

    tokens_wide = tokens.astype(jnp.float32)
    normed = (
        tokens_wide
        * lax.rsqrt(jnp.mean(tokens_wide * tokens_wide, axis=1, keepdims=True) + norm_eps)
    ).astype(jnp.bfloat16)
    expert = lax.axis_index("tp") // slices
    matches = routes == expert
    member = jnp.any(matches, axis=1)
    slot_index = jnp.cumsum(member.astype(jnp.int32)) - 1
    marked = jnp.where(member, slot_index, -1)
    picker = (marked[None, :] == jnp.arange(CAP, dtype=jnp.int32)[:, None]).astype(jnp.bfloat16)
    chosen = jnp.dot(picker, normed, preferred_element_type=jnp.float32).astype(jnp.bfloat16)
    contract_last = (((1,), (1,)), ((), ()))

    gate_moved = exchange(gate_all.reshape(features, tp_count, -1).transpose(1, 2, 0))
    gate_new, gate_pre = keep_dot(gate_moved[0], chosen)
    up_new, up_pre = flip_product(both_wide, 0, units, chosen)
    hidden = (jax.nn.silu(gate_pre) * up_pre).astype(jnp.bfloat16)
    down_new, partial_value = flip_dot(both_wide, units, units, hidden[:, :main])
    if main < units:
        rest_moved = after(down_moved[:, main:], gate_new)
        rest_wide = lax.all_gather(rest_moved, "fs", axis=0, tiled=True)
        partial_value = partial_value + lax.dot_general(
            hidden[:, main:], rest_wide, contract_last, preferred_element_type=jnp.float32
        )
        down_new = flip(rest_wide, units, main, down_new)
    partial_value = partial_value.astype(jnp.bfloat16)

    labels = jnp.arange(experts, dtype=jnp.int32)
    member_all = jnp.any(routes[:, :, None] == labels[None, None, :], axis=1)
    slots_all = jnp.cumsum(member_all.astype(jnp.int32), axis=0) - 1
    slot_pair = jnp.take_along_axis(slots_all, routes, axis=1)
    flat_index = slot_pair * experts + routes
    received = lax.all_to_all(
        partial_value.reshape(CAP, tp_count, -1), "tp", split_axis=1, concat_axis=1, tiled=True
    )
    summed = jnp.sum(received.reshape(CAP, experts, slices, -1).astype(jnp.float32), axis=2)
    summed = summed.reshape(CAP * experts, -1)
    picked = jnp.take(summed, flat_index, axis=0)
    mixed = jnp.sum(route_weights[:, :, None] * picked, axis=1)
    return (gate_new[None], up_new[None], down_new[None], mixed.astype(jnp.bfloat16))


def fits(mesh_sizes, train):
    count, tp_count = mesh_sizes
    experts, features, units = train.shape
    return (
        experts == tp_count
        and tp_count & (tp_count - 1) == 0
        and count >= 4
        and count % 2 == 0
        and features % 128 == 64
        and units % 32 == 0
        and units <= features - 64
    )


def main_start(block, features):
    return block * features + (64 if block % 2 else 0)


def gather(trains, gain, near_sources, count, held):
    mats = len(trains)
    tp_count, units, features = trains[0].shape
    wide, half = features - 64, units // 2
    pieces = mats * tp_count
    bits = tp_count.bit_length() - 1
    nears = len(near_sources)
    depth = 3

    def kernel(*refs):
        refs = list(refs)
        take = lambda number: [refs.pop(0) for _ in range(number)]
        train_refs, (gain_ref,), sources = take(mats), take(1), take(nears)
        main, rest, own_main, own_rest, early, last = take(6)
        targets = take(nears)
        raw, cast, cast_rest, load_sem, keep_sem = take(5)
        plane_send, plane_recv, plane_rest_send, plane_rest_recv = take(4)
        line_send, line_recv, line_rest_send, line_rest_recv = take(4)
        near_send, near_recv, pass_hold, pass_load, pass_keep = take(5)
        z = lax.axis_index("fs")
        t = lax.axis_index("tp")

        def peer(p):
            total = 0
            for b in range(bits):
                mine, other = (t // (1 << b)) % 2, (p // (1 << b)) % 2
                total = total + (mine + other - 2 * mine * other) * (1 << b)
            return total

        def plane(m, p):
            e = peer(p)
            return pltpu.make_async_remote_copy(
                own_main.at[m * tp_count + e], main.at[z, m * tp_count + t], plane_send.at[m, p], plane_recv.at[m, p],
                device_id={"fs": z, "tp": e}, device_id_type=pl.DeviceIdType.MESH,
            )

        def plane_rest(m, p):
            e = peer(p)
            return pltpu.make_async_remote_copy(
                own_rest.at[m, e], rest.at[z, m, t], plane_rest_send.at[m, p], plane_rest_recv.at[m, p],
                device_id={"fs": z, "tp": e}, device_id_type=pl.DeviceIdType.MESH,
            )

        def line(way, step, i):
            block = z + step if way == 0 else z - step
            target = z - 1 if way == 0 else z + 1
            piece = main.at[block, i // tp_count * tp_count + peer(i % tp_count)]
            return pltpu.make_async_remote_copy(
                piece, piece, line_send.at[way, step], line_recv.at[way, step, i],
                device_id={"fs": target, "tp": t}, device_id_type=pl.DeviceIdType.MESH,
            )

        def line_rest(way, step, m):
            block = z + step if way == 0 else z - step
            target = z - 1 if way == 0 else z + 1
            return pltpu.make_async_remote_copy(
                rest.at[block, m], rest.at[block, m], line_rest_send.at[way, step, m], line_rest_recv.at[way, step, m],
                device_id={"fs": target, "tp": t}, device_id_type=pl.DeviceIdType.MESH,
            )

        def has(way, step):
            return z + step <= count - 1 if way == 0 else z - step >= 0

        def sends(way):
            return z >= 1 if way == 0 else z <= count - 2

        def near(k):
            inward = jnp.where(z == 0, 1, count - 2)
            return pltpu.make_async_remote_copy(
                sources[k], targets[k], near_send.at[k], near_recv.at[k],
                device_id={"fs": inward, "tp": t}, device_id_type=pl.DeviceIdType.MESH,
            )

        def into_end(way, step, m, p, sender):
            if m < mats - 1 or step < count - 3:
                return True
            end = sender == 1 if way == 0 else sender == count - 2
            if step == count - 2:
                return jnp.logical_not(end)
            return jnp.logical_not(end & (peer(p) >= tp_count - held))

        def leaves(way, step, m, p):
            return into_end(way, step, m, p, z)

        def arrives(way, step, m, p):
            return into_end(way, step, m, p, z + 1 if way == 0 else z - 1)

        def load(m, p):
            slot = (m * tp_count + p) % depth
            return pltpu.make_async_copy(train_refs[m].at[peer(p)], raw.at[slot], load_sem.at[slot])

        def keep(m, p, own):
            slot, place = (m * tp_count + p) % depth, m * tp_count + peer(p)
            goal, goal_rest = (main.at[z], rest.at[z, m]) if own else (own_main, own_rest.at[m])
            return (
                pltpu.make_async_copy(cast.at[slot], goal.at[place], keep_sem.at[0, slot]),
                pltpu.make_async_copy(cast_rest.at[slot], goal_rest.at[peer(p)], keep_sem.at[1, slot]),
            )

        def load_ahead(m, p):
            if m < mats:
                load(m, p).start()

        def convert(m, p, own):
            slot = (m * tp_count + p) % depth
            load(m, p).wait()

            def put(odd):
                value = raw[slot]
                if m < mats - 1:
                    value = value * gain_ref[...].reshape(1, features)
                value = value.astype(cast.dtype)
                if odd:
                    cast[slot], end = value[:, 64:], value[:, :64]
                else:
                    cast[slot], end = value[:, :wide], value[:, wide:]
                cast_rest[slot] = jnp.concatenate([end[:half], end[half:]], axis=1)

            pl.when(z % 2 == 0)(lambda: put(False))
            pl.when(z % 2 == 1)(lambda: put(True))
            for copy in keep(m, p, own):
                copy.start()

        def finish(m, p, own):
            for copy in keep(m, p, own):
                copy.wait()
            if not own:
                plane(m, p).start()
                plane_rest(m, p).start()

        def forward(step, m, p, first=False):
            i = m * tp_count + p
            if step == 0 and not first:
                plane(m, p).wait_recv()
            for way in range(2):
                if step > 0:
                    @pl.when(has(way, step) & arrives(way, step - 1, m, p))
                    def _(way=way):
                        line(way, step - 1, i).wait_recv()
                if step < count - 1:
                    @pl.when(has(way, step) & sends(way) & leaves(way, step, m, p))
                    def _(way=way):
                        line(way, step, i).start()

        def forward_rest(step, m):
            if step == 0:
                @pl.loop(1, tp_count)
                def _(p):
                    plane_rest(m, p).wait_recv()
            for way in range(2):
                if step > 0:
                    @pl.when(has(way, step))
                    def _(way=way):
                        line_rest(way, step - 1, m).wait_recv()
                if step < count - 1:
                    @pl.when(has(way, step) & sends(way))
                    def _(way=way):
                        line_rest(way, step, m).start()

        barrier = pltpu.get_barrier_semaphore()
        for p in range(1, tp_count):
            pl.semaphore_signal(
                barrier, inc=1, device_id={"fs": z, "tp": peer(p)}, device_id_type=pl.DeviceIdType.MESH
            )

        @pl.when(z >= 1)
        def _():
            pl.semaphore_signal(
                barrier, inc=1, device_id={"fs": z - 1, "tp": t}, device_id_type=pl.DeviceIdType.MESH
            )

        @pl.when(z <= count - 2)
        def _():
            pl.semaphore_signal(
                barrier, inc=1, device_id={"fs": z + 1, "tp": t}, device_id_type=pl.DeviceIdType.MESH
            )

        for p in range(depth):
            load(0, p).start()
        for m in range(mats):
            convert(m, 0, True)
            load_ahead(m, depth)
            if m == 0:
                middle = jnp.logical_and(z >= 1, z <= count - 2)
                pl.semaphore_wait(barrier, tp_count + jnp.where(middle, 1, 0))
                finish(0, 0, True)
                forward(0, 0, 0, first=True)
            else:
                finish(m - 1, tp_count - 1, False)
                if m > 1:
                    forward(0, m - 1, 0, first=True)

            @pl.loop(1, tp_count)
            def _(p, m=m):
                convert(m, p, False)
                pl.when(p + depth < tp_count)(lambda: load(m, p + depth).start())
                if m + 1 < mats:
                    pl.when(p + depth >= tp_count)(lambda: load(m + 1, p + depth - tp_count).start())
                if m == 0:
                    pl.when(p >= 2)(lambda: finish(m, p - 1, False))
                else:
                    pl.when(p == 1)(lambda: finish(m, 0, True))
                    pl.when(p >= 2)(lambda: finish(m, p - 1, False))
                    forward(0, m - 1, p)

            if m > 0:
                forward_rest(0, m - 1)
        finish(mats - 1, tp_count - 1, False)
        forward(0, mats - 1, 0, first=True)

        @pl.loop(1, tp_count)
        def _(p):
            forward(0, mats - 1, p)

        forward_rest(0, mats - 1)

        @pl.when((z == 0) | (z == count - 1))
        def _():
            for k in range(nears):
                near(k).start()

        for step in range(1, count):
            for m in range(mats):
                @pl.loop(0, tp_count)
                def _(p, step=step, m=m):
                    forward(step, m, p)

                forward_rest(step, m)

        @pl.when((z == 1) | (z == count - 2))
        def _():
            low = z < count // 2
            far, after_far = jnp.where(low, count - 1, 0), jnp.where(low, count - 2, 1)
            first = pieces - held
            found = [main.at[far, pieces - tp_count + i] for i in range(tp_count)]
            found += [main.at[after_far, first + i] for i in range(held)]
            goal = [early.at[i] for i in range(tp_count + held - 1)] + [last.at[0]]
            loads = [pltpu.make_async_copy(f, pass_hold.at[i], pass_load.at[i]) for i, f in enumerate(found)]
            keeps = [pltpu.make_async_copy(pass_hold.at[i], g, pass_keep.at[i]) for i, g in enumerate(goal)]
            for load in loads:
                load.start()
            for load, keep in zip(loads, keeps):
                load.wait()
                keep.start()
            for keep in keeps:
                keep.wait()

        for m in range(mats):
            @pl.loop(1, tp_count)
            def _(p, m=m):
                plane(m, p).wait_send()
                plane_rest(m, p).wait_send()

        @pl.when((z == 0) | (z == count - 1))
        def _():
            for k in range(nears):
                near(k).wait_send()

        @pl.when((z == 1) | (z == count - 2))
        def _():
            for k in range(nears):
                near(k).wait_recv()

        for step in range(count - 1):
            for way in range(2):
                @pl.when(has(way, step) & sends(way))
                def _(way=way, step=step):
                    end = z == (1 if way == 0 else count - 2)

                    def settle(number, way=way, step=step):
                        sent = main.at[z, pl.ds(0, number)]
                        pltpu.make_async_copy(sent, sent, line_send.at[way, step]).wait()

                    if step == count - 2:
                        settle(pieces - tp_count)
                    elif step == count - 3:
                        pl.when(end)(lambda: settle(pieces - held))
                        pl.when(jnp.logical_not(end))(lambda: settle(pieces))
                    else:
                        settle(pieces)
                    for m in range(mats):
                        line_rest(way, step, m).wait_send()

    dma = pltpu.SemaphoreType.DMA
    dtype = jnp.bfloat16
    own = pieces * units * features
    anywhere = pl.BlockSpec(memory_space=pl.ANY)
    outs = [
        (count, pieces, units, wide),
        (count, mats, tp_count, half, 128),
        (pieces, units, wide),
        (mats, tp_count, half, 128),
        (tp_count + held - 1, units, wide),
        (1, units, wide),
    ]
    return pl.pallas_call(
        kernel,
        in_specs=[anywhere] * mats + [pl.BlockSpec(memory_space=pltpu.VMEM)] + [anywhere] * nears,
        out_specs=[anywhere] * (len(outs) + nears),
        out_shape=[jax.ShapeDtypeStruct(shape, dtype) for shape in outs]
        + [jax.ShapeDtypeStruct(source.shape, source.dtype) for source in near_sources],
        scratch_shapes=[
            pltpu.VMEM((depth, units, features), jnp.float32),
            pltpu.VMEM((depth, units, wide), dtype),
            pltpu.VMEM((depth, half, 128), dtype),
            dma((depth,)),
            dma((2, depth)),
            dma((mats, tp_count)),
            dma((mats, tp_count)),
            dma((mats, tp_count)),
            dma((mats, tp_count)),
            dma((2, count - 1)),
            dma((2, count - 1, pieces)),
            dma((2, count - 1, mats)),
            dma((2, count - 1, mats)),
            dma((nears,)),
            dma((nears,)),
            pltpu.VMEM((tp_count + held, units, wide), dtype),
            dma((tp_count + held,)),
            dma((tp_count + held,)),
        ],
        compiler_params=pltpu.CompilerParams(collective_id=0, has_side_effects=True),
        cost_estimate=pl.CostEstimate(
            flops=1000 * own, bytes_accessed=4 * (count + 3) * own, transcendentals=0
        ),
    )(*trains, gain, *near_sources)


def joined(main_ref, rest_ref, out_ref):
    count, _, units, wide = main_ref.shape
    features = wide + 64
    half = units // 2
    for block in range(count):
        out_ref[:, pl.ds(main_start(block, features), wide)] = main_ref[block, 0]
    for block in range(0, count, 2):
        first, second = rest_ref[block, 0, 0], rest_ref[block + 1, 0, 0]
        place = pl.ds(block * features + wide, 128)
        out_ref[:half, place] = jnp.concatenate([first[:, :64], second[:, :64]], axis=1)
        out_ref[half:, place] = jnp.concatenate([first[:, 64:], second[:, 64:]], axis=1)


def join_call(main, rest, which, kernel, operand, operand_spec, product_spec, product_shape):
    count, _, tp_count, half = rest.shape[:4]
    units, wide = main.shape[2:]
    features = count * (wide + 64)
    return pl.pallas_call(
        kernel,
        grid=(tp_count,),
        in_specs=[
            pl.BlockSpec((count, 1, units, wide), lambda i: (0, which * tp_count + i, 0, 0)),
            pl.BlockSpec((count, 1, 1, half, 128), lambda i: (0, which, i, 0, 0)),
            operand_spec,
        ],
        out_specs=[pl.BlockSpec((units, features), lambda i: (i, 0)), product_spec],
        out_shape=[
            jax.ShapeDtypeStruct((tp_count * units, features), main.dtype),
            jax.ShapeDtypeStruct(product_shape, jnp.float32),
        ],
        cost_estimate=pl.CostEstimate(
            flops=1000 * tp_count * units * features,
            bytes_accessed=4 * tp_count * units * features,
            transcendentals=0,
        ),
    )(main, rest, operand)


def join_in(main, rest, which, chosen):
    tp_count, units = rest.shape[2], main.shape[2]
    slots, features = chosen.shape

    def kernel(main_ref, rest_ref, chosen_ref, new_ref, product_ref):
        joined(main_ref, rest_ref, new_ref)
        product_ref[0] = lax.dot_general(
            chosen_ref[...], new_ref[...], (((1,), (1,)), ((), ())), preferred_element_type=jnp.float32
        )

    return join_call(
        main, rest, which, kernel, chosen,
        pl.BlockSpec((slots, features), lambda i: (0, 0)),
        pl.BlockSpec((1, slots, units), lambda i: (i, 0, 0)),
        (tp_count, slots, units),
    )


def join_out(main, rest, which, hidden):
    _, slots, units = hidden.shape
    features = main.shape[0] * (main.shape[3] + 64)

    def kernel(main_ref, rest_ref, hidden_ref, new_ref, total_ref):
        joined(main_ref, rest_ref, new_ref)

        @pl.when(pl.program_id(0) == 0)
        def _():
            total_ref[...] = jnp.zeros_like(total_ref)

        total_ref[...] += jnp.dot(hidden_ref[0], new_ref[...], preferred_element_type=jnp.float32)

    return join_call(
        main, rest, which, kernel, hidden,
        pl.BlockSpec((1, slots, units), lambda i: (i, 0, 0)),
        pl.BlockSpec((slots, features), lambda i: (0, 0)),
        (slots, features),
    )


def place_late(arrived, places, base, count):
    pieces, units, wide = arrived.shape
    start = jnp.stack([column for _, _, column in places])

    def kernel(start_ref, arrived_ref, base_ref, new_ref, hold, load_sem, keep_sem):
        z = lax.axis_index("fs")

        @pl.when((z == 0) | (z == count - 1))
        def _():
            loads = [pltpu.make_async_copy(arrived_ref.at[i], hold.at[i], load_sem.at[i]) for i in range(pieces)]
            keeps = [
                pltpu.make_async_copy(
                    hold.at[i],
                    new_ref.at[
                        pl.ds(row * units, units), pl.ds(pl.multiple_of(start_ref[i], 128), wide)
                    ],
                    keep_sem.at[i],
                )
                for i, row, _ in places
            ]
            for load in loads:
                load.start()
            for load, keep in zip(loads, keeps):
                load.wait()
                keep.start()
            for keep in keeps:
                keep.wait()

    return pl.pallas_call(
        kernel,
        grid_spec=pltpu.PrefetchScalarGridSpec(
            num_scalar_prefetch=1,
            grid=(1,),
            in_specs=[pl.BlockSpec(memory_space=pl.ANY)] * 2,
            out_specs=pl.BlockSpec(memory_space=pl.ANY),
            scratch_shapes=[
                pltpu.VMEM(arrived.shape, arrived.dtype),
                pltpu.SemaphoreType.DMA((pieces,)),
                pltpu.SemaphoreType.DMA((pieces,)),
            ],
        ),
        out_shape=jax.ShapeDtypeStruct(base.shape, base.dtype),
        input_output_aliases={2: 0},
        cost_estimate=pl.CostEstimate(
            flops=500 * arrived.size, bytes_accessed=4 * arrived.size, transcendentals=0
        ),
    )(start, arrived, base)


def place_last(arrived, row, column, base, count):
    units, wide = arrived.shape

    def kernel(start_ref, arrived_ref, base_ref, new_ref, keep_sem):
        z = lax.axis_index("fs")

        @pl.when((z == 0) | (z == count - 1))
        def _():
            goal = new_ref.at[pl.ds(row * units, units), pl.ds(pl.multiple_of(start_ref[0], 128), wide)]
            keep = pltpu.make_async_copy(arrived_ref, goal, keep_sem)
            keep.start()
            keep.wait()

    return pl.pallas_call(
        kernel,
        in_specs=[pl.BlockSpec(memory_space=space) for space in (pltpu.SMEM, pltpu.VMEM, pl.ANY)],
        out_specs=pl.BlockSpec(memory_space=pl.ANY),
        out_shape=jax.ShapeDtypeStruct(base.shape, base.dtype),
        scratch_shapes=[pltpu.SemaphoreType.DMA],
        input_output_aliases={2: 0},
        compiler_params=pltpu.CompilerParams(vmem_limit_bytes=4 * arrived.size),
        cost_estimate=pl.CostEstimate(
            flops=500 * arrived.size, bytes_accessed=4 * arrived.size, transcendentals=0
        ),
    )(column.reshape(1), arrived, base)


def pick(tokens, routes, expert):
    tokens_wide = tokens.astype(jnp.float32)
    normed = (
        tokens_wide
        * lax.rsqrt(jnp.mean(tokens_wide * tokens_wide, axis=2, keepdims=True) + norm_eps)
    ).astype(jnp.bfloat16)
    member = jnp.any(routes == expert, axis=2)
    slot_index = jnp.cumsum(member.astype(jnp.int32), axis=1) - 1
    marked = jnp.where(member, slot_index, -1)
    picker = (marked[:, None, :] == jnp.arange(CAP, dtype=jnp.int32)[None, :, None]).astype(jnp.bfloat16)
    chosen = jnp.einsum("gcr,grd->gcd", picker, normed, preferred_element_type=jnp.float32)
    return chosen.astype(jnp.bfloat16).reshape(-1, tokens.shape[2])


def mix(partial_value, routes, route_weights, experts):
    tp_count = lax.axis_size("tp")
    groups = routes.shape[0]
    labels = jnp.arange(experts, dtype=jnp.int32)
    member_all = jnp.any(routes[:, :, :, None] == labels, axis=2)
    slots_all = jnp.cumsum(member_all.astype(jnp.int32), axis=1) - 1
    named = routes[:, :, :, None] == labels
    slot_pair = jnp.sum(jnp.where(named, slots_all[:, :, None, :], 0), axis=3)
    first = CAP * jnp.arange(groups, dtype=jnp.int32)[:, None, None]
    flat_index = (first + slot_pair) * experts + routes
    received = lax.all_to_all(
        partial_value.reshape(groups * CAP, tp_count, -1), "tp", split_axis=1, concat_axis=1, tiled=True
    )
    summed = received.astype(jnp.float32).reshape(groups * CAP * experts, -1)
    picked = jnp.take(summed, flat_index, axis=0)
    return jnp.sum(route_weights[:, :, :, None] * picked, axis=2).astype(jnp.bfloat16)


def line_shards(tokens, gate_train, up_train, down_train, gain, routes, route_weights):
    count = lax.axis_size("fs")
    place = lax.axis_index("fs")
    experts, features, _ = gate_train.shape
    held = experts - 1
    outward = [(1, 0), (count - 2, count - 1)]
    near_sources = (tokens, routes.T, route_weights.T)
    main, rest, _, _, kept_early, kept_last, *near = gather(
        [train.transpose(0, 2, 1) for train in (gate_train, up_train, down_train)],
        gain, near_sources, count, held,
    )
    low = place < count // 2
    far_start = jnp.where(low, main_start(count - 1, features), main_start(0, features)).astype(jnp.int32)
    next_start = jnp.where(low, main_start(count - 2, features), main_start(1, features)).astype(jnp.int32)
    arrived_early = lax.ppermute(kept_early, "fs", outward)

    main, rest, near, near_sources = lax.optimization_barrier((main, rest, near, near_sources))
    both_tokens, both_routes, both_weights = [jnp.stack(pair) for pair in zip(near_sources, near)]
    both_routes, both_weights = both_routes.transpose(0, 2, 1), both_weights.transpose(0, 2, 1)
    chosen = pick(both_tokens, both_routes, lax.axis_index("tp"))
    gate_new, gate_pre = join_in(main, rest, 0, chosen)
    up_new, up_pre = join_in(main, rest, 1, chosen)
    hidden = (jax.nn.silu(gate_pre) * up_pre).astype(jnp.bfloat16)
    down_new, total = join_out(main, rest, 2, hidden)
    both_mixed = mix(total.astype(jnp.bfloat16), both_routes, both_weights, experts)
    near_mixed = lax.ppermute(both_mixed[1], "fs", outward)
    kept_last, _ = lax.optimization_barrier((kept_last, both_mixed))
    arrived_last = lax.ppermute(kept_last, "fs", outward)
    first = experts - held
    early = [(i, i, far_start) for i in range(experts)]
    early += [(experts + i, first + i, next_start) for i in range(held - 1)]
    down_new = place_late(arrived_early, early, down_new, count)
    down_new = place_last(arrived_last[0], experts - 1, next_start, down_new, count)
    at_end = (place == 0) | (place == count - 1)
    mixed = jnp.where(at_end, near_mixed, both_mixed[0])
    return (gate_new[None], up_new[None], down_new[None], mixed)


def solution(mesh):
    sizes = (mesh.shape["fs"], mesh.shape["tp"])

    def step(*args):
        if not fits(sizes, args[1]):
            return shards(*args)
        return line_shards(*args)

    in_specs = (
        P("fs", None),
        P(None, "fs", "tp"),
        P(None, "fs", "tp"),
        P(None, "fs", "tp"),
        P("fs"),
        P("fs", None),
        P("fs", None),
    )
    out_specs = (P("tp", None, None), P("tp", None, None), P("tp", None, None), P("fs", "tp"))
    return jax.shard_map(step, mesh=mesh, in_specs=in_specs, out_specs=out_specs, check_vma=False)
```

```python
import jax
import jax.numpy as jnp
from jax import lax
from jax.experimental import pallas as pl
from jax.experimental.pallas import tpu as pltpu
from jax.sharding import PartitionSpec as P


CAP = 72


norm_eps = 1e-06


def arrange(matrix, tp_count):
    experts, row_count, col_count = matrix.shape
    slices = tp_count // experts
    piece_width = col_count // slices
    shaped = matrix.reshape(experts, row_count, slices, piece_width)
    return shaped.transpose(0, 2, 3, 1).reshape(tp_count, piece_width, row_count)


def block_of(*counts):
    for size in (256, 128):
        if all(count % size == 0 for count in counts):
            return size
    return None


def flip(wide, total_rows, first_row, base=None):
    features, rows = wide.shape
    size = block_of(rows, first_row, total_rows) or rows
    first = first_row // size

    def kernel(*refs):
        refs[-1][...] = refs[0][...].T

    in_specs = [pl.BlockSpec((features, size), lambda i: (0, i))]
    operands = [wide]
    aliases = {}
    if base is not None:
        in_specs.append(pl.BlockSpec(memory_space=pl.ANY))
        operands.append(base)
        aliases = {1: 0}
    return pl.pallas_call(
        kernel,
        grid=(rows // size,),
        in_specs=in_specs,
        out_specs=pl.BlockSpec((size, features), lambda i: (first + i, 0)),
        out_shape=jax.ShapeDtypeStruct((total_rows, features), wide.dtype),
        input_output_aliases=aliases,
        cost_estimate=pl.CostEstimate(
            flops=0, bytes_accessed=4 * features * rows, transcendentals=0
        ),
    )(*operands)


def columns(wide, first, count, *others):
    size = block_of(first, count, *others)
    if size is None:
        return lax.slice_in_dim(wide, first, first + count, axis=1), count, 0
    return wide, size, first // size


def flip_product(wide, first, rows, chosen):
    features = wide.shape[0]
    wide, size, start = columns(wide, first, rows)
    slots = chosen.shape[0]

    def kernel(wide_ref, chosen_ref, rows_ref, product_ref):
        value = wide_ref[...]
        rows_ref[...] = value.T
        product_ref[...] = jnp.dot(chosen_ref[...], value, preferred_element_type=jnp.float32)

    return pl.pallas_call(
        kernel,
        grid=(rows // size,),
        in_specs=[
            pl.BlockSpec((features, size), lambda i: (0, start + i)),
            pl.BlockSpec((slots, features), lambda i: (0, 0)),
        ],
        out_specs=[
            pl.BlockSpec((size, features), lambda i: (i, 0)),
            pl.BlockSpec((slots, size), lambda i: (0, i)),
        ],
        out_shape=[
            jax.ShapeDtypeStruct((rows, features), wide.dtype),
            jax.ShapeDtypeStruct((slots, rows), jnp.float32),
        ],
        cost_estimate=pl.CostEstimate(
            flops=2 * slots * features * rows,
            bytes_accessed=4 * features * rows,
            transcendentals=0,
        ),
    )(wide, chosen)


def spread(train, gain):
    experts, features, count = train.shape
    rows = experts * count
    size = block_of(rows) or rows

    def kernel(train_ref, gain_ref, out_ref):
        out_ref[...] = (train_ref[...] * gain_ref[...]).astype(jnp.bfloat16).T

    return pl.pallas_call(
        kernel,
        grid=(rows // size,),
        in_specs=[
            pl.BlockSpec((size, features), lambda i: (i, 0)),
            pl.BlockSpec((1, features), lambda i: (0, 0)),
        ],
        out_specs=pl.BlockSpec((features, size), lambda i: (0, i)),
        out_shape=jax.ShapeDtypeStruct((features, rows), jnp.bfloat16),
        cost_estimate=pl.CostEstimate(
            flops=train.size, bytes_accessed=6 * train.size, transcendentals=0
        ),
    )(train.transpose(0, 2, 1).reshape(rows, features), gain[None, :])


def flip_dot(wide, first, total_rows, hidden):
    features = wide.shape[0]
    slots, rows = hidden.shape
    wide, size, start = columns(wide, first, rows, total_rows)

    def kernel(wide_ref, hidden_ref, rows_ref, total_ref):
        turned = wide_ref[...].T
        rows_ref[...] = turned

        @pl.when(pl.program_id(0) == 0)
        def _():
            total_ref[...] = jnp.zeros_like(total_ref)

        total_ref[...] += jnp.dot(hidden_ref[...], turned, preferred_element_type=jnp.float32)

    return pl.pallas_call(
        kernel,
        grid=(rows // size,),
        in_specs=[
            pl.BlockSpec((features, size), lambda i: (0, start + i)),
            pl.BlockSpec((slots, size), lambda i: (0, i)),
        ],
        out_specs=[
            pl.BlockSpec((size, features), lambda i: (i, 0)),
            pl.BlockSpec((slots, features), lambda i: (0, 0)),
        ],
        out_shape=[
            jax.ShapeDtypeStruct((total_rows, features), wide.dtype),
            jax.ShapeDtypeStruct((slots, features), jnp.float32),
        ],
        cost_estimate=pl.CostEstimate(
            flops=2 * slots * features * rows,
            bytes_accessed=4 * features * rows,
            transcendentals=0,
        ),
    )(wide, hidden)


def keep_dot(weights, chosen):
    rows, features = weights.shape
    size = block_of(rows) or rows
    slots = chosen.shape[0]

    def kernel(weights_ref, chosen_ref, rows_ref, product_ref):
        rows_ref[...] = weights_ref[...]
        product_ref[...] = lax.dot_general(
            chosen_ref[...],
            weights_ref[...],
            (((1,), (1,)), ((), ())),
            preferred_element_type=jnp.float32,
        )

    return pl.pallas_call(
        kernel,
        grid=(rows // size,),
        in_specs=[
            pl.BlockSpec((size, features), lambda i: (i, 0)),
            pl.BlockSpec((slots, features), lambda i: (0, 0)),
        ],
        out_specs=[
            pl.BlockSpec((size, features), lambda i: (i, 0)),
            pl.BlockSpec((slots, size), lambda i: (0, i)),
        ],
        out_shape=[
            jax.ShapeDtypeStruct((rows, features), weights.dtype),
            jax.ShapeDtypeStruct((slots, rows), jnp.float32),
        ],
        cost_estimate=pl.CostEstimate(
            flops=2 * slots * features * rows,
            bytes_accessed=4 * features * rows,
            transcendentals=0,
        ),
    )(weights, chosen)


def after(value, *others):
    def kernel(*refs):
        pass

    return pl.pallas_call(
        kernel,
        in_specs=[pl.BlockSpec(memory_space=pl.ANY)] * (1 + len(others)),
        out_specs=pl.BlockSpec(memory_space=pl.ANY),
        out_shape=jax.ShapeDtypeStruct(value.shape, value.dtype),
        input_output_aliases={0: 0},
    )(value, *others)


def shards(tokens, gate_train, up_train, down_train, gain, routes, route_weights):
    tp_count = lax.axis_size("tp")
    experts = gate_train.shape[0]
    slices = tp_count // experts
    gain_column = gain[None, :, None]
    up_round = (up_train * gain_column).astype(jnp.bfloat16)
    down_round = down_train.astype(jnp.bfloat16)

    def exchange(matrix):
        return lax.all_to_all(matrix, "tp", split_axis=0, concat_axis=1, tiled=True)

    gate_all = lax.all_gather(spread(gate_train, gain), "fs", axis=0, tiled=True)
    features = gate_all.shape[0]

    up_moved = exchange(arrange(up_round, tp_count))[0].T
    down_moved = exchange(arrange(down_round, tp_count))[0].T
    units = down_moved.shape[1]
    size = block_of(units) or units
    main = units - size if units > size else units
    both_wide = lax.all_gather(
        jnp.concatenate([up_moved, down_moved[:, :main]], axis=1), "fs", axis=0, tiled=True
    )

    tokens_wide = tokens.astype(jnp.float32)
    normed = (
        tokens_wide
        * lax.rsqrt(jnp.mean(tokens_wide * tokens_wide, axis=1, keepdims=True) + norm_eps)
    ).astype(jnp.bfloat16)
    expert = lax.axis_index("tp") // slices
    matches = routes == expert
    member = jnp.any(matches, axis=1)
    slot_index = jnp.cumsum(member.astype(jnp.int32)) - 1
    marked = jnp.where(member, slot_index, -1)
    picker = (marked[None, :] == jnp.arange(CAP, dtype=jnp.int32)[:, None]).astype(jnp.bfloat16)
    chosen = jnp.dot(picker, normed, preferred_element_type=jnp.float32).astype(jnp.bfloat16)
    contract_last = (((1,), (1,)), ((), ()))

    gate_moved = exchange(gate_all.reshape(features, tp_count, -1).transpose(1, 2, 0))
    gate_new, gate_pre = keep_dot(gate_moved[0], chosen)
    up_new, up_pre = flip_product(both_wide, 0, units, chosen)
    hidden = (jax.nn.silu(gate_pre) * up_pre).astype(jnp.bfloat16)
    down_new, partial_value = flip_dot(both_wide, units, units, hidden[:, :main])
    if main < units:
        rest_moved = after(down_moved[:, main:], gate_new)
        rest_wide = lax.all_gather(rest_moved, "fs", axis=0, tiled=True)
        partial_value = partial_value + lax.dot_general(
            hidden[:, main:], rest_wide, contract_last, preferred_element_type=jnp.float32
        )
        down_new = flip(rest_wide, units, main, down_new)
    partial_value = partial_value.astype(jnp.bfloat16)

    labels = jnp.arange(experts, dtype=jnp.int32)
    member_all = jnp.any(routes[:, :, None] == labels[None, None, :], axis=1)
    slots_all = jnp.cumsum(member_all.astype(jnp.int32), axis=0) - 1
    slot_pair = jnp.take_along_axis(slots_all, routes, axis=1)
    flat_index = slot_pair * experts + routes
    received = lax.all_to_all(
        partial_value.reshape(CAP, tp_count, -1), "tp", split_axis=1, concat_axis=1, tiled=True
    )
    summed = jnp.sum(received.reshape(CAP, experts, slices, -1).astype(jnp.float32), axis=2)
    summed = summed.reshape(CAP * experts, -1)
    picked = jnp.take(summed, flat_index, axis=0)
    mixed = jnp.sum(route_weights[:, :, None] * picked, axis=1)
    return (gate_new[None], up_new[None], down_new[None], mixed.astype(jnp.bfloat16))


def fits(mesh_sizes, train):
    count, tp_count = mesh_sizes
    experts, features, units = train.shape
    return (
        experts == tp_count
        and tp_count & (tp_count - 1) == 0
        and tp_count >= 4
        and count >= 4
        and count % 2 == 0
        and features % 128 == 64
        and units % 32 == 0
        and units <= features - 64
    )


def main_start(block, features):
    return block * features + (64 if block % 2 else 0)


def gather(trains, gain, near_sources, count, held, lead):
    mats = len(trains)
    tp_count, units, features = trains[0].shape
    wide, half = features - 64, units // 2
    pieces = mats * tp_count
    bits = tp_count.bit_length() - 1
    nears = len(near_sources)
    depth = 3

    def kernel(*refs):
        refs = list(refs)
        take = lambda number: [refs.pop(0) for _ in range(number)]
        train_refs, (gain_ref,), sources = take(mats), take(1), take(nears)
        main, rest, own_main, own_rest, early, extra, last = take(7)
        targets = take(nears)
        raw, cast, cast_rest, load_sem, keep_sem = take(5)
        plane_send, plane_recv, plane_rest_send, plane_rest_recv = take(4)
        line_send, line_recv, line_rest_send, line_rest_recv = take(4)
        near_send, near_recv, pass_hold, pass_load, pass_keep = take(5)
        z = lax.axis_index("fs")
        t = lax.axis_index("tp")

        def peer(p):
            total = 0
            for b in range(bits):
                mine, other = (t // (1 << b)) % 2, (p // (1 << b)) % 2
                total = total + (mine + other - 2 * mine * other) * (1 << b)
            return total

        def plane(m, p):
            e = peer(p)
            return pltpu.make_async_remote_copy(
                own_main.at[m * tp_count + e], main.at[z, m * tp_count + t], plane_send.at[m, p], plane_recv.at[m, p],
                device_id={"fs": z, "tp": e}, device_id_type=pl.DeviceIdType.MESH,
            )

        def plane_rest(m, p):
            e = peer(p)
            return pltpu.make_async_remote_copy(
                own_rest.at[m, e], rest.at[z, m, t], plane_rest_send.at[m, p], plane_rest_recv.at[m, p],
                device_id={"fs": z, "tp": e}, device_id_type=pl.DeviceIdType.MESH,
            )

        def line(way, step, i):
            block = z + step if way == 0 else z - step
            target = z - 1 if way == 0 else z + 1
            piece = main.at[block, i // tp_count * tp_count + peer(i % tp_count)]
            return pltpu.make_async_remote_copy(
                piece, piece, line_send.at[way, step], line_recv.at[way, step, i],
                device_id={"fs": target, "tp": t}, device_id_type=pl.DeviceIdType.MESH,
            )

        def line_rest(way, step, m):
            block = z + step if way == 0 else z - step
            target = z - 1 if way == 0 else z + 1
            return pltpu.make_async_remote_copy(
                rest.at[block, m], rest.at[block, m], line_rest_send.at[way, step, m], line_rest_recv.at[way, step, m],
                device_id={"fs": target, "tp": t}, device_id_type=pl.DeviceIdType.MESH,
            )

        def has(way, step):
            return z + step <= count - 1 if way == 0 else z - step >= 0

        def sends(way):
            return z >= 1 if way == 0 else z <= count - 2

        def near(k):
            inward = jnp.where(z == 0, 1, count - 2)
            return pltpu.make_async_remote_copy(
                sources[k], targets[k], near_send.at[k], near_recv.at[k],
                device_id={"fs": inward, "tp": t}, device_id_type=pl.DeviceIdType.MESH,
            )

        def into_end(way, step, m, p, sender):
            if m < mats - 1 or step < count - 3:
                return True
            end = sender == 1 if way == 0 else sender == count - 2
            if step == count - 2:
                return jnp.logical_not(end)
            return jnp.logical_not(end & (peer(p) >= tp_count - held - lead * (1 - t % 2)))

        def leaves(way, step, m, p):
            return into_end(way, step, m, p, z)

        def arrives(way, step, m, p):
            return into_end(way, step, m, p, z + 1 if way == 0 else z - 1)

        def load(m, p):
            slot = (m * tp_count + p) % depth
            return pltpu.make_async_copy(train_refs[m].at[peer(p)], raw.at[slot], load_sem.at[slot])

        def keep(m, p, own):
            slot, place = (m * tp_count + p) % depth, m * tp_count + peer(p)
            goal, goal_rest = (main.at[z], rest.at[z, m]) if own else (own_main, own_rest.at[m])
            return (
                pltpu.make_async_copy(cast.at[slot], goal.at[place], keep_sem.at[0, slot]),
                pltpu.make_async_copy(cast_rest.at[slot], goal_rest.at[peer(p)], keep_sem.at[1, slot]),
            )

        def load_ahead(m, p):
            if m < mats:
                load(m, p).start()

        def convert(m, p, own):
            slot = (m * tp_count + p) % depth
            load(m, p).wait()

            def put(odd):
                value = raw[slot]
                if m < mats - 1:
                    value = value * gain_ref[...].reshape(1, features)
                value = value.astype(cast.dtype)
                if odd:
                    cast[slot], end = value[:, 64:], value[:, :64]
                else:
                    cast[slot], end = value[:, :wide], value[:, wide:]
                cast_rest[slot] = jnp.concatenate([end[:half], end[half:]], axis=1)

            pl.when(z % 2 == 0)(lambda: put(False))
            pl.when(z % 2 == 1)(lambda: put(True))
            for copy in keep(m, p, own):
                copy.start()

        def finish(m, p, own):
            for copy in keep(m, p, own):
                copy.wait()
            if not own:
                plane(m, p).start()
                plane_rest(m, p).start()

        def forward(step, m, p, first=False):
            i = m * tp_count + p
            if step == 0 and not first:
                plane(m, p).wait_recv()
            for way in range(2):
                if step > 0:
                    @pl.when(has(way, step) & arrives(way, step - 1, m, p))
                    def _(way=way):
                        line(way, step - 1, i).wait_recv()
                if step < count - 1:
                    @pl.when(has(way, step) & sends(way) & leaves(way, step, m, p))
                    def _(way=way):
                        line(way, step, i).start()

        def forward_rest(step, m):
            if step == 0:
                @pl.loop(1, tp_count)
                def _(p):
                    plane_rest(m, p).wait_recv()
            for way in range(2):
                if step > 0:
                    @pl.when(has(way, step))
                    def _(way=way):
                        line_rest(way, step - 1, m).wait_recv()
                if step < count - 1:
                    @pl.when(has(way, step) & sends(way))
                    def _(way=way):
                        line_rest(way, step, m).start()

        barrier = pltpu.get_barrier_semaphore()
        for p in range(1, tp_count):
            pl.semaphore_signal(
                barrier, inc=1, device_id={"fs": z, "tp": peer(p)}, device_id_type=pl.DeviceIdType.MESH
            )

        @pl.when(z >= 1)
        def _():
            pl.semaphore_signal(
                barrier, inc=1, device_id={"fs": z - 1, "tp": t}, device_id_type=pl.DeviceIdType.MESH
            )

        @pl.when(z <= count - 2)
        def _():
            pl.semaphore_signal(
                barrier, inc=1, device_id={"fs": z + 1, "tp": t}, device_id_type=pl.DeviceIdType.MESH
            )

        for p in range(depth):
            load(0, p).start()
        for m in range(mats):
            convert(m, 0, True)
            load_ahead(m, depth)
            if m == 0:
                middle = jnp.logical_and(z >= 1, z <= count - 2)
                pl.semaphore_wait(barrier, tp_count + jnp.where(middle, 1, 0))
                finish(0, 0, True)
                forward(0, 0, 0, first=True)
            else:
                finish(m - 1, tp_count - 1, False)
                if m > 1:
                    forward(0, m - 1, 0, first=True)

            @pl.loop(1, tp_count)
            def _(p, m=m):
                convert(m, p, False)
                pl.when(p + depth < tp_count)(lambda: load(m, p + depth).start())
                if m + 1 < mats:
                    pl.when(p + depth >= tp_count)(lambda: load(m + 1, p + depth - tp_count).start())
                if m == 0:
                    pl.when(p >= 2)(lambda: finish(m, p - 1, False))
                else:
                    pl.when(p == 1)(lambda: finish(m, 0, True))
                    pl.when(p >= 2)(lambda: finish(m, p - 1, False))
                    forward(0, m - 1, p)

            if m > 0:
                forward_rest(0, m - 1)
        finish(mats - 1, tp_count - 1, False)
        forward(0, mats - 1, 0, first=True)

        @pl.loop(1, tp_count)
        def _(p):
            forward(0, mats - 1, p)

        forward_rest(0, mats - 1)

        @pl.when((z == 0) | (z == count - 1))
        def _():
            for k in range(nears):
                near(k).start()

        for step in range(1, count):
            for m in range(mats):
                @pl.loop(0, tp_count)
                def _(p, step=step, m=m):
                    forward(step, m, p)

                forward_rest(step, m)

        @pl.when((z == 1) | (z == count - 2))
        def _():
            low = z < count // 2
            far, after_far = jnp.where(low, count - 1, 0), jnp.where(low, count - 2, 1)
            first = pieces - held - lead
            found = [main.at[far, pieces - tp_count + i] for i in range(tp_count)]
            found += [main.at[after_far, first + i] for i in range(lead + held)]
            goal = [early.at[i] for i in range(tp_count)] + [extra.at[i] for i in range(lead)]
            goal += [early.at[tp_count + i] for i in range(held - 1)] + [last.at[0]]
            loads = [pltpu.make_async_copy(f, pass_hold.at[i], pass_load.at[i]) for i, f in enumerate(found)]
            keeps = [pltpu.make_async_copy(pass_hold.at[i], g, pass_keep.at[i]) for i, g in enumerate(goal)]
            for load in loads:
                load.start()
            for load, keep in zip(loads, keeps):
                load.wait()
                keep.start()
            for keep in keeps:
                keep.wait()

        for m in range(mats):
            @pl.loop(1, tp_count)
            def _(p, m=m):
                plane(m, p).wait_send()
                plane_rest(m, p).wait_send()

        @pl.when((z == 0) | (z == count - 1))
        def _():
            for k in range(nears):
                near(k).wait_send()

        @pl.when((z == 1) | (z == count - 2))
        def _():
            for k in range(nears):
                near(k).wait_recv()

        for step in range(count - 1):
            for way in range(2):
                @pl.when(has(way, step) & sends(way))
                def _(way=way, step=step):
                    end = z == (1 if way == 0 else count - 2)

                    def settle(number, way=way, step=step):
                        sent = main.at[z, pl.ds(0, number)]
                        pltpu.make_async_copy(sent, sent, line_send.at[way, step]).wait()

                    if step == count - 2:
                        settle(pieces - tp_count)
                    elif step == count - 3:
                        pl.when(end & (t % 2 == 0))(lambda: settle(pieces - held - lead))
                        pl.when(end & (t % 2 == 1))(lambda: settle(pieces - held))
                        pl.when(jnp.logical_not(end))(lambda: settle(pieces))
                    else:
                        settle(pieces)
                    for m in range(mats):
                        line_rest(way, step, m).wait_send()

    dma = pltpu.SemaphoreType.DMA
    dtype = jnp.bfloat16
    own = pieces * units * features
    anywhere = pl.BlockSpec(memory_space=pl.ANY)
    outs = [
        (count, pieces, units, wide),
        (count, mats, tp_count, half, 128),
        (pieces, units, wide),
        (mats, tp_count, half, 128),
        (tp_count + held - 1, units, wide),
        (lead, units, wide),
        (1, units, wide),
    ]
    return pl.pallas_call(
        kernel,
        in_specs=[anywhere] * mats + [pl.BlockSpec(memory_space=pltpu.VMEM)] + [anywhere] * nears,
        out_specs=[anywhere] * (len(outs) + nears),
        out_shape=[jax.ShapeDtypeStruct(shape, dtype) for shape in outs]
        + [jax.ShapeDtypeStruct(source.shape, source.dtype) for source in near_sources],
        scratch_shapes=[
            pltpu.VMEM((depth, units, features), jnp.float32),
            pltpu.VMEM((depth, units, wide), dtype),
            pltpu.VMEM((depth, half, 128), dtype),
            dma((depth,)),
            dma((2, depth)),
            dma((mats, tp_count)),
            dma((mats, tp_count)),
            dma((mats, tp_count)),
            dma((mats, tp_count)),
            dma((2, count - 1)),
            dma((2, count - 1, pieces)),
            dma((2, count - 1, mats)),
            dma((2, count - 1, mats)),
            dma((nears,)),
            dma((nears,)),
            pltpu.VMEM((tp_count + held + lead, units, wide), dtype),
            dma((tp_count + held + lead,)),
            dma((tp_count + held + lead,)),
        ],
        compiler_params=pltpu.CompilerParams(collective_id=0, has_side_effects=True),
        cost_estimate=pl.CostEstimate(
            flops=1000 * own, bytes_accessed=4 * (count + 3) * own, transcendentals=0
        ),
    )(*trains, gain, *near_sources)


def joined(main_ref, rest_ref, out_ref):
    count, _, units, wide = main_ref.shape
    features = wide + 64
    half = units // 2
    for block in range(count):
        out_ref[:, pl.ds(main_start(block, features), wide)] = main_ref[block, 0]
    for block in range(0, count, 2):
        first, second = rest_ref[block, 0, 0], rest_ref[block + 1, 0, 0]
        place = pl.ds(block * features + wide, 128)
        out_ref[:half, place] = jnp.concatenate([first[:, :64], second[:, :64]], axis=1)
        out_ref[half:, place] = jnp.concatenate([first[:, 64:], second[:, 64:]], axis=1)


def join_call(main, rest, which, kernel, operand, operand_spec, product_spec, product_shape):
    count, _, tp_count, half = rest.shape[:4]
    units, wide = main.shape[2:]
    features = count * (wide + 64)
    return pl.pallas_call(
        kernel,
        grid=(tp_count,),
        in_specs=[
            pl.BlockSpec((count, 1, units, wide), lambda i: (0, which * tp_count + i, 0, 0)),
            pl.BlockSpec((count, 1, 1, half, 128), lambda i: (0, which, i, 0, 0)),
            operand_spec,
        ],
        out_specs=[pl.BlockSpec((units, features), lambda i: (i, 0)), product_spec],
        out_shape=[
            jax.ShapeDtypeStruct((tp_count * units, features), main.dtype),
            jax.ShapeDtypeStruct(product_shape, jnp.float32),
        ],
        cost_estimate=pl.CostEstimate(
            flops=1000 * tp_count * units * features,
            bytes_accessed=4 * tp_count * units * features,
            transcendentals=0,
        ),
    )(main, rest, operand)


def join_in(main, rest, which, chosen):
    tp_count, units = rest.shape[2], main.shape[2]
    slots, features = chosen.shape

    def kernel(main_ref, rest_ref, chosen_ref, new_ref, product_ref):
        joined(main_ref, rest_ref, new_ref)
        product_ref[0] = lax.dot_general(
            chosen_ref[...], new_ref[...], (((1,), (1,)), ((), ())), preferred_element_type=jnp.float32
        )

    return join_call(
        main, rest, which, kernel, chosen,
        pl.BlockSpec((slots, features), lambda i: (0, 0)),
        pl.BlockSpec((1, slots, units), lambda i: (i, 0, 0)),
        (tp_count, slots, units),
    )


def join_out(main, rest, which, hidden):
    _, slots, units = hidden.shape
    features = main.shape[0] * (main.shape[3] + 64)

    def kernel(main_ref, rest_ref, hidden_ref, new_ref, total_ref):
        joined(main_ref, rest_ref, new_ref)

        @pl.when(pl.program_id(0) == 0)
        def _():
            total_ref[...] = jnp.zeros_like(total_ref)

        total_ref[...] += jnp.dot(hidden_ref[0], new_ref[...], preferred_element_type=jnp.float32)

    return join_call(
        main, rest, which, kernel, hidden,
        pl.BlockSpec((1, slots, units), lambda i: (i, 0, 0)),
        pl.BlockSpec((slots, features), lambda i: (0, 0)),
        (slots, features),
    )


def place_late(arrived, places, extra, extra_places, base, count):
    units, wide = arrived.shape[1:]
    places, extra_places = list(places), list(extra_places)
    total = len(places) + len(extra_places)
    start = jnp.stack([column for _, column in places + extra_places])

    def kernel(start_ref, arrived_ref, extra_ref, base_ref, new_ref, hold, load_sem, keep_sem):
        z, t = lax.axis_index("fs"), lax.axis_index("tp")

        def move(source, number, first, rows):
            loads, keeps = [], []
            for i in range(number):
                k = first + i
                goal = new_ref.at[
                    pl.ds(rows[i][0] * units, units), pl.ds(pl.multiple_of(start_ref[k], 128), wide)
                ]
                loads.append(pltpu.make_async_copy(source.at[i], hold.at[k], load_sem.at[k]))
                keeps.append(pltpu.make_async_copy(hold.at[k], goal, keep_sem.at[k]))
            for load in loads:
                load.start()
            for load, keep in zip(loads, keeps):
                load.wait()
                keep.start()
            for keep in keeps:
                keep.wait()

        at_end = (z == 0) | (z == count - 1)
        pl.when(at_end)(lambda: move(arrived_ref, len(places), 0, places))
        pl.when(at_end & (t % 2 == 0))(
            lambda: move(extra_ref, len(extra_places), len(places), extra_places)
        )

    return pl.pallas_call(
        kernel,
        in_specs=[pl.BlockSpec(memory_space=pltpu.SMEM)] + [pl.BlockSpec(memory_space=pl.ANY)] * 3,
        out_specs=pl.BlockSpec(memory_space=pl.ANY),
        scratch_shapes=[
            pltpu.VMEM((total, units, wide), arrived.dtype),
            pltpu.SemaphoreType.DMA((total,)),
            pltpu.SemaphoreType.DMA((total,)),
        ],
        out_shape=jax.ShapeDtypeStruct(base.shape, base.dtype),
        input_output_aliases={3: 0},
        cost_estimate=pl.CostEstimate(
            flops=500 * arrived.size, bytes_accessed=4 * arrived.size, transcendentals=0
        ),
    )(start, arrived, extra, base)


def place_last(arrived, row, column, base, count):
    units, wide = arrived.shape

    def kernel(start_ref, arrived_ref, base_ref, new_ref, keep_sem):
        z = lax.axis_index("fs")

        @pl.when((z == 0) | (z == count - 1))
        def _():
            goal = new_ref.at[pl.ds(row * units, units), pl.ds(pl.multiple_of(start_ref[0], 128), wide)]
            keep = pltpu.make_async_copy(arrived_ref, goal, keep_sem)
            keep.start()
            keep.wait()

    return pl.pallas_call(
        kernel,
        in_specs=[pl.BlockSpec(memory_space=space) for space in (pltpu.SMEM, pltpu.VMEM, pl.ANY)],
        out_specs=pl.BlockSpec(memory_space=pl.ANY),
        out_shape=jax.ShapeDtypeStruct(base.shape, base.dtype),
        scratch_shapes=[pltpu.SemaphoreType.DMA],
        input_output_aliases={2: 0},
        compiler_params=pltpu.CompilerParams(vmem_limit_bytes=4 * arrived.size),
        cost_estimate=pl.CostEstimate(
            flops=500 * arrived.size, bytes_accessed=4 * arrived.size, transcendentals=0
        ),
    )(column.reshape(1), arrived, base)


def pick(tokens, routes, expert):
    tokens_wide = tokens.astype(jnp.float32)
    normed = (
        tokens_wide
        * lax.rsqrt(jnp.mean(tokens_wide * tokens_wide, axis=2, keepdims=True) + norm_eps)
    ).astype(jnp.bfloat16)
    member = jnp.any(routes == expert, axis=2)
    slot_index = jnp.cumsum(member.astype(jnp.int32), axis=1) - 1
    marked = jnp.where(member, slot_index, -1)
    picker = (marked[:, None, :] == jnp.arange(CAP, dtype=jnp.int32)[None, :, None]).astype(jnp.bfloat16)
    chosen = jnp.einsum("gcr,grd->gcd", picker, normed, preferred_element_type=jnp.float32)
    return chosen.astype(jnp.bfloat16).reshape(-1, tokens.shape[2])


def mix(partial_value, routes, route_weights, experts):
    tp_count = lax.axis_size("tp")
    groups = routes.shape[0]
    labels = jnp.arange(experts, dtype=jnp.int32)
    member_all = jnp.any(routes[:, :, :, None] == labels, axis=2)
    slots_all = jnp.cumsum(member_all.astype(jnp.int32), axis=1) - 1
    named = routes[:, :, :, None] == labels
    slot_pair = jnp.sum(jnp.where(named, slots_all[:, :, None, :], 0), axis=3)
    first = CAP * jnp.arange(groups, dtype=jnp.int32)[:, None, None]
    flat_index = (first + slot_pair) * experts + routes
    received = lax.all_to_all(
        partial_value.reshape(groups * CAP, tp_count, -1), "tp", split_axis=1, concat_axis=1, tiled=True
    )
    summed = received.astype(jnp.float32).reshape(groups * CAP * experts, -1)
    picked = jnp.take(summed, flat_index, axis=0)
    return jnp.sum(route_weights[:, :, :, None] * picked, axis=2).astype(jnp.bfloat16)


def line_shards(tokens, gate_train, up_train, down_train, gain, routes, route_weights):
    count = lax.axis_size("fs")
    place = lax.axis_index("fs")
    experts, features, _ = gate_train.shape
    lead = 2
    held = experts - lead
    outward = [(1, 0), (count - 2, count - 1)]
    near_sources = (tokens, routes.T, route_weights.T)
    main, rest, _, _, kept_early, kept_extra, kept_last, *near = gather(
        [train.transpose(0, 2, 1) for train in (gate_train, up_train, down_train)],
        gain, near_sources, count, held, lead,
    )
    low = place < count // 2
    far_start = jnp.where(low, main_start(count - 1, features), main_start(0, features)).astype(jnp.int32)
    next_start = jnp.where(low, main_start(count - 2, features), main_start(1, features)).astype(jnp.int32)
    pairs = [(a * experts + t, b * experts + t) for a, b in outward for t in range(0, experts, 2)]
    arrived_extra = lax.ppermute(kept_extra, ("fs", "tp"), pairs)
    arrived_early = lax.ppermute(kept_early, "fs", outward)

    main, rest, near, near_sources = lax.optimization_barrier((main, rest, near, near_sources))
    both_tokens, both_routes, both_weights = [jnp.stack(pair) for pair in zip(near_sources, near)]
    both_routes, both_weights = both_routes.transpose(0, 2, 1), both_weights.transpose(0, 2, 1)
    chosen = pick(both_tokens, both_routes, lax.axis_index("tp"))
    gate_new, gate_pre = join_in(main, rest, 0, chosen)
    up_new, up_pre = join_in(main, rest, 1, chosen)
    hidden = (jax.nn.silu(gate_pre) * up_pre).astype(jnp.bfloat16)
    down_new, total = join_out(main, rest, 2, hidden)
    both_mixed = mix(total.astype(jnp.bfloat16), both_routes, both_weights, experts)
    near_mixed = lax.ppermute(both_mixed[1], "fs", outward)
    kept_last, _ = lax.optimization_barrier((kept_last, both_mixed))
    arrived_last = lax.ppermute(kept_last, "fs", outward)
    early = [(i, far_start) for i in range(experts)]
    early += [(i, next_start) for i in range(experts - held, experts - 1)]
    extra = [(i, next_start) for i in range(experts - held - lead, experts - held)]
    down_new = place_late(arrived_early, early, arrived_extra, extra, down_new, count)
    down_new = place_last(arrived_last[0], experts - 1, next_start, down_new, count)
    at_end = (place == 0) | (place == count - 1)
    mixed = jnp.where(at_end, near_mixed, both_mixed[0])
    return (gate_new[None], up_new[None], down_new[None], mixed)


def solution(mesh):
    sizes = (mesh.shape["fs"], mesh.shape["tp"])

    def step(*args):
        if not fits(sizes, args[1]):
            return shards(*args)
        return line_shards(*args)

    in_specs = (
        P("fs", None),
        P(None, "fs", "tp"),
        P(None, "fs", "tp"),
        P(None, "fs", "tp"),
        P("fs"),
        P("fs", None),
        P("fs", None),
    )
    out_specs = (P("tp", None, None), P("tp", None, None), P("tp", None, None), P("fs", "tp"))
    return jax.shard_map(step, mesh=mesh, in_specs=in_specs, out_specs=out_specs, check_vma=False)
```

```python
import jax
import jax.numpy as jnp
from jax import lax
from jax.experimental import pallas as pl
from jax.experimental.pallas import tpu as pltpu
from jax.sharding import PartitionSpec as P


CAP = 72


norm_eps = 1e-06


def arrange(matrix, tp_count):
    experts, row_count, col_count = matrix.shape
    slices = tp_count // experts
    piece_width = col_count // slices
    shaped = matrix.reshape(experts, row_count, slices, piece_width)
    return shaped.transpose(0, 2, 3, 1).reshape(tp_count, piece_width, row_count)


def block_of(*counts):
    for size in (256, 128):
        if all(count % size == 0 for count in counts):
            return size
    return None


def flip(wide, total_rows, first_row, base=None):
    features, rows = wide.shape
    size = block_of(rows, first_row, total_rows) or rows
    first = first_row // size

    def kernel(*refs):
        refs[-1][...] = refs[0][...].T

    in_specs = [pl.BlockSpec((features, size), lambda i: (0, i))]
    operands = [wide]
    aliases = {}
    if base is not None:
        in_specs.append(pl.BlockSpec(memory_space=pl.ANY))
        operands.append(base)
        aliases = {1: 0}
    return pl.pallas_call(
        kernel,
        grid=(rows // size,),
        in_specs=in_specs,
        out_specs=pl.BlockSpec((size, features), lambda i: (first + i, 0)),
        out_shape=jax.ShapeDtypeStruct((total_rows, features), wide.dtype),
        input_output_aliases=aliases,
        cost_estimate=pl.CostEstimate(
            flops=0, bytes_accessed=4 * features * rows, transcendentals=0
        ),
    )(*operands)


def columns(wide, first, count, *others):
    size = block_of(first, count, *others)
    if size is None:
        return lax.slice_in_dim(wide, first, first + count, axis=1), count, 0
    return wide, size, first // size


def flip_product(wide, first, rows, chosen):
    features = wide.shape[0]
    wide, size, start = columns(wide, first, rows)
    slots = chosen.shape[0]

    def kernel(wide_ref, chosen_ref, rows_ref, product_ref):
        value = wide_ref[...]
        rows_ref[...] = value.T
        product_ref[...] = jnp.dot(chosen_ref[...], value, preferred_element_type=jnp.float32)

    return pl.pallas_call(
        kernel,
        grid=(rows // size,),
        in_specs=[
            pl.BlockSpec((features, size), lambda i: (0, start + i)),
            pl.BlockSpec((slots, features), lambda i: (0, 0)),
        ],
        out_specs=[
            pl.BlockSpec((size, features), lambda i: (i, 0)),
            pl.BlockSpec((slots, size), lambda i: (0, i)),
        ],
        out_shape=[
            jax.ShapeDtypeStruct((rows, features), wide.dtype),
            jax.ShapeDtypeStruct((slots, rows), jnp.float32),
        ],
        cost_estimate=pl.CostEstimate(
            flops=2 * slots * features * rows,
            bytes_accessed=4 * features * rows,
            transcendentals=0,
        ),
    )(wide, chosen)


def spread(train, gain):
    experts, features, count = train.shape
    rows = experts * count
    size = block_of(rows) or rows

    def kernel(train_ref, gain_ref, out_ref):
        out_ref[...] = (train_ref[...] * gain_ref[...]).astype(jnp.bfloat16).T

    return pl.pallas_call(
        kernel,
        grid=(rows // size,),
        in_specs=[
            pl.BlockSpec((size, features), lambda i: (i, 0)),
            pl.BlockSpec((1, features), lambda i: (0, 0)),
        ],
        out_specs=pl.BlockSpec((features, size), lambda i: (0, i)),
        out_shape=jax.ShapeDtypeStruct((features, rows), jnp.bfloat16),
        cost_estimate=pl.CostEstimate(
            flops=train.size, bytes_accessed=6 * train.size, transcendentals=0
        ),
    )(train.transpose(0, 2, 1).reshape(rows, features), gain[None, :])


def flip_dot(wide, first, total_rows, hidden):
    features = wide.shape[0]
    slots, rows = hidden.shape
    wide, size, start = columns(wide, first, rows, total_rows)

    def kernel(wide_ref, hidden_ref, rows_ref, total_ref):
        turned = wide_ref[...].T
        rows_ref[...] = turned

        @pl.when(pl.program_id(0) == 0)
        def _():
            total_ref[...] = jnp.zeros_like(total_ref)

        total_ref[...] += jnp.dot(hidden_ref[...], turned, preferred_element_type=jnp.float32)

    return pl.pallas_call(
        kernel,
        grid=(rows // size,),
        in_specs=[
            pl.BlockSpec((features, size), lambda i: (0, start + i)),
            pl.BlockSpec((slots, size), lambda i: (0, i)),
        ],
        out_specs=[
            pl.BlockSpec((size, features), lambda i: (i, 0)),
            pl.BlockSpec((slots, features), lambda i: (0, 0)),
        ],
        out_shape=[
            jax.ShapeDtypeStruct((total_rows, features), wide.dtype),
            jax.ShapeDtypeStruct((slots, features), jnp.float32),
        ],
        cost_estimate=pl.CostEstimate(
            flops=2 * slots * features * rows,
            bytes_accessed=4 * features * rows,
            transcendentals=0,
        ),
    )(wide, hidden)


def keep_dot(weights, chosen):
    rows, features = weights.shape
    size = block_of(rows) or rows
    slots = chosen.shape[0]

    def kernel(weights_ref, chosen_ref, rows_ref, product_ref):
        rows_ref[...] = weights_ref[...]
        product_ref[...] = lax.dot_general(
            chosen_ref[...],
            weights_ref[...],
            (((1,), (1,)), ((), ())),
            preferred_element_type=jnp.float32,
        )

    return pl.pallas_call(
        kernel,
        grid=(rows // size,),
        in_specs=[
            pl.BlockSpec((size, features), lambda i: (i, 0)),
            pl.BlockSpec((slots, features), lambda i: (0, 0)),
        ],
        out_specs=[
            pl.BlockSpec((size, features), lambda i: (i, 0)),
            pl.BlockSpec((slots, size), lambda i: (0, i)),
        ],
        out_shape=[
            jax.ShapeDtypeStruct((rows, features), weights.dtype),
            jax.ShapeDtypeStruct((slots, rows), jnp.float32),
        ],
        cost_estimate=pl.CostEstimate(
            flops=2 * slots * features * rows,
            bytes_accessed=4 * features * rows,
            transcendentals=0,
        ),
    )(weights, chosen)


def after(value, *others):
    def kernel(*refs):
        pass

    return pl.pallas_call(
        kernel,
        in_specs=[pl.BlockSpec(memory_space=pl.ANY)] * (1 + len(others)),
        out_specs=pl.BlockSpec(memory_space=pl.ANY),
        out_shape=jax.ShapeDtypeStruct(value.shape, value.dtype),
        input_output_aliases={0: 0},
    )(value, *others)


def shards(tokens, gate_train, up_train, down_train, gain, routes, route_weights):
    tp_count = lax.axis_size("tp")
    experts = gate_train.shape[0]
    slices = tp_count // experts
    gain_column = gain[None, :, None]
    up_round = (up_train * gain_column).astype(jnp.bfloat16)
    down_round = down_train.astype(jnp.bfloat16)

    def exchange(matrix):
        return lax.all_to_all(matrix, "tp", split_axis=0, concat_axis=1, tiled=True)

    gate_all = lax.all_gather(spread(gate_train, gain), "fs", axis=0, tiled=True)
    features = gate_all.shape[0]

    up_moved = exchange(arrange(up_round, tp_count))[0].T
    down_moved = exchange(arrange(down_round, tp_count))[0].T
    units = down_moved.shape[1]
    size = block_of(units) or units
    main = units - size if units > size else units
    both_wide = lax.all_gather(
        jnp.concatenate([up_moved, down_moved[:, :main]], axis=1), "fs", axis=0, tiled=True
    )

    tokens_wide = tokens.astype(jnp.float32)
    normed = (
        tokens_wide
        * lax.rsqrt(jnp.mean(tokens_wide * tokens_wide, axis=1, keepdims=True) + norm_eps)
    ).astype(jnp.bfloat16)
    expert = lax.axis_index("tp") // slices
    matches = routes == expert
    member = jnp.any(matches, axis=1)
    slot_index = jnp.cumsum(member.astype(jnp.int32)) - 1
    marked = jnp.where(member, slot_index, -1)
    picker = (marked[None, :] == jnp.arange(CAP, dtype=jnp.int32)[:, None]).astype(jnp.bfloat16)
    chosen = jnp.dot(picker, normed, preferred_element_type=jnp.float32).astype(jnp.bfloat16)
    contract_last = (((1,), (1,)), ((), ()))

    gate_moved = exchange(gate_all.reshape(features, tp_count, -1).transpose(1, 2, 0))
    gate_new, gate_pre = keep_dot(gate_moved[0], chosen)
    up_new, up_pre = flip_product(both_wide, 0, units, chosen)
    hidden = (jax.nn.silu(gate_pre) * up_pre).astype(jnp.bfloat16)
    down_new, partial_value = flip_dot(both_wide, units, units, hidden[:, :main])
    if main < units:
        rest_moved = after(down_moved[:, main:], gate_new)
        rest_wide = lax.all_gather(rest_moved, "fs", axis=0, tiled=True)
        partial_value = partial_value + lax.dot_general(
            hidden[:, main:], rest_wide, contract_last, preferred_element_type=jnp.float32
        )
        down_new = flip(rest_wide, units, main, down_new)
    partial_value = partial_value.astype(jnp.bfloat16)

    labels = jnp.arange(experts, dtype=jnp.int32)
    member_all = jnp.any(routes[:, :, None] == labels[None, None, :], axis=1)
    slots_all = jnp.cumsum(member_all.astype(jnp.int32), axis=0) - 1
    slot_pair = jnp.take_along_axis(slots_all, routes, axis=1)
    flat_index = slot_pair * experts + routes
    received = lax.all_to_all(
        partial_value.reshape(CAP, tp_count, -1), "tp", split_axis=1, concat_axis=1, tiled=True
    )
    summed = jnp.sum(received.reshape(CAP, experts, slices, -1).astype(jnp.float32), axis=2)
    summed = summed.reshape(CAP * experts, -1)
    picked = jnp.take(summed, flat_index, axis=0)
    mixed = jnp.sum(route_weights[:, :, None] * picked, axis=1)
    return (gate_new[None], up_new[None], down_new[None], mixed.astype(jnp.bfloat16))


def fits(mesh_sizes, train):
    count, tp_count = mesh_sizes
    experts, features, units = train.shape
    return (
        experts == tp_count
        and tp_count & (tp_count - 1) == 0
        and tp_count >= 4
        and count >= 4
        and count % 2 == 0
        and features % 128 == 64
        and units % 32 == 0
        and units <= features - 64
    )


def main_start(block, features):
    return block * features + (64 if block % 2 else 0)


def gather(trains, gain, near_sources, count, held, lead):
    mats = len(trains)
    tp_count, units, features = trains[0].shape
    wide, half = features - 64, units // 2
    pieces = mats * tp_count
    bits = tp_count.bit_length() - 1
    nears = len(near_sources)
    depth = 3

    def kernel(*refs):
        refs = list(refs)
        take = lambda number: [refs.pop(0) for _ in range(number)]
        train_refs, (gain_ref,), sources = take(mats), take(1), take(nears)
        main, rest, own_main, own_rest, early, extra, last = take(7)
        targets = take(nears)
        raw, cast, cast_rest, load_sem, keep_sem = take(5)
        plane_send, plane_recv, plane_rest_send, plane_rest_recv = take(4)
        line_send, line_recv, line_rest_send, line_rest_recv = take(4)
        near_send, near_recv, pass_hold, pass_load, pass_keep = take(5)
        z = lax.axis_index("fs")
        t = lax.axis_index("tp")

        def peer(p):
            total = 0
            for b in range(bits):
                mine, other = (t // (1 << b)) % 2, (p // (1 << b)) % 2
                total = total + (mine + other - 2 * mine * other) * (1 << b)
            return total

        def plane(m, p):
            e = peer(p)
            return pltpu.make_async_remote_copy(
                own_main.at[m * tp_count + e], main.at[z, m * tp_count + t], plane_send.at[m, p], plane_recv.at[m, p],
                device_id={"fs": z, "tp": e}, device_id_type=pl.DeviceIdType.MESH,
            )

        def plane_rest(m, p):
            e = peer(p)
            return pltpu.make_async_remote_copy(
                own_rest.at[m, e], rest.at[z, m, t], plane_rest_send.at[m, p], plane_rest_recv.at[m, p],
                device_id={"fs": z, "tp": e}, device_id_type=pl.DeviceIdType.MESH,
            )

        def line(way, step, i, source=True):
            block = z + step if way == 0 else z - step
            target = z - 1 if way == 0 else z + 1
            piece = main.at[block, i // tp_count * tp_count + peer(i % tp_count)]
            return pltpu.make_async_remote_copy(
                cast.at[depth] if source is None else piece, piece, line_send.at[way, step], line_recv.at[way, step, i],
                device_id={"fs": target, "tp": t}, device_id_type=pl.DeviceIdType.MESH,
            )

        def line_rest(way, step, m):
            block = z + step if way == 0 else z - step
            target = z - 1 if way == 0 else z + 1
            return pltpu.make_async_remote_copy(
                rest.at[block, m], rest.at[block, m], line_rest_send.at[way, step, m], line_rest_recv.at[way, step, m],
                device_id={"fs": target, "tp": t}, device_id_type=pl.DeviceIdType.MESH,
            )

        def has(way, step):
            return z + step <= count - 1 if way == 0 else z - step >= 0

        def sends(way):
            return z >= 1 if way == 0 else z <= count - 2

        def near(k):
            inward = jnp.where(z == 0, 1, count - 2)
            return pltpu.make_async_remote_copy(
                sources[k], targets[k], near_send.at[k], near_recv.at[k],
                device_id={"fs": inward, "tp": t}, device_id_type=pl.DeviceIdType.MESH,
            )

        def into_end(way, step, m, p, sender):
            if m < mats - 1 or step < count - 3:
                return True
            end = sender == 1 if way == 0 else sender == count - 2
            if step == count - 2:
                return jnp.logical_not(end)
            return jnp.logical_not(end & (peer(p) >= tp_count - held - lead * (1 - t % 2)))

        def leaves(way, step, m, p):
            return into_end(way, step, m, p, z)

        def arrives(way, step, m, p):
            return into_end(way, step, m, p, z + 1 if way == 0 else z - 1)

        def load(m, p):
            slot = (m * tp_count + p) % depth
            return pltpu.make_async_copy(train_refs[m].at[peer(p)], raw.at[slot], load_sem.at[slot])

        def keep(m, p, own):
            slot, place = cast_slot(m, p), m * tp_count + peer(p)
            goal, goal_rest = (main.at[z], rest.at[z, m]) if own else (own_main, own_rest.at[m])
            return (
                pltpu.make_async_copy(cast.at[slot], goal.at[place], keep_sem.at[0, slot]),
                pltpu.make_async_copy(cast_rest.at[slot], goal_rest.at[peer(p)], keep_sem.at[1, slot]),
            )

        def cast_slot(m, p):
            return depth if m == 0 and isinstance(p, int) and p == 0 else (m * tp_count + p) % depth

        def convert(m, p, own):
            slot = cast_slot(m, p)
            load(m, p).wait()

            def put(odd):
                value = raw[(m * tp_count + p) % depth]
                if m < mats - 1:
                    value = value * gain_ref[...].reshape(1, features)
                value = value.astype(cast.dtype)
                if odd:
                    cast[slot], end = value[:, 64:], value[:, :64]
                else:
                    cast[slot], end = value[:, :wide], value[:, wide:]
                cast_rest[slot] = jnp.concatenate([end[:half], end[half:]], axis=1)

            pl.when(z % 2 == 0)(lambda: put(False))
            pl.when(z % 2 == 1)(lambda: put(True))
            for copy in keep(m, p, own):
                copy.start()

        def finish(m, p, own):
            for copy in keep(m, p, own):
                copy.wait()
            if not own:
                plane(m, p).start()
                plane_rest(m, p).start()

        def forward(step, m, p, first=False):
            i = m * tp_count + p
            if step == 0 and not first:
                plane(m, p).wait_recv()
            for way in range(2):
                if step > 0:
                    @pl.when(has(way, step) & arrives(way, step - 1, m, p))
                    def _(way=way):
                        line(way, step - 1, i).wait_recv()
                if step < count - 1:
                    @pl.when(has(way, step) & sends(way) & leaves(way, step, m, p))
                    def _(way=way):
                        line(way, step, i).start()

        def forward_rest(step, m):
            if step == 0:
                @pl.loop(1, tp_count)
                def _(p):
                    plane_rest(m, p).wait_recv()
            for way in range(2):
                if step > 0:
                    @pl.when(has(way, step))
                    def _(way=way):
                        line_rest(way, step - 1, m).wait_recv()
                if step < count - 1:
                    @pl.when(has(way, step) & sends(way))
                    def _(way=way):
                        line_rest(way, step, m).start()

        barrier = pltpu.get_barrier_semaphore()
        for p in range(1, tp_count):
            pl.semaphore_signal(
                barrier, inc=1, device_id={"fs": z, "tp": peer(p)}, device_id_type=pl.DeviceIdType.MESH
            )

        @pl.when(z >= 1)
        def _():
            pl.semaphore_signal(
                barrier, inc=1, device_id={"fs": z - 1, "tp": t}, device_id_type=pl.DeviceIdType.MESH
            )

        @pl.when(z <= count - 2)
        def _():
            pl.semaphore_signal(
                barrier, inc=1, device_id={"fs": z + 1, "tp": t}, device_id_type=pl.DeviceIdType.MESH
            )

        for p in range(depth):
            load(0, p).start()
        for m in range(mats):
            convert(m, 0, True)
            load(m, depth).start()
            if m == 0:
                middle = jnp.logical_and(z >= 1, z <= count - 2)
                pl.semaphore_wait(barrier, tp_count + jnp.where(middle, 1, 0))
                for way in range(2):
                    pl.when(sends(way))(lambda way=way: line(way, 0, 0, None).start())
                finish(0, 0, True)
            else:
                finish(m - 1, tp_count - 1, False)
                if m > 1:
                    forward(0, m - 1, 0, first=True)

            @pl.loop(1, tp_count)
            def _(p, m=m):
                convert(m, p, False)
                pl.when(p + depth < tp_count)(lambda: load(m, p + depth).start())
                if m + 1 < mats:
                    pl.when(p + depth >= tp_count)(lambda: load(m + 1, p + depth - tp_count).start())
                if m == 0:
                    pl.when(p >= 2)(lambda: finish(m, p - 1, False))
                    pl.when(p == tp_count // 2)(lambda: forward(0, 0, 1))
                else:
                    pl.when(p == 1)(lambda: finish(m, 0, True))
                    pl.when(p >= 2)(lambda: finish(m, p - 1, False))
                    if m == 1:
                        pl.when(p >= 2)(lambda: forward(0, 0, p))
                    else:
                        forward(0, m - 1, p)

            if m > 0:
                forward_rest(0, m - 1)
        finish(mats - 1, tp_count - 1, False)
        forward(0, mats - 1, 0, first=True)

        @pl.loop(1, tp_count)
        def _(p):
            forward(0, mats - 1, p)

        forward_rest(0, mats - 1)

        @pl.when((z == 0) | (z == count - 1))
        def _():
            for k in range(nears):
                near(k).start()

        for step in range(1, count):
            for m in range(mats):
                @pl.loop(0, tp_count)
                def _(p, step=step, m=m):
                    forward(step, m, p)

                forward_rest(step, m)

        @pl.when((z == 1) | (z == count - 2))
        def _():
            low = z < count // 2
            far, after_far = jnp.where(low, count - 1, 0), jnp.where(low, count - 2, 1)
            first = pieces - held - lead
            found = [main.at[far, pieces - tp_count + i] for i in range(tp_count)]
            found += [main.at[after_far, first + i] for i in range(lead + held)]
            goal = [early.at[i] for i in range(tp_count)] + [extra.at[i] for i in range(lead)]
            goal += [early.at[tp_count + i] for i in range(held - 1)] + [last.at[0]]
            loads = [pltpu.make_async_copy(f, pass_hold.at[i], pass_load.at[i]) for i, f in enumerate(found)]
            keeps = [pltpu.make_async_copy(pass_hold.at[i], g, pass_keep.at[i]) for i, g in enumerate(goal)]
            for load in loads:
                load.start()
            for load, keep in zip(loads, keeps):
                load.wait()
                keep.start()
            for keep in keeps:
                keep.wait()

        for m in range(mats):
            @pl.loop(1, tp_count)
            def _(p, m=m):
                plane(m, p).wait_send()
                plane_rest(m, p).wait_send()

        @pl.when((z == 0) | (z == count - 1))
        def _():
            for k in range(nears):
                near(k).wait_send()

        @pl.when((z == 1) | (z == count - 2))
        def _():
            for k in range(nears):
                near(k).wait_recv()

        for step in range(count - 1):
            for way in range(2):
                @pl.when(has(way, step) & sends(way))
                def _(way=way, step=step):
                    end = z == (1 if way == 0 else count - 2)

                    def settle(number, way=way, step=step):
                        sent = main.at[z, pl.ds(0, number)]
                        pltpu.make_async_copy(sent, sent, line_send.at[way, step]).wait()

                    if step == count - 2:
                        settle(pieces - tp_count)
                    elif step == count - 3:
                        pl.when(end & (t % 2 == 0))(lambda: settle(pieces - held - lead))
                        pl.when(end & (t % 2 == 1))(lambda: settle(pieces - held))
                        pl.when(jnp.logical_not(end))(lambda: settle(pieces))
                    else:
                        settle(pieces)
                    for m in range(mats):
                        line_rest(way, step, m).wait_send()

    dma = pltpu.SemaphoreType.DMA
    dtype = jnp.bfloat16
    own = pieces * units * features
    anywhere = pl.BlockSpec(memory_space=pl.ANY)
    outs = [
        (count, pieces, units, wide),
        (count, mats, tp_count, half, 128),
        (pieces, units, wide),
        (mats, tp_count, half, 128),
        (tp_count + held - 1, units, wide),
        (lead, units, wide),
        (1, units, wide),
    ]
    return pl.pallas_call(
        kernel,
        in_specs=[anywhere] * mats + [pl.BlockSpec(memory_space=pltpu.VMEM)] + [anywhere] * nears,
        out_specs=[anywhere] * (len(outs) + nears),
        out_shape=[jax.ShapeDtypeStruct(shape, dtype) for shape in outs]
        + [jax.ShapeDtypeStruct(source.shape, source.dtype) for source in near_sources],
        scratch_shapes=[
            pltpu.VMEM((depth, units, features), jnp.float32),
            pltpu.VMEM((depth + 1, units, wide), dtype),
            pltpu.VMEM((depth + 1, half, 128), dtype),
            dma((depth,)),
            dma((2, depth + 1)),
            dma((mats, tp_count)),
            dma((mats, tp_count)),
            dma((mats, tp_count)),
            dma((mats, tp_count)),
            dma((2, count - 1)),
            dma((2, count - 1, pieces)),
            dma((2, count - 1, mats)),
            dma((2, count - 1, mats)),
            dma((nears,)),
            dma((nears,)),
            pltpu.VMEM((tp_count + held + lead, units, wide), dtype),
            dma((tp_count + held + lead,)),
            dma((tp_count + held + lead,)),
        ],
        compiler_params=pltpu.CompilerParams(collective_id=0, has_side_effects=True),
        cost_estimate=pl.CostEstimate(
            flops=1000 * own, bytes_accessed=4 * (count + 3) * own, transcendentals=0
        ),
    )(*trains, gain, *near_sources)


def joined(main_ref, rest_ref, out_ref):
    count, _, units, wide = main_ref.shape
    features = wide + 64
    half = units // 2
    for block in range(count):
        out_ref[:, pl.ds(main_start(block, features), wide)] = main_ref[block, 0]
    for block in range(0, count, 2):
        first, second = rest_ref[block, 0, 0], rest_ref[block + 1, 0, 0]
        place = pl.ds(block * features + wide, 128)
        out_ref[:half, place] = jnp.concatenate([first[:, :64], second[:, :64]], axis=1)
        out_ref[half:, place] = jnp.concatenate([first[:, 64:], second[:, 64:]], axis=1)


def join_call(main, rest, which, kernel, operand, operand_spec, product_spec, product_shape):
    count, _, tp_count, half = rest.shape[:4]
    units, wide = main.shape[2:]
    features = count * (wide + 64)
    return pl.pallas_call(
        kernel,
        grid=(tp_count,),
        in_specs=[
            pl.BlockSpec((count, 1, units, wide), lambda i: (0, which * tp_count + i, 0, 0)),
            pl.BlockSpec((count, 1, 1, half, 128), lambda i: (0, which, i, 0, 0)),
            operand_spec,
        ],
        out_specs=[pl.BlockSpec((units, features), lambda i: (i, 0)), product_spec],
        out_shape=[
            jax.ShapeDtypeStruct((tp_count * units, features), main.dtype),
            jax.ShapeDtypeStruct(product_shape, jnp.float32),
        ],
        cost_estimate=pl.CostEstimate(
            flops=1000 * tp_count * units * features,
            bytes_accessed=4 * tp_count * units * features,
            transcendentals=0,
        ),
    )(main, rest, operand)


def join_in(main, rest, which, chosen):
    tp_count, units = rest.shape[2], main.shape[2]
    slots, features = chosen.shape

    def kernel(main_ref, rest_ref, chosen_ref, new_ref, product_ref):
        joined(main_ref, rest_ref, new_ref)
        product_ref[0] = lax.dot_general(
            chosen_ref[...], new_ref[...], (((1,), (1,)), ((), ())), preferred_element_type=jnp.float32
        )

    return join_call(
        main, rest, which, kernel, chosen,
        pl.BlockSpec((slots, features), lambda i: (0, 0)),
        pl.BlockSpec((1, slots, units), lambda i: (i, 0, 0)),
        (tp_count, slots, units),
    )


def join_out(main, rest, which, hidden):
    _, slots, units = hidden.shape
    features = main.shape[0] * (main.shape[3] + 64)

    def kernel(main_ref, rest_ref, hidden_ref, new_ref, total_ref):
        joined(main_ref, rest_ref, new_ref)

        @pl.when(pl.program_id(0) == 0)
        def _():
            total_ref[...] = jnp.zeros_like(total_ref)

        total_ref[...] += jnp.dot(hidden_ref[0], new_ref[...], preferred_element_type=jnp.float32)

    return join_call(
        main, rest, which, kernel, hidden,
        pl.BlockSpec((1, slots, units), lambda i: (i, 0, 0)),
        pl.BlockSpec((slots, features), lambda i: (0, 0)),
        (slots, features),
    )


def place_late(arrived, places, extra, extra_places, base, count):
    units, wide = arrived.shape[1:]
    places, extra_places = list(places), list(extra_places)
    total = len(places) + len(extra_places)
    start = jnp.stack([column for _, column in places + extra_places])

    def kernel(start_ref, arrived_ref, extra_ref, base_ref, new_ref, hold, load_sem, keep_sem):
        z, t = lax.axis_index("fs"), lax.axis_index("tp")

        def move(source, number, first, rows):
            loads, keeps = [], []
            for i in range(number):
                k = first + i
                goal = new_ref.at[
                    pl.ds(rows[i][0] * units, units), pl.ds(pl.multiple_of(start_ref[k], 128), wide)
                ]
                loads.append(pltpu.make_async_copy(source.at[i], hold.at[k], load_sem.at[k]))
                keeps.append(pltpu.make_async_copy(hold.at[k], goal, keep_sem.at[k]))
            for load in loads:
                load.start()
            for load, keep in zip(loads, keeps):
                load.wait()
                keep.start()
            for keep in keeps:
                keep.wait()

        at_end = (z == 0) | (z == count - 1)
        pl.when(at_end)(lambda: move(arrived_ref, len(places), 0, places))
        pl.when(at_end & (t % 2 == 0))(
            lambda: move(extra_ref, len(extra_places), len(places), extra_places)
        )

    return pl.pallas_call(
        kernel,
        in_specs=[pl.BlockSpec(memory_space=pltpu.SMEM)] + [pl.BlockSpec(memory_space=pl.ANY)] * 3,
        out_specs=pl.BlockSpec(memory_space=pl.ANY),
        scratch_shapes=[
            pltpu.VMEM((total, units, wide), arrived.dtype),
            pltpu.SemaphoreType.DMA((total,)),
            pltpu.SemaphoreType.DMA((total,)),
        ],
        out_shape=jax.ShapeDtypeStruct(base.shape, base.dtype),
        input_output_aliases={3: 0},
        cost_estimate=pl.CostEstimate(
            flops=500 * arrived.size, bytes_accessed=4 * arrived.size, transcendentals=0
        ),
    )(start, arrived, extra, base)


def place_last(arrived, row, column, base, count):
    units, wide = arrived.shape

    def kernel(start_ref, arrived_ref, base_ref, new_ref, keep_sem):
        z = lax.axis_index("fs")

        @pl.when((z == 0) | (z == count - 1))
        def _():
            goal = new_ref.at[pl.ds(row * units, units), pl.ds(pl.multiple_of(start_ref[0], 128), wide)]
            keep = pltpu.make_async_copy(arrived_ref, goal, keep_sem)
            keep.start()
            keep.wait()

    return pl.pallas_call(
        kernel,
        in_specs=[pl.BlockSpec(memory_space=space) for space in (pltpu.SMEM, pltpu.VMEM, pl.ANY)],
        out_specs=pl.BlockSpec(memory_space=pl.ANY),
        out_shape=jax.ShapeDtypeStruct(base.shape, base.dtype),
        scratch_shapes=[pltpu.SemaphoreType.DMA],
        input_output_aliases={2: 0},
        compiler_params=pltpu.CompilerParams(vmem_limit_bytes=4 * arrived.size),
        cost_estimate=pl.CostEstimate(
            flops=500 * arrived.size, bytes_accessed=4 * arrived.size, transcendentals=0
        ),
    )(column.reshape(1), arrived, base)


def pick(tokens, routes, expert):
    tokens_wide = tokens.astype(jnp.float32)
    normed = (
        tokens_wide
        * lax.rsqrt(jnp.mean(tokens_wide * tokens_wide, axis=2, keepdims=True) + norm_eps)
    ).astype(jnp.bfloat16)
    member = jnp.any(routes == expert, axis=2)
    slot_index = jnp.cumsum(member.astype(jnp.int32), axis=1) - 1
    marked = jnp.where(member, slot_index, -1)
    picker = (marked[:, None, :] == jnp.arange(CAP, dtype=jnp.int32)[None, :, None]).astype(jnp.bfloat16)
    chosen = jnp.einsum("gcr,grd->gcd", picker, normed, preferred_element_type=jnp.float32)
    return chosen.astype(jnp.bfloat16).reshape(-1, tokens.shape[2])


def mix(partial_value, routes, route_weights, experts):
    tp_count = lax.axis_size("tp")
    groups = routes.shape[0]
    labels = jnp.arange(experts, dtype=jnp.int32)
    member_all = jnp.any(routes[:, :, :, None] == labels, axis=2)
    slots_all = jnp.cumsum(member_all.astype(jnp.int32), axis=1) - 1
    named = routes[:, :, :, None] == labels
    slot_pair = jnp.sum(jnp.where(named, slots_all[:, :, None, :], 0), axis=3)
    first = CAP * jnp.arange(groups, dtype=jnp.int32)[:, None, None]
    flat_index = (first + slot_pair) * experts + routes
    received = lax.all_to_all(
        partial_value.reshape(groups * CAP, tp_count, -1), "tp", split_axis=1, concat_axis=1, tiled=True
    )
    summed = received.astype(jnp.float32).reshape(groups * CAP * experts, -1)
    picked = jnp.take(summed, flat_index, axis=0)
    return jnp.sum(route_weights[:, :, :, None] * picked, axis=2).astype(jnp.bfloat16)


def line_shards(tokens, gate_train, up_train, down_train, gain, routes, route_weights):
    count = lax.axis_size("fs")
    place = lax.axis_index("fs")
    experts, features, _ = gate_train.shape
    lead = 2
    held = experts - lead
    outward = [(1, 0), (count - 2, count - 1)]
    near_sources = (tokens, routes.T, route_weights.T)
    main, rest, _, _, kept_early, kept_extra, kept_last, *near = gather(
        [train.transpose(0, 2, 1) for train in (gate_train, up_train, down_train)],
        gain, near_sources, count, held, lead,
    )
    low = place < count // 2
    far_start = jnp.where(low, main_start(count - 1, features), main_start(0, features)).astype(jnp.int32)
    next_start = jnp.where(low, main_start(count - 2, features), main_start(1, features)).astype(jnp.int32)
    pairs = [(a * experts + t, b * experts + t) for a, b in outward for t in range(0, experts, 2)]
    arrived_extra = lax.ppermute(kept_extra, ("fs", "tp"), pairs)
    arrived_early = lax.ppermute(kept_early, "fs", outward)

    main, rest, near, near_sources = lax.optimization_barrier((main, rest, near, near_sources))
    both_tokens, both_routes, both_weights = [jnp.stack(pair) for pair in zip(near_sources, near)]
    both_routes, both_weights = both_routes.transpose(0, 2, 1), both_weights.transpose(0, 2, 1)
    chosen = pick(both_tokens, both_routes, lax.axis_index("tp"))
    gate_new, gate_pre = join_in(main, rest, 0, chosen)
    up_new, up_pre = join_in(main, rest, 1, chosen)
    hidden = (jax.nn.silu(gate_pre) * up_pre).astype(jnp.bfloat16)
    down_new, total = join_out(main, rest, 2, hidden)
    both_mixed = mix(total.astype(jnp.bfloat16), both_routes, both_weights, experts)
    near_mixed = lax.ppermute(both_mixed[1], "fs", outward)
    kept_last, _ = lax.optimization_barrier((kept_last, both_mixed))
    arrived_last = lax.ppermute(kept_last, "fs", outward)
    early = [(i, far_start) for i in range(experts)]
    early += [(i, next_start) for i in range(experts - held, experts - 1)]
    extra = [(i, next_start) for i in range(experts - held - lead, experts - held)]
    down_new = place_late(arrived_early, early, arrived_extra, extra, down_new, count)
    down_new = place_last(arrived_last[0], experts - 1, next_start, down_new, count)
    at_end = (place == 0) | (place == count - 1)
    mixed = jnp.where(at_end, near_mixed, both_mixed[0])
    return (gate_new[None], up_new[None], down_new[None], mixed)


def solution(mesh):
    sizes = (mesh.shape["fs"], mesh.shape["tp"])

    def step(*args):
        if not fits(sizes, args[1]):
            return shards(*args)
        return line_shards(*args)

    in_specs = (
        P("fs", None),
        P(None, "fs", "tp"),
        P(None, "fs", "tp"),
        P(None, "fs", "tp"),
        P("fs"),
        P("fs", None),
        P("fs", None),
    )
    out_specs = (P("tp", None, None), P("tp", None, None), P("tp", None, None), P("fs", "tp"))
    return jax.shard_map(step, mesh=mesh, in_specs=in_specs, out_specs=out_specs, check_vma=False)
```

```python
import jax
import jax.numpy as jnp
from jax import lax
from jax.experimental import pallas as pl
from jax.experimental.pallas import tpu as pltpu
from jax.sharding import PartitionSpec as P


CAP = 72


norm_eps = 1e-06


def arrange(matrix, tp_count):
    experts, row_count, col_count = matrix.shape
    slices = tp_count // experts
    piece_width = col_count // slices
    shaped = matrix.reshape(experts, row_count, slices, piece_width)
    return shaped.transpose(0, 2, 3, 1).reshape(tp_count, piece_width, row_count)


def block_of(*counts):
    for size in (256, 128):
        if all(count % size == 0 for count in counts):
            return size
    return None


def flip(wide, total_rows, first_row, base=None):
    features, rows = wide.shape
    size = block_of(rows, first_row, total_rows) or rows
    first = first_row // size

    def kernel(*refs):
        refs[-1][...] = refs[0][...].T

    in_specs = [pl.BlockSpec((features, size), lambda i: (0, i))]
    operands = [wide]
    aliases = {}
    if base is not None:
        in_specs.append(pl.BlockSpec(memory_space=pl.ANY))
        operands.append(base)
        aliases = {1: 0}
    return pl.pallas_call(
        kernel,
        grid=(rows // size,),
        in_specs=in_specs,
        out_specs=pl.BlockSpec((size, features), lambda i: (first + i, 0)),
        out_shape=jax.ShapeDtypeStruct((total_rows, features), wide.dtype),
        input_output_aliases=aliases,
        cost_estimate=pl.CostEstimate(
            flops=0, bytes_accessed=4 * features * rows, transcendentals=0
        ),
    )(*operands)


def columns(wide, first, count, *others):
    size = block_of(first, count, *others)
    if size is None:
        return lax.slice_in_dim(wide, first, first + count, axis=1), count, 0
    return wide, size, first // size


def flip_product(wide, first, rows, chosen):
    features = wide.shape[0]
    wide, size, start = columns(wide, first, rows)
    slots = chosen.shape[0]

    def kernel(wide_ref, chosen_ref, rows_ref, product_ref):
        value = wide_ref[...]
        rows_ref[...] = value.T
        product_ref[...] = jnp.dot(chosen_ref[...], value, preferred_element_type=jnp.float32)

    return pl.pallas_call(
        kernel,
        grid=(rows // size,),
        in_specs=[
            pl.BlockSpec((features, size), lambda i: (0, start + i)),
            pl.BlockSpec((slots, features), lambda i: (0, 0)),
        ],
        out_specs=[
            pl.BlockSpec((size, features), lambda i: (i, 0)),
            pl.BlockSpec((slots, size), lambda i: (0, i)),
        ],
        out_shape=[
            jax.ShapeDtypeStruct((rows, features), wide.dtype),
            jax.ShapeDtypeStruct((slots, rows), jnp.float32),
        ],
        cost_estimate=pl.CostEstimate(
            flops=2 * slots * features * rows,
            bytes_accessed=4 * features * rows,
            transcendentals=0,
        ),
    )(wide, chosen)


def spread(train, gain):
    experts, features, count = train.shape
    rows = experts * count
    size = block_of(rows) or rows

    def kernel(train_ref, gain_ref, out_ref):
        out_ref[...] = (train_ref[...] * gain_ref[...]).astype(jnp.bfloat16).T

    return pl.pallas_call(
        kernel,
        grid=(rows // size,),
        in_specs=[
            pl.BlockSpec((size, features), lambda i: (i, 0)),
            pl.BlockSpec((1, features), lambda i: (0, 0)),
        ],
        out_specs=pl.BlockSpec((features, size), lambda i: (0, i)),
        out_shape=jax.ShapeDtypeStruct((features, rows), jnp.bfloat16),
        cost_estimate=pl.CostEstimate(
            flops=train.size, bytes_accessed=6 * train.size, transcendentals=0
        ),
    )(train.transpose(0, 2, 1).reshape(rows, features), gain[None, :])


def flip_dot(wide, first, total_rows, hidden):
    features = wide.shape[0]
    slots, rows = hidden.shape
    wide, size, start = columns(wide, first, rows, total_rows)

    def kernel(wide_ref, hidden_ref, rows_ref, total_ref):
        turned = wide_ref[...].T
        rows_ref[...] = turned

        @pl.when(pl.program_id(0) == 0)
        def _():
            total_ref[...] = jnp.zeros_like(total_ref)

        total_ref[...] += jnp.dot(hidden_ref[...], turned, preferred_element_type=jnp.float32)

    return pl.pallas_call(
        kernel,
        grid=(rows // size,),
        in_specs=[
            pl.BlockSpec((features, size), lambda i: (0, start + i)),
            pl.BlockSpec((slots, size), lambda i: (0, i)),
        ],
        out_specs=[
            pl.BlockSpec((size, features), lambda i: (i, 0)),
            pl.BlockSpec((slots, features), lambda i: (0, 0)),
        ],
        out_shape=[
            jax.ShapeDtypeStruct((total_rows, features), wide.dtype),
            jax.ShapeDtypeStruct((slots, features), jnp.float32),
        ],
        cost_estimate=pl.CostEstimate(
            flops=2 * slots * features * rows,
            bytes_accessed=4 * features * rows,
            transcendentals=0,
        ),
    )(wide, hidden)


def keep_dot(weights, chosen):
    rows, features = weights.shape
    size = block_of(rows) or rows
    slots = chosen.shape[0]

    def kernel(weights_ref, chosen_ref, rows_ref, product_ref):
        rows_ref[...] = weights_ref[...]
        product_ref[...] = lax.dot_general(
            chosen_ref[...],
            weights_ref[...],
            (((1,), (1,)), ((), ())),
            preferred_element_type=jnp.float32,
        )

    return pl.pallas_call(
        kernel,
        grid=(rows // size,),
        in_specs=[
            pl.BlockSpec((size, features), lambda i: (i, 0)),
            pl.BlockSpec((slots, features), lambda i: (0, 0)),
        ],
        out_specs=[
            pl.BlockSpec((size, features), lambda i: (i, 0)),
            pl.BlockSpec((slots, size), lambda i: (0, i)),
        ],
        out_shape=[
            jax.ShapeDtypeStruct((rows, features), weights.dtype),
            jax.ShapeDtypeStruct((slots, rows), jnp.float32),
        ],
        cost_estimate=pl.CostEstimate(
            flops=2 * slots * features * rows,
            bytes_accessed=4 * features * rows,
            transcendentals=0,
        ),
    )(weights, chosen)


def after(value, *others):
    def kernel(*refs):
        pass

    return pl.pallas_call(
        kernel,
        in_specs=[pl.BlockSpec(memory_space=pl.ANY)] * (1 + len(others)),
        out_specs=pl.BlockSpec(memory_space=pl.ANY),
        out_shape=jax.ShapeDtypeStruct(value.shape, value.dtype),
        input_output_aliases={0: 0},
    )(value, *others)


def shards(tokens, gate_train, up_train, down_train, gain, routes, route_weights):
    tp_count = lax.axis_size("tp")
    experts = gate_train.shape[0]
    slices = tp_count // experts
    gain_column = gain[None, :, None]
    up_round = (up_train * gain_column).astype(jnp.bfloat16)
    down_round = down_train.astype(jnp.bfloat16)

    def exchange(matrix):
        return lax.all_to_all(matrix, "tp", split_axis=0, concat_axis=1, tiled=True)

    gate_all = lax.all_gather(spread(gate_train, gain), "fs", axis=0, tiled=True)
    features = gate_all.shape[0]

    up_moved = exchange(arrange(up_round, tp_count))[0].T
    down_moved = exchange(arrange(down_round, tp_count))[0].T
    units = down_moved.shape[1]
    size = block_of(units) or units
    main = units - size if units > size else units
    both_wide = lax.all_gather(
        jnp.concatenate([up_moved, down_moved[:, :main]], axis=1), "fs", axis=0, tiled=True
    )

    tokens_wide = tokens.astype(jnp.float32)
    normed = (
        tokens_wide
        * lax.rsqrt(jnp.mean(tokens_wide * tokens_wide, axis=1, keepdims=True) + norm_eps)
    ).astype(jnp.bfloat16)
    expert = lax.axis_index("tp") // slices
    matches = routes == expert
    member = jnp.any(matches, axis=1)
    slot_index = jnp.cumsum(member.astype(jnp.int32)) - 1
    marked = jnp.where(member, slot_index, -1)
    picker = (marked[None, :] == jnp.arange(CAP, dtype=jnp.int32)[:, None]).astype(jnp.bfloat16)
    chosen = jnp.dot(picker, normed, preferred_element_type=jnp.float32).astype(jnp.bfloat16)
    contract_last = (((1,), (1,)), ((), ()))

    gate_moved = exchange(gate_all.reshape(features, tp_count, -1).transpose(1, 2, 0))
    gate_new, gate_pre = keep_dot(gate_moved[0], chosen)
    up_new, up_pre = flip_product(both_wide, 0, units, chosen)
    hidden = (jax.nn.silu(gate_pre) * up_pre).astype(jnp.bfloat16)
    down_new, partial_value = flip_dot(both_wide, units, units, hidden[:, :main])
    if main < units:
        rest_moved = after(down_moved[:, main:], gate_new)
        rest_wide = lax.all_gather(rest_moved, "fs", axis=0, tiled=True)
        partial_value = partial_value + lax.dot_general(
            hidden[:, main:], rest_wide, contract_last, preferred_element_type=jnp.float32
        )
        down_new = flip(rest_wide, units, main, down_new)
    partial_value = partial_value.astype(jnp.bfloat16)

    labels = jnp.arange(experts, dtype=jnp.int32)
    member_all = jnp.any(routes[:, :, None] == labels[None, None, :], axis=1)
    slots_all = jnp.cumsum(member_all.astype(jnp.int32), axis=0) - 1
    slot_pair = jnp.take_along_axis(slots_all, routes, axis=1)
    flat_index = slot_pair * experts + routes
    received = lax.all_to_all(
        partial_value.reshape(CAP, tp_count, -1), "tp", split_axis=1, concat_axis=1, tiled=True
    )
    summed = jnp.sum(received.reshape(CAP, experts, slices, -1).astype(jnp.float32), axis=2)
    summed = summed.reshape(CAP * experts, -1)
    picked = jnp.take(summed, flat_index, axis=0)
    mixed = jnp.sum(route_weights[:, :, None] * picked, axis=1)
    return (gate_new[None], up_new[None], down_new[None], mixed.astype(jnp.bfloat16))


def fits(mesh_sizes, rows, train):
    count, tp_count = mesh_sizes
    experts, features, units = train.shape
    return (
        experts == tp_count
        and tp_count & (tp_count - 1) == 0
        and tp_count >= 4
        and count >= 4
        and rows % 32 == 0
        and count % 2 == 0
        and features % 128 == 64
        and units % 32 == 0
        and units <= features - 64
    )


def main_start(block, features):
    return block * features + (64 if block % 2 else 0)


def gather(trains, gain, near_sources, count, held, lead):
    mats = len(trains)
    tp_count, units, features = trains[0].shape
    wide, half = features - 64, units // 2
    pieces = mats * tp_count
    bits = tp_count.bit_length() - 1
    nears = len(near_sources)
    depth = 3

    def kernel(*refs):
        refs = list(refs)
        take = lambda number: [refs.pop(0) for _ in range(number)]
        train_refs, (gain_ref,), sources = take(mats), take(1), take(nears)
        main, rest, own_main, own_rest, early, extra, last = take(7)
        targets = take(nears)
        raw, cast, cast_rest, load_sem, keep_sem = take(5)
        plane_send, plane_recv, plane_rest_send, plane_rest_recv = take(4)
        line_send, line_recv, line_rest_send, line_rest_recv = take(4)
        near_send, near_recv, pass_hold, pass_load, pass_keep = take(5)
        z = lax.axis_index("fs")
        t = lax.axis_index("tp")

        def peer(p):
            total = 0
            for b in range(bits):
                mine, other = (t // (1 << b)) % 2, (p // (1 << b)) % 2
                total = total + (mine + other - 2 * mine * other) * (1 << b)
            return total

        def plane(m, p):
            e = peer(p)
            return pltpu.make_async_remote_copy(
                own_main.at[m * tp_count + e], main.at[z, m * tp_count + t], plane_send.at[m, p], plane_recv.at[m, p],
                device_id={"fs": z, "tp": e}, device_id_type=pl.DeviceIdType.MESH,
            )

        def plane_rest(m, p):
            e = peer(p)
            return pltpu.make_async_remote_copy(
                own_rest.at[m, e], rest.at[z, m, t], plane_rest_send.at[m, p], plane_rest_recv.at[m, p],
                device_id={"fs": z, "tp": e}, device_id_type=pl.DeviceIdType.MESH,
            )

        def line(way, step, i):
            block = z + step if way == 0 else z - step
            target = z - 1 if way == 0 else z + 1
            piece = main.at[block, i // tp_count * tp_count + peer(i % tp_count)]
            return pltpu.make_async_remote_copy(
                piece, piece, line_send.at[way, step], line_recv.at[way, step, i],
                device_id={"fs": target, "tp": t}, device_id_type=pl.DeviceIdType.MESH,
            )

        def line_rest(way, step, m):
            block = z + step if way == 0 else z - step
            target = z - 1 if way == 0 else z + 1
            return pltpu.make_async_remote_copy(
                rest.at[block, m], rest.at[block, m], line_rest_send.at[way, step, m], line_rest_recv.at[way, step, m],
                device_id={"fs": target, "tp": t}, device_id_type=pl.DeviceIdType.MESH,
            )

        def has(way, step):
            return z + step <= count - 1 if way == 0 else z - step >= 0

        def sends(way):
            return z >= 1 if way == 0 else z <= count - 2

        def near(k):
            inward = jnp.where(z == 0, 1, count - 2)
            return pltpu.make_async_remote_copy(
                sources[k], targets[k], near_send.at[k], near_recv.at[k],
                device_id={"fs": inward, "tp": t}, device_id_type=pl.DeviceIdType.MESH,
            )

        def into_end(way, step, m, p, sender):
            if m < mats - 1 or step < count - 3:
                return True
            end = sender == 1 if way == 0 else sender == count - 2
            if step == count - 2:
                return jnp.logical_not(end)
            return jnp.logical_not(end & (peer(p) >= tp_count - held - lead * (1 - t % 2)))

        def leaves(way, step, m, p):
            return into_end(way, step, m, p, z)

        def arrives(way, step, m, p):
            return into_end(way, step, m, p, z + 1 if way == 0 else z - 1)

        def load(m, p):
            slot = (m * tp_count + p) % depth
            return pltpu.make_async_copy(train_refs[m].at[peer(p)], raw.at[slot], load_sem.at[slot])

        def keep(m, p, own):
            slot, place = (m * tp_count + p) % depth, m * tp_count + peer(p)
            goal, goal_rest = (main.at[z], rest.at[z, m]) if own else (own_main, own_rest.at[m])
            return (
                pltpu.make_async_copy(cast.at[slot], goal.at[place], keep_sem.at[0, slot]),
                pltpu.make_async_copy(cast_rest.at[slot], goal_rest.at[peer(p)], keep_sem.at[1, slot]),
            )

        def load_ahead(m, p):
            if m < mats:
                load(m, p).start()

        def convert(m, p, own):
            slot = (m * tp_count + p) % depth
            load(m, p).wait()

            def put(odd):
                value = raw[slot]
                if m < mats - 1:
                    value = value * gain_ref[...].reshape(1, features)
                value = value.astype(cast.dtype)
                if odd:
                    cast[slot], end = value[:, 64:], value[:, :64]
                else:
                    cast[slot], end = value[:, :wide], value[:, wide:]
                cast_rest[slot] = jnp.concatenate([end[:half], end[half:]], axis=1)

            pl.when(z % 2 == 0)(lambda: put(False))
            pl.when(z % 2 == 1)(lambda: put(True))
            for copy in keep(m, p, own):
                copy.start()

        def finish(m, p, own):
            for copy in keep(m, p, own):
                copy.wait()
            if not own:
                plane(m, p).start()
                plane_rest(m, p).start()

        def forward(step, m, p, first=False):
            i = m * tp_count + p
            if step == 0 and not first:
                plane(m, p).wait_recv()
            for way in range(2):
                if step > 0:
                    @pl.when(has(way, step) & arrives(way, step - 1, m, p))
                    def _(way=way):
                        line(way, step - 1, i).wait_recv()
                if step < count - 1:
                    @pl.when(has(way, step) & sends(way) & leaves(way, step, m, p))
                    def _(way=way):
                        line(way, step, i).start()

        def forward_rest(step, m):
            if step == 0:
                @pl.loop(1, tp_count)
                def _(p):
                    plane_rest(m, p).wait_recv()
            for way in range(2):
                if step > 0:
                    @pl.when(has(way, step))
                    def _(way=way):
                        line_rest(way, step - 1, m).wait_recv()
                if step < count - 1:
                    @pl.when(has(way, step) & sends(way))
                    def _(way=way):
                        line_rest(way, step, m).start()

        barrier = pltpu.get_barrier_semaphore()
        for p in range(1, tp_count):
            pl.semaphore_signal(
                barrier, inc=1, device_id={"fs": z, "tp": peer(p)}, device_id_type=pl.DeviceIdType.MESH
            )

        @pl.when(z >= 1)
        def _():
            pl.semaphore_signal(
                barrier, inc=1, device_id={"fs": z - 1, "tp": t}, device_id_type=pl.DeviceIdType.MESH
            )

        @pl.when(z <= count - 2)
        def _():
            pl.semaphore_signal(
                barrier, inc=1, device_id={"fs": z + 1, "tp": t}, device_id_type=pl.DeviceIdType.MESH
            )

        for p in range(depth):
            load(0, p).start()
        for m in range(mats):
            convert(m, 0, True)
            load_ahead(m, depth)
            if m == 0:
                middle = jnp.logical_and(z >= 1, z <= count - 2)
                pl.semaphore_wait(barrier, tp_count + jnp.where(middle, 1, 0))
                finish(0, 0, True)
                forward(0, 0, 0, first=True)
            else:
                finish(m - 1, tp_count - 1, False)
                if m > 1:
                    forward(0, m - 1, 0, first=True)

            @pl.loop(1, tp_count)
            def _(p, m=m):
                convert(m, p, False)
                pl.when(p + depth < tp_count)(lambda: load(m, p + depth).start())
                if m + 1 < mats:
                    pl.when(p + depth >= tp_count)(lambda: load(m + 1, p + depth - tp_count).start())
                if m == 0:
                    pl.when(p >= 2)(lambda: finish(m, p - 1, False))
                else:
                    pl.when(p == 1)(lambda: finish(m, 0, True))
                    pl.when(p >= 2)(lambda: finish(m, p - 1, False))
                    forward(0, m - 1, p)

            if m > 0:
                forward_rest(0, m - 1)
        finish(mats - 1, tp_count - 1, False)
        forward(0, mats - 1, 0, first=True)

        @pl.loop(1, tp_count)
        def _(p):
            forward(0, mats - 1, p)

        forward_rest(0, mats - 1)

        @pl.when((z == 0) | (z == count - 1))
        def _():
            for k in range(nears):
                near(k).start()

        for step in range(1, count):
            for m in range(mats):
                @pl.loop(0, tp_count)
                def _(p, step=step, m=m):
                    forward(step, m, p)

                forward_rest(step, m)

        @pl.when((z == 1) | (z == count - 2))
        def _():
            low = z < count // 2
            far, after_far = jnp.where(low, count - 1, 0), jnp.where(low, count - 2, 1)
            first = pieces - held - lead
            found = [main.at[far, pieces - tp_count + i] for i in range(tp_count)]
            found += [main.at[after_far, first + i] for i in range(lead + held)]
            goal = [early.at[i] for i in range(tp_count)] + [extra.at[i] for i in range(lead)]
            goal += [early.at[tp_count + i] for i in range(held - 1)] + [last.at[0]]
            loads = [pltpu.make_async_copy(f, pass_hold.at[i], pass_load.at[i]) for i, f in enumerate(found)]
            keeps = [pltpu.make_async_copy(pass_hold.at[i], g, pass_keep.at[i]) for i, g in enumerate(goal)]
            for load in loads:
                load.start()
            for load, keep in zip(loads, keeps):
                load.wait()
                keep.start()
            for keep in keeps:
                keep.wait()

        for m in range(mats):
            @pl.loop(1, tp_count)
            def _(p, m=m):
                plane(m, p).wait_send()
                plane_rest(m, p).wait_send()

        @pl.when((z == 0) | (z == count - 1))
        def _():
            for k in range(nears):
                near(k).wait_send()

        @pl.when((z == 1) | (z == count - 2))
        def _():
            for k in range(nears):
                near(k).wait_recv()

        for step in range(count - 1):
            for way in range(2):
                @pl.when(has(way, step) & sends(way))
                def _(way=way, step=step):
                    end = z == (1 if way == 0 else count - 2)

                    def settle(number, way=way, step=step):
                        sent = main.at[z, pl.ds(0, number)]
                        pltpu.make_async_copy(sent, sent, line_send.at[way, step]).wait()

                    if step == count - 2:
                        settle(pieces - tp_count)
                    elif step == count - 3:
                        pl.when(end & (t % 2 == 0))(lambda: settle(pieces - held - lead))
                        pl.when(end & (t % 2 == 1))(lambda: settle(pieces - held))
                        pl.when(jnp.logical_not(end))(lambda: settle(pieces))
                    else:
                        settle(pieces)
                    for m in range(mats):
                        line_rest(way, step, m).wait_send()

    dma = pltpu.SemaphoreType.DMA
    dtype = jnp.bfloat16
    own = pieces * units * features
    anywhere = pl.BlockSpec(memory_space=pl.ANY)
    outs = [
        (count, pieces, units, wide),
        (count, mats, tp_count, half, 128),
        (pieces, units, wide),
        (mats, tp_count, half, 128),
        (tp_count + held - 1, units, wide),
        (lead, units, wide),
        (1, units, wide),
    ]
    return pl.pallas_call(
        kernel,
        in_specs=[anywhere] * mats + [pl.BlockSpec(memory_space=pltpu.VMEM)] + [anywhere] * nears,
        out_specs=[anywhere] * (len(outs) + nears),
        out_shape=[jax.ShapeDtypeStruct(shape, dtype) for shape in outs]
        + [jax.ShapeDtypeStruct(source.shape, source.dtype) for source in near_sources],
        scratch_shapes=[
            pltpu.VMEM((depth, units, features), jnp.float32),
            pltpu.VMEM((depth, units, wide), dtype),
            pltpu.VMEM((depth, half, 128), dtype),
            dma((depth,)),
            dma((2, depth)),
            dma((mats, tp_count)),
            dma((mats, tp_count)),
            dma((mats, tp_count)),
            dma((mats, tp_count)),
            dma((2, count - 1)),
            dma((2, count - 1, pieces)),
            dma((2, count - 1, mats)),
            dma((2, count - 1, mats)),
            dma((nears,)),
            dma((nears,)),
            pltpu.VMEM((tp_count + held + lead, units, wide), dtype),
            dma((tp_count + held + lead,)),
            dma((tp_count + held + lead,)),
        ],
        compiler_params=pltpu.CompilerParams(collective_id=0, has_side_effects=True),
        cost_estimate=pl.CostEstimate(
            flops=1000 * own, bytes_accessed=4 * (count + 3) * own, transcendentals=0
        ),
    )(*trains, gain, *near_sources)


def joined(main_ref, rest_ref, out_ref):
    count, _, units, wide = main_ref.shape
    features = wide + 64
    half = units // 2
    for block in range(count):
        out_ref[:, pl.ds(main_start(block, features), wide)] = main_ref[block, 0]
    for block in range(0, count, 2):
        first, second = rest_ref[block, 0, 0], rest_ref[block + 1, 0, 0]
        place = pl.ds(block * features + wide, 128)
        out_ref[:half, place] = jnp.concatenate([first[:, :64], second[:, :64]], axis=1)
        out_ref[half:, place] = jnp.concatenate([first[:, 64:], second[:, 64:]], axis=1)


def join_call(main, rest, which, kernel, operand, operand_spec, product_spec, product_shape):
    count, _, tp_count, half = rest.shape[:4]
    units, wide = main.shape[2:]
    features = count * (wide + 64)
    return pl.pallas_call(
        kernel,
        grid=(tp_count,),
        in_specs=[
            pl.BlockSpec((count, 1, units, wide), lambda i: (0, which * tp_count + i, 0, 0)),
            pl.BlockSpec((count, 1, 1, half, 128), lambda i: (0, which, i, 0, 0)),
            operand_spec,
        ],
        out_specs=[pl.BlockSpec((units, features), lambda i: (i, 0)), product_spec],
        out_shape=[
            jax.ShapeDtypeStruct((tp_count * units, features), main.dtype),
            jax.ShapeDtypeStruct(product_shape, jnp.float32),
        ],
        cost_estimate=pl.CostEstimate(
            flops=1000 * tp_count * units * features,
            bytes_accessed=4 * tp_count * units * features,
            transcendentals=0,
        ),
    )(main, rest, operand)


def join_in(main, rest, which, chosen):
    tp_count, units = rest.shape[2], main.shape[2]
    slots, features = chosen.shape

    def kernel(main_ref, rest_ref, chosen_ref, new_ref, product_ref):
        joined(main_ref, rest_ref, new_ref)
        product_ref[0] = lax.dot_general(
            chosen_ref[...], new_ref[...], (((1,), (1,)), ((), ())), preferred_element_type=jnp.float32
        )

    return join_call(
        main, rest, which, kernel, chosen,
        pl.BlockSpec((slots, features), lambda i: (0, 0)),
        pl.BlockSpec((1, slots, units), lambda i: (i, 0, 0)),
        (tp_count, slots, units),
    )


def join_out(main, rest, which, hidden):
    _, slots, units = hidden.shape
    features = main.shape[0] * (main.shape[3] + 64)

    def kernel(main_ref, rest_ref, hidden_ref, new_ref, total_ref):
        joined(main_ref, rest_ref, new_ref)

        @pl.when(pl.program_id(0) == 0)
        def _():
            total_ref[...] = jnp.zeros_like(total_ref)

        total_ref[...] += jnp.dot(hidden_ref[0], new_ref[...], preferred_element_type=jnp.float32)

    return join_call(
        main, rest, which, kernel, hidden,
        pl.BlockSpec((1, slots, units), lambda i: (i, 0, 0)),
        pl.BlockSpec((slots, features), lambda i: (0, 0)),
        (slots, features),
    )


def place_late(arrived, places, even_only, base, count):
    pieces, units, wide = arrived.shape
    start = jnp.stack([column for _, column in places])

    def kernel(start_ref, arrived_ref, base_ref, new_ref, hold, load_sem, keep_sem):
        z, t = lax.axis_index("fs"), lax.axis_index("tp")
        wanted = (z == 0) | (z == count - 1)
        if even_only:
            wanted = wanted & (t % 2 == 0)

        @pl.when(wanted)
        def _():
            loads = [pltpu.make_async_copy(arrived_ref.at[i], hold.at[i], load_sem.at[i]) for i in range(pieces)]
            keeps = [
                pltpu.make_async_copy(
                    hold.at[i],
                    new_ref.at[
                        pl.ds(row * units, units), pl.ds(pl.multiple_of(start_ref[i], 128), wide)
                    ],
                    keep_sem.at[i],
                )
                for i, (row, _) in enumerate(places)
            ]
            for load in loads:
                load.start()
            for load, keep in zip(loads, keeps):
                load.wait()
                keep.start()
            for keep in keeps:
                keep.wait()

    return pl.pallas_call(
        kernel,
        in_specs=[pl.BlockSpec(memory_space=pltpu.SMEM)] + [pl.BlockSpec(memory_space=pl.ANY)] * 2,
        out_specs=pl.BlockSpec(memory_space=pl.ANY),
        scratch_shapes=[
            pltpu.VMEM(arrived.shape, arrived.dtype),
            pltpu.SemaphoreType.DMA((pieces,)),
            pltpu.SemaphoreType.DMA((pieces,)),
        ],
        out_shape=jax.ShapeDtypeStruct(base.shape, base.dtype),
        input_output_aliases={2: 0},
        cost_estimate=pl.CostEstimate(
            flops=500 * arrived.size, bytes_accessed=4 * arrived.size, transcendentals=0
        ),
    )(start, arrived, base)


def place_last(arrived, row, column, base, count):
    units, wide = arrived.shape

    def kernel(start_ref, arrived_ref, base_ref, new_ref, keep_sem):
        z = lax.axis_index("fs")

        @pl.when((z == 0) | (z == count - 1))
        def _():
            goal = new_ref.at[pl.ds(row * units, units), pl.ds(pl.multiple_of(start_ref[0], 128), wide)]
            keep = pltpu.make_async_copy(arrived_ref, goal, keep_sem)
            keep.start()
            keep.wait()

    return pl.pallas_call(
        kernel,
        in_specs=[pl.BlockSpec(memory_space=space) for space in (pltpu.SMEM, pltpu.VMEM, pl.ANY)],
        out_specs=pl.BlockSpec(memory_space=pl.ANY),
        out_shape=jax.ShapeDtypeStruct(base.shape, base.dtype),
        scratch_shapes=[pltpu.SemaphoreType.DMA],
        input_output_aliases={2: 0},
        compiler_params=pltpu.CompilerParams(vmem_limit_bytes=4 * arrived.size),
        cost_estimate=pl.CostEstimate(
            flops=500 * arrived.size, bytes_accessed=4 * arrived.size, transcendentals=0
        ),
    )(column.reshape(1), arrived, base)


def pick(tokens, routes, expert):
    tokens_wide = tokens.astype(jnp.float32)
    normed = (
        tokens_wide
        * lax.rsqrt(jnp.mean(tokens_wide * tokens_wide, axis=2, keepdims=True) + norm_eps)
    ).astype(jnp.bfloat16)
    member = jnp.any(routes == expert, axis=2)
    slot_index = jnp.cumsum(member.astype(jnp.int32), axis=1) - 1
    marked = jnp.where(member, slot_index, -1)
    picker = (marked[:, None, :] == jnp.arange(CAP, dtype=jnp.int32)[None, :, None]).astype(jnp.bfloat16)
    chosen = jnp.einsum("gcr,grd->gcd", picker, normed, preferred_element_type=jnp.float32)
    return chosen.astype(jnp.bfloat16).reshape(-1, tokens.shape[2])


def mix(partial_value, routes, route_weights, experts):
    tp_count = lax.axis_size("tp")
    groups = routes.shape[0]
    labels = jnp.arange(experts, dtype=jnp.int32)
    member_all = jnp.any(routes[:, :, :, None] == labels, axis=2)
    slots_all = jnp.cumsum(member_all.astype(jnp.int32), axis=1) - 1
    named = routes[:, :, :, None] == labels
    slot_pair = jnp.sum(jnp.where(named, slots_all[:, :, None, :], 0), axis=3)
    first = CAP * jnp.arange(groups, dtype=jnp.int32)[:, None, None]
    flat_index = (first + slot_pair) * experts + routes
    received = lax.all_to_all(
        partial_value.reshape(groups * CAP, tp_count, -1), "tp", split_axis=1, concat_axis=1, tiled=True
    )
    summed = received.astype(jnp.float32).reshape(groups * CAP * experts, -1)
    picked = jnp.take(summed, flat_index, axis=0)
    return jnp.sum(route_weights[:, :, :, None] * picked, axis=2).astype(jnp.bfloat16)


def line_shards(tokens, gate_train, up_train, down_train, gain, routes, route_weights):
    count = lax.axis_size("fs")
    place = lax.axis_index("fs")
    experts, features, _ = gate_train.shape
    lead = 2
    held = experts - lead
    outward = [(1, 0), (count - 2, count - 1)]
    near_sources = (tokens, routes.T, route_weights.T)
    main, rest, _, _, kept_early, kept_extra, kept_last, *near = gather(
        [train.transpose(0, 2, 1) for train in (gate_train, up_train, down_train)],
        gain, near_sources, count, held, lead,
    )
    low = place < count // 2
    far_start = jnp.where(low, main_start(count - 1, features), main_start(0, features)).astype(jnp.int32)
    next_start = jnp.where(low, main_start(count - 2, features), main_start(1, features)).astype(jnp.int32)
    pairs = [(a * experts + t, b * experts + t) for a, b in outward for t in range(0, experts, 2)]
    arrived_extra = lax.ppermute(kept_extra, ("fs", "tp"), pairs)
    arrived_early = lax.ppermute(kept_early, "fs", outward)

    main, rest, near, near_sources = lax.optimization_barrier((main, rest, near, near_sources))
    both_tokens, both_routes, both_weights = [jnp.stack(pair) for pair in zip(near_sources, near)]
    both_routes, both_weights = both_routes.transpose(0, 2, 1), both_weights.transpose(0, 2, 1)
    chosen = pick(both_tokens, both_routes, lax.axis_index("tp"))
    gate_new, gate_pre = join_in(main, rest, 0, chosen)
    up_new, up_pre = join_in(main, rest, 1, chosen)
    hidden = (jax.nn.silu(gate_pre) * up_pre).astype(jnp.bfloat16)
    down_new, total = join_out(main, rest, 2, hidden)
    both_mixed = mix(total.astype(jnp.bfloat16), both_routes, both_weights, experts)
    half, width = both_mixed.shape[1] // 2, both_mixed.shape[2]
    packed = jnp.concatenate([both_mixed[1, :half], both_mixed[1, half:]], axis=1)
    packed = lax.ppermute(packed, "fs", outward)
    near_mixed = jnp.concatenate([packed[:, :width], packed[:, width:]])
    kept_last, _ = lax.optimization_barrier((kept_last, both_mixed))
    arrived_last = lax.ppermute(kept_last, "fs", outward)
    early = [(i, far_start) for i in range(experts)]
    early += [(i, next_start) for i in range(experts - held, experts - 1)]
    extra = [(i, next_start) for i in range(experts - held - lead, experts - held)]
    down_new = place_late(arrived_extra, extra, True, down_new, count)
    down_new = place_late(arrived_early, early, False, down_new, count)
    down_new = place_last(arrived_last[0], experts - 1, next_start, down_new, count)
    at_end = (place == 0) | (place == count - 1)
    mixed = jnp.where(at_end, near_mixed, both_mixed[0])
    return (gate_new[None], up_new[None], down_new[None], mixed)


def solution(mesh):
    sizes = (mesh.shape["fs"], mesh.shape["tp"])

    def step(*args):
        if not fits(sizes, args[0].shape[0], args[1]):
            return shards(*args)
        return line_shards(*args)

    in_specs = (
        P("fs", None),
        P(None, "fs", "tp"),
        P(None, "fs", "tp"),
        P(None, "fs", "tp"),
        P("fs"),
        P("fs", None),
        P("fs", None),
    )
    out_specs = (P("tp", None, None), P("tp", None, None), P("tp", None, None), P("fs", "tp"))
    return jax.shard_map(step, mesh=mesh, in_specs=in_specs, out_specs=out_specs, check_vma=False)
```

```python
import jax
import jax.numpy as jnp
from jax import lax
from jax.experimental import pallas as pl
from jax.experimental.pallas import tpu as pltpu
from jax.sharding import PartitionSpec as P


CAP = 72


norm_eps = 1e-06


def arrange(matrix, tp_count):
    experts, row_count, col_count = matrix.shape
    slices = tp_count // experts
    piece_width = col_count // slices
    shaped = matrix.reshape(experts, row_count, slices, piece_width)
    return shaped.transpose(0, 2, 3, 1).reshape(tp_count, piece_width, row_count)


def block_of(*counts):
    for size in (256, 128):
        if all(count % size == 0 for count in counts):
            return size
    return None


def flip(wide, total_rows, first_row, base=None):
    features, rows = wide.shape
    size = block_of(rows, first_row, total_rows) or rows
    first = first_row // size

    def kernel(*refs):
        refs[-1][...] = refs[0][...].T

    in_specs = [pl.BlockSpec((features, size), lambda i: (0, i))]
    operands = [wide]
    aliases = {}
    if base is not None:
        in_specs.append(pl.BlockSpec(memory_space=pl.ANY))
        operands.append(base)
        aliases = {1: 0}
    return pl.pallas_call(
        kernel,
        grid=(rows // size,),
        in_specs=in_specs,
        out_specs=pl.BlockSpec((size, features), lambda i: (first + i, 0)),
        out_shape=jax.ShapeDtypeStruct((total_rows, features), wide.dtype),
        input_output_aliases=aliases,
        cost_estimate=pl.CostEstimate(
            flops=0, bytes_accessed=4 * features * rows, transcendentals=0
        ),
    )(*operands)


def columns(wide, first, count, *others):
    size = block_of(first, count, *others)
    if size is None:
        return lax.slice_in_dim(wide, first, first + count, axis=1), count, 0
    return wide, size, first // size


def flip_product(wide, first, rows, chosen):
    features = wide.shape[0]
    wide, size, start = columns(wide, first, rows)
    slots = chosen.shape[0]

    def kernel(wide_ref, chosen_ref, rows_ref, product_ref):
        value = wide_ref[...]
        rows_ref[...] = value.T
        product_ref[...] = jnp.dot(chosen_ref[...], value, preferred_element_type=jnp.float32)

    return pl.pallas_call(
        kernel,
        grid=(rows // size,),
        in_specs=[
            pl.BlockSpec((features, size), lambda i: (0, start + i)),
            pl.BlockSpec((slots, features), lambda i: (0, 0)),
        ],
        out_specs=[
            pl.BlockSpec((size, features), lambda i: (i, 0)),
            pl.BlockSpec((slots, size), lambda i: (0, i)),
        ],
        out_shape=[
            jax.ShapeDtypeStruct((rows, features), wide.dtype),
            jax.ShapeDtypeStruct((slots, rows), jnp.float32),
        ],
        cost_estimate=pl.CostEstimate(
            flops=2 * slots * features * rows,
            bytes_accessed=4 * features * rows,
            transcendentals=0,
        ),
    )(wide, chosen)


def spread(train, gain):
    experts, features, count = train.shape
    rows = experts * count
    size = block_of(rows) or rows

    def kernel(train_ref, gain_ref, out_ref):
        out_ref[...] = (train_ref[...] * gain_ref[...]).astype(jnp.bfloat16).T

    return pl.pallas_call(
        kernel,
        grid=(rows // size,),
        in_specs=[
            pl.BlockSpec((size, features), lambda i: (i, 0)),
            pl.BlockSpec((1, features), lambda i: (0, 0)),
        ],
        out_specs=pl.BlockSpec((features, size), lambda i: (0, i)),
        out_shape=jax.ShapeDtypeStruct((features, rows), jnp.bfloat16),
        cost_estimate=pl.CostEstimate(
            flops=train.size, bytes_accessed=6 * train.size, transcendentals=0
        ),
    )(train.transpose(0, 2, 1).reshape(rows, features), gain[None, :])


def flip_dot(wide, first, total_rows, hidden):
    features = wide.shape[0]
    slots, rows = hidden.shape
    wide, size, start = columns(wide, first, rows, total_rows)

    def kernel(wide_ref, hidden_ref, rows_ref, total_ref):
        turned = wide_ref[...].T
        rows_ref[...] = turned

        @pl.when(pl.program_id(0) == 0)
        def _():
            total_ref[...] = jnp.zeros_like(total_ref)

        total_ref[...] += jnp.dot(hidden_ref[...], turned, preferred_element_type=jnp.float32)

    return pl.pallas_call(
        kernel,
        grid=(rows // size,),
        in_specs=[
            pl.BlockSpec((features, size), lambda i: (0, start + i)),
            pl.BlockSpec((slots, size), lambda i: (0, i)),
        ],
        out_specs=[
            pl.BlockSpec((size, features), lambda i: (i, 0)),
            pl.BlockSpec((slots, features), lambda i: (0, 0)),
        ],
        out_shape=[
            jax.ShapeDtypeStruct((total_rows, features), wide.dtype),
            jax.ShapeDtypeStruct((slots, features), jnp.float32),
        ],
        cost_estimate=pl.CostEstimate(
            flops=2 * slots * features * rows,
            bytes_accessed=4 * features * rows,
            transcendentals=0,
        ),
    )(wide, hidden)


def keep_dot(weights, chosen):
    rows, features = weights.shape
    size = block_of(rows) or rows
    slots = chosen.shape[0]

    def kernel(weights_ref, chosen_ref, rows_ref, product_ref):
        rows_ref[...] = weights_ref[...]
        product_ref[...] = lax.dot_general(
            chosen_ref[...],
            weights_ref[...],
            (((1,), (1,)), ((), ())),
            preferred_element_type=jnp.float32,
        )

    return pl.pallas_call(
        kernel,
        grid=(rows // size,),
        in_specs=[
            pl.BlockSpec((size, features), lambda i: (i, 0)),
            pl.BlockSpec((slots, features), lambda i: (0, 0)),
        ],
        out_specs=[
            pl.BlockSpec((size, features), lambda i: (i, 0)),
            pl.BlockSpec((slots, size), lambda i: (0, i)),
        ],
        out_shape=[
            jax.ShapeDtypeStruct((rows, features), weights.dtype),
            jax.ShapeDtypeStruct((slots, rows), jnp.float32),
        ],
        cost_estimate=pl.CostEstimate(
            flops=2 * slots * features * rows,
            bytes_accessed=4 * features * rows,
            transcendentals=0,
        ),
    )(weights, chosen)


def after(value, *others):
    def kernel(*refs):
        pass

    return pl.pallas_call(
        kernel,
        in_specs=[pl.BlockSpec(memory_space=pl.ANY)] * (1 + len(others)),
        out_specs=pl.BlockSpec(memory_space=pl.ANY),
        out_shape=jax.ShapeDtypeStruct(value.shape, value.dtype),
        input_output_aliases={0: 0},
    )(value, *others)


def shards(tokens, gate_train, up_train, down_train, gain, routes, route_weights):
    tp_count = lax.axis_size("tp")
    experts = gate_train.shape[0]
    slices = tp_count // experts
    gain_column = gain[None, :, None]
    up_round = (up_train * gain_column).astype(jnp.bfloat16)
    down_round = down_train.astype(jnp.bfloat16)

    def exchange(matrix):
        return lax.all_to_all(matrix, "tp", split_axis=0, concat_axis=1, tiled=True)

    gate_all = lax.all_gather(spread(gate_train, gain), "fs", axis=0, tiled=True)
    features = gate_all.shape[0]

    up_moved = exchange(arrange(up_round, tp_count))[0].T
    down_moved = exchange(arrange(down_round, tp_count))[0].T
    units = down_moved.shape[1]
    size = block_of(units) or units
    main = units - size if units > size else units
    both_wide = lax.all_gather(
        jnp.concatenate([up_moved, down_moved[:, :main]], axis=1), "fs", axis=0, tiled=True
    )

    tokens_wide = tokens.astype(jnp.float32)
    normed = (
        tokens_wide
        * lax.rsqrt(jnp.mean(tokens_wide * tokens_wide, axis=1, keepdims=True) + norm_eps)
    ).astype(jnp.bfloat16)
    expert = lax.axis_index("tp") // slices
    matches = routes == expert
    member = jnp.any(matches, axis=1)
    slot_index = jnp.cumsum(member.astype(jnp.int32)) - 1
    marked = jnp.where(member, slot_index, -1)
    picker = (marked[None, :] == jnp.arange(CAP, dtype=jnp.int32)[:, None]).astype(jnp.bfloat16)
    chosen = jnp.dot(picker, normed, preferred_element_type=jnp.float32).astype(jnp.bfloat16)
    contract_last = (((1,), (1,)), ((), ()))

    gate_moved = exchange(gate_all.reshape(features, tp_count, -1).transpose(1, 2, 0))
    gate_new, gate_pre = keep_dot(gate_moved[0], chosen)
    up_new, up_pre = flip_product(both_wide, 0, units, chosen)
    hidden = (jax.nn.silu(gate_pre) * up_pre).astype(jnp.bfloat16)
    down_new, partial_value = flip_dot(both_wide, units, units, hidden[:, :main])
    if main < units:
        rest_moved = after(down_moved[:, main:], gate_new)
        rest_wide = lax.all_gather(rest_moved, "fs", axis=0, tiled=True)
        partial_value = partial_value + lax.dot_general(
            hidden[:, main:], rest_wide, contract_last, preferred_element_type=jnp.float32
        )
        down_new = flip(rest_wide, units, main, down_new)
    partial_value = partial_value.astype(jnp.bfloat16)

    labels = jnp.arange(experts, dtype=jnp.int32)
    member_all = jnp.any(routes[:, :, None] == labels[None, None, :], axis=1)
    slots_all = jnp.cumsum(member_all.astype(jnp.int32), axis=0) - 1
    slot_pair = jnp.take_along_axis(slots_all, routes, axis=1)
    flat_index = slot_pair * experts + routes
    received = lax.all_to_all(
        partial_value.reshape(CAP, tp_count, -1), "tp", split_axis=1, concat_axis=1, tiled=True
    )
    summed = jnp.sum(received.reshape(CAP, experts, slices, -1).astype(jnp.float32), axis=2)
    summed = summed.reshape(CAP * experts, -1)
    picked = jnp.take(summed, flat_index, axis=0)
    mixed = jnp.sum(route_weights[:, :, None] * picked, axis=1)
    return (gate_new[None], up_new[None], down_new[None], mixed.astype(jnp.bfloat16))


def fits(mesh_sizes, rows, train):
    count, tp_count = mesh_sizes
    experts, features, units = train.shape
    return (
        experts == tp_count
        and tp_count & (tp_count - 1) == 0
        and tp_count >= 4
        and count >= 4
        and rows % 64 == 0
        and count % 2 == 0
        and features % 128 == 64
        and units % 32 == 0
        and units <= features - 64
    )


def main_start(block, features):
    return block * features + (64 if block % 2 else 0)


def gather(trains, gain, near_sources, count, held, lead):
    mats = len(trains)
    tp_count, units, features = trains[0].shape
    wide, half = features - 64, units // 2
    pieces = mats * tp_count
    bits = tp_count.bit_length() - 1
    nears = len(near_sources)
    depth = 3

    def kernel(*refs):
        refs = list(refs)
        take = lambda number: [refs.pop(0) for _ in range(number)]
        train_refs, (gain_ref,), sources = take(mats), take(1), take(nears)
        main, rest, own_main, own_rest, early, extra, last = take(7)
        targets = take(nears)
        raw, cast, cast_rest, load_sem, keep_sem = take(5)
        plane_send, plane_recv, plane_rest_send, plane_rest_recv = take(4)
        line_send, line_recv, line_rest_send, line_rest_recv = take(4)
        near_send, near_recv, pass_hold, pass_load, pass_keep = take(5)
        scale, scale_sem = take(2)
        z = lax.axis_index("fs")
        t = lax.axis_index("tp")

        def peer(p):
            total = 0
            for b in range(bits):
                mine, other = (t // (1 << b)) % 2, (p // (1 << b)) % 2
                total = total + (mine + other - 2 * mine * other) * (1 << b)
            return total

        def plane(m, p):
            e = peer(p)
            return pltpu.make_async_remote_copy(
                own_main.at[m * tp_count + e], main.at[z, m * tp_count + t], plane_send.at[m, p], plane_recv.at[m, p],
                device_id={"fs": z, "tp": e}, device_id_type=pl.DeviceIdType.MESH,
            )

        def plane_rest(m, p):
            e = peer(p)
            return pltpu.make_async_remote_copy(
                own_rest.at[m, e], rest.at[z, m, t], plane_rest_send.at[m, p], plane_rest_recv.at[m, p],
                device_id={"fs": z, "tp": e}, device_id_type=pl.DeviceIdType.MESH,
            )

        def line(way, step, i):
            block = z + step if way == 0 else z - step
            target = z - 1 if way == 0 else z + 1
            piece = main.at[block, i // tp_count * tp_count + peer(i % tp_count)]
            return pltpu.make_async_remote_copy(
                piece, piece, line_send.at[way, step], line_recv.at[way, step, i],
                device_id={"fs": target, "tp": t}, device_id_type=pl.DeviceIdType.MESH,
            )

        def line_rest(way, step, m):
            block = z + step if way == 0 else z - step
            target = z - 1 if way == 0 else z + 1
            return pltpu.make_async_remote_copy(
                rest.at[block, m], rest.at[block, m], line_rest_send.at[way, step, m], line_rest_recv.at[way, step, m],
                device_id={"fs": target, "tp": t}, device_id_type=pl.DeviceIdType.MESH,
            )

        def has(way, step):
            return z + step <= count - 1 if way == 0 else z - step >= 0

        def sends(way):
            return z >= 1 if way == 0 else z <= count - 2

        def near(k):
            inward = jnp.where(z == 0, 1, count - 2)
            return pltpu.make_async_remote_copy(
                sources[k], targets[k], near_send.at[k], near_recv.at[k],
                device_id={"fs": inward, "tp": t}, device_id_type=pl.DeviceIdType.MESH,
            )

        def into_end(way, step, m, p, sender):
            if m < mats - 1 or step < count - 3:
                return True
            end = sender == 1 if way == 0 else sender == count - 2
            if step == count - 2:
                return jnp.logical_not(end)
            return jnp.logical_not(end & (peer(p) >= tp_count - held - lead * (1 - t % 2)))

        def leaves(way, step, m, p):
            return into_end(way, step, m, p, z)

        def arrives(way, step, m, p):
            return into_end(way, step, m, p, z + 1 if way == 0 else z - 1)

        def load(m, p):
            slot = (m * tp_count + p) % depth
            return pltpu.make_async_copy(train_refs[m].at[peer(p)], raw.at[slot], load_sem.at[slot])

        def keep(m, p, own):
            slot, place = (m * tp_count + p) % depth, m * tp_count + peer(p)
            goal, goal_rest = (main.at[z], rest.at[z, m]) if own else (own_main, own_rest.at[m])
            return (
                pltpu.make_async_copy(cast.at[slot], goal.at[place], keep_sem.at[0, slot]),
                pltpu.make_async_copy(cast_rest.at[slot], goal_rest.at[peer(p)], keep_sem.at[1, slot]),
            )

        def load_ahead(m, p):
            if m < mats:
                load(m, p).start()

        def convert(m, p, own):
            slot = (m * tp_count + p) % depth
            load(m, p).wait()

            def put(odd):
                value = raw[slot]
                if m < mats - 1:
                    value = value * scale[...].reshape(1, features)
                value = value.astype(cast.dtype)
                if odd:
                    cast[slot], end = value[:, 64:], value[:, :64]
                else:
                    cast[slot], end = value[:, :wide], value[:, wide:]
                cast_rest[slot] = jnp.concatenate([end[:half], end[half:]], axis=1)

            pl.when(z % 2 == 0)(lambda: put(False))
            pl.when(z % 2 == 1)(lambda: put(True))
            for copy in keep(m, p, own):
                copy.start()

        def finish(m, p, own):
            for copy in keep(m, p, own):
                copy.wait()
            if not own:
                plane(m, p).start()
                plane_rest(m, p).start()

        def forward(step, m, p, first=False):
            i = m * tp_count + p
            if step == 0 and not first:
                plane(m, p).wait_recv()
            for way in range(2):
                if step > 0:
                    @pl.when(has(way, step) & arrives(way, step - 1, m, p))
                    def _(way=way):
                        line(way, step - 1, i).wait_recv()
                if step < count - 1:
                    @pl.when(has(way, step) & sends(way) & leaves(way, step, m, p))
                    def _(way=way):
                        line(way, step, i).start()

        def forward_rest(step, m):
            if step == 0:
                @pl.loop(1, tp_count)
                def _(p):
                    plane_rest(m, p).wait_recv()
            for way in range(2):
                if step > 0:
                    @pl.when(has(way, step))
                    def _(way=way):
                        line_rest(way, step - 1, m).wait_recv()
                if step < count - 1:
                    @pl.when(has(way, step) & sends(way))
                    def _(way=way):
                        line_rest(way, step, m).start()

        barrier = pltpu.get_barrier_semaphore()
        for p in range(1, tp_count):
            pl.semaphore_signal(
                barrier, inc=1, device_id={"fs": z, "tp": peer(p)}, device_id_type=pl.DeviceIdType.MESH
            )

        @pl.when(z >= 1)
        def _():
            pl.semaphore_signal(
                barrier, inc=1, device_id={"fs": z - 1, "tp": t}, device_id_type=pl.DeviceIdType.MESH
            )

        @pl.when(z <= count - 2)
        def _():
            pl.semaphore_signal(
                barrier, inc=1, device_id={"fs": z + 1, "tp": t}, device_id_type=pl.DeviceIdType.MESH
            )

        scale_copy = pltpu.make_async_copy(gain_ref, scale, scale_sem)
        scale_copy.start()
        for p in range(depth):
            load(0, p).start()
        scale_copy.wait()
        for m in range(mats):
            convert(m, 0, True)
            load_ahead(m, depth)
            if m == 0:
                middle = jnp.logical_and(z >= 1, z <= count - 2)
                pl.semaphore_wait(barrier, tp_count + jnp.where(middle, 1, 0))
                finish(0, 0, True)
                forward(0, 0, 0, first=True)
            else:
                finish(m - 1, tp_count - 1, False)
                if m > 1:
                    forward(0, m - 1, 0, first=True)

            @pl.loop(1, tp_count)
            def _(p, m=m):
                convert(m, p, False)
                pl.when(p + depth < tp_count)(lambda: load(m, p + depth).start())
                if m + 1 < mats:
                    pl.when(p + depth >= tp_count)(lambda: load(m + 1, p + depth - tp_count).start())
                if m == 0:
                    pl.when(p >= 2)(lambda: finish(m, p - 1, False))
                    pl.when(p == tp_count // 2)(lambda: forward(0, 0, 1))
                else:
                    pl.when(p == 1)(lambda: finish(m, 0, True))
                    pl.when(p >= 2)(lambda: finish(m, p - 1, False))
                    if m == 1:
                        pl.when(p >= 2)(lambda: forward(0, 0, p))
                    else:
                        forward(0, m - 1, p)

            if m > 0:
                forward_rest(0, m - 1)
        finish(mats - 1, tp_count - 1, False)
        forward(0, mats - 1, 0, first=True)

        @pl.loop(1, tp_count)
        def _(p):
            forward(0, mats - 1, p)

        forward_rest(0, mats - 1)

        @pl.when((z == 0) | (z == count - 1))
        def _():
            for k in range(nears):
                near(k).start()

        for step in range(1, count):
            for m in range(mats):
                @pl.loop(0, tp_count)
                def _(p, step=step, m=m):
                    forward(step, m, p)

                forward_rest(step, m)

        @pl.when((z == 1) | (z == count - 2))
        def _():
            low = z < count // 2
            far, after_far = jnp.where(low, count - 1, 0), jnp.where(low, count - 2, 1)
            first = pieces - held - lead
            found = [main.at[far, pieces - tp_count + i] for i in range(tp_count)]
            found += [main.at[after_far, first + i] for i in range(lead + held)]
            goal = [early.at[i] for i in range(tp_count)] + [extra.at[i] for i in range(lead)]
            goal += [early.at[tp_count + i] for i in range(held - 1)] + [last.at[0]]
            loads = [pltpu.make_async_copy(f, pass_hold.at[i], pass_load.at[i]) for i, f in enumerate(found)]
            keeps = [pltpu.make_async_copy(pass_hold.at[i], g, pass_keep.at[i]) for i, g in enumerate(goal)]
            for load in loads:
                load.start()
            for load, keep in zip(loads, keeps):
                load.wait()
                keep.start()
            for keep in keeps:
                keep.wait()

        for m in range(mats):
            @pl.loop(1, tp_count)
            def _(p, m=m):
                plane(m, p).wait_send()
                plane_rest(m, p).wait_send()

        @pl.when((z == 0) | (z == count - 1))
        def _():
            for k in range(nears):
                near(k).wait_send()

        @pl.when((z == 1) | (z == count - 2))
        def _():
            for k in range(nears):
                near(k).wait_recv()

        for step in range(count - 1):
            for way in range(2):
                @pl.when(has(way, step) & sends(way))
                def _(way=way, step=step):
                    end = z == (1 if way == 0 else count - 2)

                    def settle(number, way=way, step=step):
                        sent = main.at[z, pl.ds(0, number)]
                        pltpu.make_async_copy(sent, sent, line_send.at[way, step]).wait()

                    if step == count - 2:
                        settle(pieces - tp_count)
                    elif step == count - 3:
                        pl.when(end & (t % 2 == 0))(lambda: settle(pieces - held - lead))
                        pl.when(end & (t % 2 == 1))(lambda: settle(pieces - held))
                        pl.when(jnp.logical_not(end))(lambda: settle(pieces))
                    else:
                        settle(pieces)
                    for m in range(mats):
                        line_rest(way, step, m).wait_send()

    dma = pltpu.SemaphoreType.DMA
    dtype = jnp.bfloat16
    own = pieces * units * features
    anywhere = pl.BlockSpec(memory_space=pl.ANY)
    outs = [
        (count, pieces, units, wide),
        (count, mats, tp_count, half, 128),
        (pieces, units, wide),
        (mats, tp_count, half, 128),
        (tp_count + held - 1, units, wide),
        (lead, units, wide),
        (1, units, wide),
    ]
    return pl.pallas_call(
        kernel,
        in_specs=[anywhere] * (mats + 1 + nears),
        out_specs=[anywhere] * (len(outs) + nears),
        out_shape=[jax.ShapeDtypeStruct(shape, dtype) for shape in outs]
        + [jax.ShapeDtypeStruct(source.shape, source.dtype) for source in near_sources],
        scratch_shapes=[
            pltpu.VMEM((depth, units, features), jnp.float32),
            pltpu.VMEM((depth, units, wide), dtype),
            pltpu.VMEM((depth, half, 128), dtype),
            dma((depth,)),
            dma((2, depth)),
            dma((mats, tp_count)),
            dma((mats, tp_count)),
            dma((mats, tp_count)),
            dma((mats, tp_count)),
            dma((2, count - 1)),
            dma((2, count - 1, pieces)),
            dma((2, count - 1, mats)),
            dma((2, count - 1, mats)),
            dma((nears,)),
            dma((nears,)),
            pltpu.VMEM((tp_count + held + lead, units, wide), dtype),
            dma((tp_count + held + lead,)),
            dma((tp_count + held + lead,)),
            pltpu.VMEM(gain.shape, gain.dtype),
            dma,
        ],
        compiler_params=pltpu.CompilerParams(collective_id=0, has_side_effects=True),
        cost_estimate=pl.CostEstimate(
            flops=1000 * own, bytes_accessed=4 * (count + 3) * own, transcendentals=0
        ),
    )(*trains, gain, *near_sources)


def joined(main_ref, rest_ref, out_ref):
    count, _, units, wide = main_ref.shape
    features = wide + 64
    half = units // 2
    for block in range(count):
        out_ref[:, pl.ds(main_start(block, features), wide)] = main_ref[block, 0]
    for block in range(0, count, 2):
        first, second = rest_ref[block, 0, 0], rest_ref[block + 1, 0, 0]
        place = pl.ds(block * features + wide, 128)
        out_ref[:half, place] = jnp.concatenate([first[:, :64], second[:, :64]], axis=1)
        out_ref[half:, place] = jnp.concatenate([first[:, 64:], second[:, 64:]], axis=1)


def join_call(main, rest, which, kernel, operand, operand_spec, product_spec, product_shape):
    count, _, tp_count, half = rest.shape[:4]
    units, wide = main.shape[2:]
    features = count * (wide + 64)
    return pl.pallas_call(
        kernel,
        grid=(tp_count,),
        in_specs=[
            pl.BlockSpec((count, 1, units, wide), lambda i: (0, which * tp_count + i, 0, 0)),
            pl.BlockSpec((count, 1, 1, half, 128), lambda i: (0, which, i, 0, 0)),
            operand_spec,
        ],
        out_specs=[pl.BlockSpec((units, features), lambda i: (i, 0)), product_spec],
        out_shape=[
            jax.ShapeDtypeStruct((tp_count * units, features), main.dtype),
            jax.ShapeDtypeStruct(product_shape, jnp.float32),
        ],
        cost_estimate=pl.CostEstimate(
            flops=1000 * tp_count * units * features,
            bytes_accessed=4 * tp_count * units * features,
            transcendentals=0,
        ),
    )(main, rest, operand)


def join_in(main, rest, which, chosen):
    tp_count, units = rest.shape[2], main.shape[2]
    slots, features = chosen.shape

    def kernel(main_ref, rest_ref, chosen_ref, new_ref, product_ref):
        joined(main_ref, rest_ref, new_ref)
        product_ref[0] = lax.dot_general(
            chosen_ref[...], new_ref[...], (((1,), (1,)), ((), ())), preferred_element_type=jnp.float32
        )

    return join_call(
        main, rest, which, kernel, chosen,
        pl.BlockSpec((slots, features), lambda i: (0, 0)),
        pl.BlockSpec((1, slots, units), lambda i: (i, 0, 0)),
        (tp_count, slots, units),
    )


def join_out(main, rest, which, hidden):
    _, slots, units = hidden.shape
    features = main.shape[0] * (main.shape[3] + 64)

    def kernel(main_ref, rest_ref, hidden_ref, new_ref, total_ref):
        joined(main_ref, rest_ref, new_ref)

        @pl.when(pl.program_id(0) == 0)
        def _():
            total_ref[...] = jnp.zeros_like(total_ref)

        total_ref[...] += jnp.dot(hidden_ref[0], new_ref[...], preferred_element_type=jnp.float32)

    return join_call(
        main, rest, which, kernel, hidden,
        pl.BlockSpec((1, slots, units), lambda i: (i, 0, 0)),
        pl.BlockSpec((slots, features), lambda i: (0, 0)),
        (slots, features),
    )


def place_late(arrived, places, even_only, base, count):
    pieces, units, wide = arrived.shape
    start = jnp.stack([column for _, column in places])

    def kernel(start_ref, arrived_ref, base_ref, new_ref, hold, load_sem, keep_sem):
        z, t = lax.axis_index("fs"), lax.axis_index("tp")
        wanted = (z == 0) | (z == count - 1)
        if even_only:
            wanted = wanted & (t % 2 == 0)

        @pl.when(wanted)
        def _():
            loads = [pltpu.make_async_copy(arrived_ref.at[i], hold.at[i], load_sem.at[i]) for i in range(pieces)]
            keeps = [
                pltpu.make_async_copy(
                    hold.at[i],
                    new_ref.at[
                        pl.ds(row * units, units), pl.ds(pl.multiple_of(start_ref[i], 128), wide)
                    ],
                    keep_sem.at[i],
                )
                for i, (row, _) in enumerate(places)
            ]
            for load in loads:
                load.start()
            for load, keep in zip(loads, keeps):
                load.wait()
                keep.start()
            for keep in keeps:
                keep.wait()

    return pl.pallas_call(
        kernel,
        in_specs=[pl.BlockSpec(memory_space=pltpu.SMEM)] + [pl.BlockSpec(memory_space=pl.ANY)] * 2,
        out_specs=pl.BlockSpec(memory_space=pl.ANY),
        scratch_shapes=[
            pltpu.VMEM(arrived.shape, arrived.dtype),
            pltpu.SemaphoreType.DMA((pieces,)),
            pltpu.SemaphoreType.DMA((pieces,)),
        ],
        out_shape=jax.ShapeDtypeStruct(base.shape, base.dtype),
        input_output_aliases={2: 0},
        cost_estimate=pl.CostEstimate(
            flops=500 * arrived.size, bytes_accessed=4 * arrived.size, transcendentals=0
        ),
    )(start, arrived, base)


def place_last(arrived, row, column, base, count):
    units, wide = arrived.shape

    def kernel(start_ref, arrived_ref, base_ref, new_ref, keep_sem):
        z = lax.axis_index("fs")

        @pl.when((z == 0) | (z == count - 1))
        def _():
            goal = new_ref.at[pl.ds(row * units, units), pl.ds(pl.multiple_of(start_ref[0], 128), wide)]
            keep = pltpu.make_async_copy(arrived_ref, goal, keep_sem)
            keep.start()
            keep.wait()

    return pl.pallas_call(
        kernel,
        in_specs=[pl.BlockSpec(memory_space=space) for space in (pltpu.SMEM, pltpu.VMEM, pl.ANY)],
        out_specs=pl.BlockSpec(memory_space=pl.ANY),
        out_shape=jax.ShapeDtypeStruct(base.shape, base.dtype),
        scratch_shapes=[pltpu.SemaphoreType.DMA],
        input_output_aliases={2: 0},
        compiler_params=pltpu.CompilerParams(vmem_limit_bytes=4 * arrived.size),
        cost_estimate=pl.CostEstimate(
            flops=500 * arrived.size, bytes_accessed=4 * arrived.size, transcendentals=0
        ),
    )(column.reshape(1), arrived, base)


def pick(tokens, routes, expert):
    tokens_wide = tokens.astype(jnp.float32)
    normed = (
        tokens_wide
        * lax.rsqrt(jnp.mean(tokens_wide * tokens_wide, axis=2, keepdims=True) + norm_eps)
    ).astype(jnp.bfloat16)
    member = jnp.any(routes == expert, axis=2)
    slot_index = jnp.cumsum(member.astype(jnp.int32), axis=1) - 1
    marked = jnp.where(member, slot_index, -1)
    picker = (marked[:, None, :] == jnp.arange(CAP, dtype=jnp.int32)[None, :, None]).astype(jnp.bfloat16)
    chosen = jnp.einsum("gcr,grd->gcd", picker, normed, preferred_element_type=jnp.float32)
    return chosen.astype(jnp.bfloat16).reshape(-1, tokens.shape[2])


def mix(partial_value, routes, route_weights, experts):
    tp_count = lax.axis_size("tp")
    groups = routes.shape[0]
    labels = jnp.arange(experts, dtype=jnp.int32)
    member_all = jnp.any(routes[:, :, :, None] == labels, axis=2)
    slots_all = jnp.cumsum(member_all.astype(jnp.int32), axis=1) - 1
    named = routes[:, :, :, None] == labels
    slot_pair = jnp.sum(jnp.where(named, slots_all[:, :, None, :], 0), axis=3)
    first = CAP * jnp.arange(groups, dtype=jnp.int32)[:, None, None]
    flat_index = (first + slot_pair) * experts + routes
    received = lax.all_to_all(
        partial_value.reshape(groups * CAP, tp_count, -1), "tp", split_axis=1, concat_axis=1, tiled=True
    )
    summed = received.astype(jnp.float32).reshape(groups * CAP * experts, -1)
    picked = jnp.take(summed, flat_index, axis=0)
    return jnp.sum(route_weights[:, :, :, None] * picked, axis=2).astype(jnp.bfloat16)


def line_shards(tokens, gate_train, up_train, down_train, gain, routes, route_weights):
    count = lax.axis_size("fs")
    place = lax.axis_index("fs")
    experts, features, _ = gate_train.shape
    lead = 2
    held = experts - lead
    outward = [(1, 0), (count - 2, count - 1)]
    near_sources = (tokens, routes.T, route_weights.T)
    main, rest, _, _, kept_early, kept_extra, kept_last, *near = gather(
        [train.transpose(0, 2, 1) for train in (gate_train, up_train, down_train)],
        gain, near_sources, count, held, lead,
    )
    low = place < count // 2
    far_start = jnp.where(low, main_start(count - 1, features), main_start(0, features)).astype(jnp.int32)
    next_start = jnp.where(low, main_start(count - 2, features), main_start(1, features)).astype(jnp.int32)
    pairs = [(a * experts + t, b * experts + t) for a, b in outward for t in range(0, experts, 2)]
    arrived_extra = lax.ppermute(kept_extra, ("fs", "tp"), pairs)
    arrived_early = lax.ppermute(kept_early, "fs", outward)

    main, rest, near, near_sources = lax.optimization_barrier((main, rest, near, near_sources))
    both_tokens, both_routes, both_weights = [jnp.stack(pair) for pair in zip(near_sources, near)]
    both_routes, both_weights = both_routes.transpose(0, 2, 1), both_weights.transpose(0, 2, 1)
    chosen = pick(both_tokens, both_routes, lax.axis_index("tp"))
    gate_new, gate_pre = join_in(main, rest, 0, chosen)
    up_new, up_pre = join_in(main, rest, 1, chosen)
    hidden = (jax.nn.silu(gate_pre) * up_pre).astype(jnp.bfloat16)
    down_new, total = join_out(main, rest, 2, hidden)
    both_mixed = mix(total.astype(jnp.bfloat16), both_routes, both_weights, experts)
    width = both_mixed.shape[2]
    packed = jnp.concatenate(jnp.split(both_mixed[1], 4), axis=1)
    packed = lax.ppermute(packed, "fs", outward)
    near_mixed = jnp.concatenate([packed[:, i * width : (i + 1) * width] for i in range(4)])
    kept_last, _ = lax.optimization_barrier((kept_last, both_mixed))
    arrived_last = lax.ppermute(kept_last, "fs", outward)
    early = [(i, far_start) for i in range(experts)]
    early += [(i, next_start) for i in range(experts - held, experts - 1)]
    extra = [(i, next_start) for i in range(experts - held - lead, experts - held)]
    down_new = place_late(arrived_extra, extra, True, down_new, count)
    down_new = place_late(arrived_early, early, False, down_new, count)
    down_new = place_last(arrived_last[0], experts - 1, next_start, down_new, count)
    at_end = (place == 0) | (place == count - 1)
    mixed = jnp.where(at_end, near_mixed, both_mixed[0])
    return (gate_new[None], up_new[None], down_new[None], mixed)


def solution(mesh):
    sizes = (mesh.shape["fs"], mesh.shape["tp"])

    def step(*args):
        if not fits(sizes, args[0].shape[0], args[1]):
            return shards(*args)
        return line_shards(*args)

    in_specs = (
        P("fs", None),
        P(None, "fs", "tp"),
        P(None, "fs", "tp"),
        P(None, "fs", "tp"),
        P("fs"),
        P("fs", None),
        P("fs", None),
    )
    out_specs = (P("tp", None, None), P("tp", None, None), P("tp", None, None), P("fs", "tp"))
    return jax.shard_map(step, mesh=mesh, in_specs=in_specs, out_specs=out_specs, check_vma=False)
```
